512 devices in a mesh: grp: 2 (over y), tp: 16 (over z), dp: 16 (over x, core).
Axes of the slice: x: 8, y: 2, z: 16, core: 2. Of those that a mesh axis runs over, the one named last changes fastest.
The devices are a block of a 8x16x16 slice.
Arguments:
- tokens: bfloat16 [512, 2048], P(('grp', 'tp'), 'dp'), parts along dimension 0, may hold values from -200 to 200
- norm_gain: bfloat16 [2, 2048], P(None, 'dp'), may hold values from 0.099609375 to 1.8984375
- w_z: bfloat16 [2, 2048, 4096], P(None, 'dp', 'tp'), may hold values from -0.125 to 0.125
- w_x: bfloat16 [2, 2048, 4096], P(None, 'dp', 'tp'), may hold values from -0.125 to 0.125
- w_b: bfloat16 [2, 2048, 1024], P(None, 'dp', 'tp'), may hold values from -0.125 to 0.125
- w_c: bfloat16 [2, 2048, 1024], P(None, 'dp', 'tp'), may hold values from -0.125 to 0.125
- w_dt: bfloat16 [2, 2048, 64], P(None, 'dp'), may hold values from -0.125 to 0.125
- conv_x: bfloat16 [2, 4, 4096], P(None, None, 'tp'), may hold values from -3 to 3
- conv_b: bfloat16 [2, 4, 1024], P(None, None, 'tp'), may hold values from -3 to 3
- conv_c: bfloat16 [2, 4, 1024], P(None, None, 'tp'), may hold values from -3 to 3
- dt_bias: float32 [2, 64], P(None, 'tp'), may hold values from -3 to 0.5
- a_log: float32 [2, 64], P(None, 'tp'), may hold values from 0 to 2.5
- d_skip: float32 [2, 64], P(None, 'tp'), may hold values from 0.5 to 2
- out_gain: bfloat16 [2, 4096], P(None, 'tp'), may hold values from 0.099609375 to 1.8984375
- w_out: bfloat16 [2, 4096, 2048], P(None, 'tp', 'dp'), may hold values from -0.09375 to 0.09375
- ssm_state: float32 [2, 512, 64, 64, 64], P(None, ('grp', 'dp'), 'tp'), parts along dimension 1, may hold values from -3 to 3
- state_x: bfloat16 [2, 512, 3, 4096], P(None, ('grp', 'dp'), None, 'tp'), parts along dimension 1, may hold values from -6 to 6
- state_b: bfloat16 [2, 512, 3, 1024], P(None, ('grp', 'dp'), None, 'tp'), parts along dimension 1, may hold values from -6 to 6
- state_c: bfloat16 [2, 512, 3, 1024], P(None, ('grp', 'dp'), None, 'tp'), parts along dimension 1, may hold values from -6 to 6
Outputs:
- residual: bfloat16 [512, 2048], P(('grp', 'tp'), 'dp'), parts along dimension 0
- ssm_next: float32 [2, 512, 64, 64, 64], P(None, ('grp', 'dp'), 'tp'), parts along dimension 1
- next_x: bfloat16 [2, 512, 3, 4096], P(None, ('grp', 'dp'), None, 'tp'), parts along dimension 1
- next_b: bfloat16 [2, 512, 3, 1024], P(None, ('grp', 'dp'), None, 'tp'), parts along dimension 1
- next_c: bfloat16 [2, 512, 3, 1024], P(None, ('grp', 'dp'), None, 'tp'), parts along dimension 1
The draws below stay inside these ranges and needn't reach their ends.
There are 2 independent parts, one for each index of `grp`. The reference program is written for one: setup_inputs(seed, part) draws one part's arguments, and reference() takes and returns one part's arrays. A program takes and returns all parts, laid end to end along the dimension named above; an argument that names none is the same for every part. Nothing has to cross between parts.
All inputs are finite; a program needn't handle non-finite values.
Results may differ from the reference program's by a relative error of at most 0.0095.
Values may be sent and summed in bfloat16 or wider, within the bound.
A program may use at most 64 MiB of HBM per device.

```python
import jax
import jax.numpy as jnp
from jax import lax

D = 2048
HEADS = 64
HEAD_DIM = 64
GROUPS = 16
STATE = 64
KW = 4
LAYERS = 2
SW = 4096
SEQS = 256


def draw_tokens(key, part):
    ramp = jnp.exp(jnp.log(4.0) * jnp.arange(D, dtype=jnp.float32) / D)
    values = jnp.clip(jax.random.normal(jax.random.fold_in(key, 13), (SEQS, D), jnp.float32), -5.0, 5.0)
    return (values * ramp[None, :]).astype(jnp.bfloat16)


def block_levels(key, shape, cuts, low, high):
    level = 1.0
    for axis_at, blocks in cuts:
        steps = jax.random.uniform(jax.random.fold_in(jax.random.fold_in(key, 6), axis_at), (blocks,), jnp.float32, low / len(cuts), high / len(cuts))
        level = level * jnp.repeat(jnp.exp(steps), shape[axis_at] // blocks).reshape((-1,) + (1,) * (len(shape) - 1 - axis_at))
    return level


def normal_values(rng, dims, spread, most, split=(), kind=jnp.bfloat16):
    level = block_levels(rng, dims, split, -0.22, 0.18) if split else 1.0
    drawn = jax.random.normal(rng, dims, jnp.float32) * spread * level
    return jnp.minimum(jnp.maximum(drawn, -most), most).astype(kind)


def setup_inputs(seed: int = 0, part: int = 0) -> dict:
    arg_keys = jax.random.split(jax.random.key(seed), 20)
    part_splits = jax.random.split(jax.random.fold_in(arg_keys[19], part), 20)
    tokens = draw_tokens(jax.random.fold_in(jax.random.fold_in(arg_keys[19], part), 71), part)
    norm_gain = jnp.clip(1.0 + 0.18 * jax.random.normal(arg_keys[1], (LAYERS, D), jnp.float32), 0.099609375, 1.8984375).astype(jnp.bfloat16)
    w_z = normal_values(arg_keys[2], (LAYERS, D, SW), D ** -0.5, 0.125, ((1, 16), (2, 16)))
    w_x = normal_values(arg_keys[3], (LAYERS, D, SW), D ** -0.5, 0.125, ((1, 16), (2, 16)))
    w_b = normal_values(arg_keys[4], (LAYERS, D, GROUPS * STATE), D ** -0.5, 0.125, ((1, 16), (2, 16)))
    w_c = normal_values(arg_keys[5], (LAYERS, D, GROUPS * STATE), D ** -0.5, 0.125, ((1, 16), (2, 16)))
    w_dt = normal_values(arg_keys[6], (LAYERS, D, HEADS), D ** -0.5, 0.125, ((1, 16),))
    conv_x = normal_values(arg_keys[7], (LAYERS, KW, SW), 0.5, 3.0, ((2, 16),))
    conv_b = normal_values(arg_keys[8], (LAYERS, KW, GROUPS * STATE), 0.5, 3.0, ((2, 16),))
    conv_c = normal_values(arg_keys[9], (LAYERS, KW, GROUPS * STATE), 0.5, 3.0, ((2, 16),))
    dt_bias = jnp.clip(-3.0 + 3.5 * jax.random.uniform(arg_keys[10], (LAYERS, HEADS), jnp.float32) ** block_levels(arg_keys[10], (LAYERS, HEADS), ((1, 16),), -0.2, 0.2), -3.0, 0.5)
    a_log = jnp.clip(2.5 * jax.random.uniform(arg_keys[11], (LAYERS, HEADS), jnp.float32) ** block_levels(arg_keys[11], (LAYERS, HEADS), ((1, 16),), -0.2, 0.2), 0.0, 2.5)
    d_skip = jnp.clip(0.5 + 1.5 * jax.random.uniform(arg_keys[12], (LAYERS, HEADS), jnp.float32) ** block_levels(arg_keys[12], (LAYERS, HEADS), ((1, 16),), -0.2, 0.2), 0.5, 2.0)
    out_gain = jnp.clip(1.0 + 0.18 * jax.random.normal(arg_keys[13], (LAYERS, SW), jnp.float32), 0.099609375, 1.8984375).astype(jnp.bfloat16)
    w_out = normal_values(arg_keys[14], (LAYERS, SW, D), SW ** -0.5, 0.09375, ((1, 16), (2, 16)))
    ssm_state = normal_values(part_splits[15], (LAYERS, SEQS, HEADS, HEAD_DIM, STATE), 0.5, 3.0, ((1, 16), (2, 16)), jnp.float32)
    state_x = normal_values(part_splits[16], (LAYERS, SEQS, KW - 1, SW), 1.0, 6.0, ((1, 16), (3, 16)))
    state_b = normal_values(part_splits[17], (LAYERS, SEQS, KW - 1, GROUPS * STATE), 1.0, 6.0, ((1, 16), (3, 16)))
    state_c = normal_values(part_splits[18], (LAYERS, SEQS, KW - 1, GROUPS * STATE), 1.0, 6.0, ((1, 16), (3, 16)))
    return {"tokens": tokens, "norm_gain": norm_gain, "w_z": w_z, "w_x": w_x, "w_b": w_b, "w_c": w_c, "w_dt": w_dt, "conv_x": conv_x, "conv_b": conv_b, "conv_c": conv_c, "dt_bias": dt_bias, "a_log": a_log, "d_skip": d_skip, "out_gain": out_gain, "w_out": w_out, "ssm_state": ssm_state, "state_x": state_x, "state_b": state_b, "state_c": state_c}


EPSILON = 1e-05

def convolve(history, latest, weight):
    window = jnp.concatenate([history, latest[:, None, :]], axis=1)
    summed = lax.optimization_barrier(jnp.sum(window.astype(jnp.float32) * weight.astype(jnp.float32)[None], axis=1))
    return (jax.nn.silu(summed), window[:, 1:])

def mixer(gate_in, conv_xv, conv_bv, conv_cv, step_raw, bias, log_rate, skip, gain, state_prev):
    seq_count = conv_xv.shape[0]
    heads_here = step_raw.shape[1]
    group_count = conv_bv.shape[1] // STATE
    per_group = heads_here // group_count
    step_size = jax.nn.softplus(step_raw + bias)
    decay_rate = jnp.exp(-step_size * jnp.exp(log_rate))
    x_heads = conv_xv.reshape(seq_count, group_count, per_group, HEAD_DIM)
    b_state = conv_bv.reshape(seq_count, group_count, 1, 1, STATE)
    c_state = conv_cv.reshape(seq_count, group_count, 1, 1, STATE)
    step_heads = step_size.reshape(seq_count, group_count, per_group, 1)
    decay_heads = decay_rate.reshape(seq_count, group_count, per_group, 1, 1)
    previous = state_prev.reshape(seq_count, group_count, per_group, HEAD_DIM, STATE)
    state_next = decay_heads * previous + (step_heads * x_heads)[..., None] * b_state
    readout = lax.optimization_barrier(jnp.sum(state_next * c_state, axis=-1)) + skip.reshape(1, group_count, per_group, 1) * x_heads
    gated_out = readout.reshape(seq_count, group_count, -1) * jax.nn.silu(gate_in.astype(jnp.float32)).reshape(seq_count, group_count, -1)
    normed = gated_out * lax.rsqrt(lax.optimization_barrier(jnp.mean(gated_out * gated_out, axis=-1, keepdims=True)) + EPSILON)
    mixed_out = (normed.reshape(seq_count, -1) * gain.astype(jnp.float32)).astype(jnp.bfloat16)
    return (mixed_out, state_next.reshape(seq_count, heads_here, HEAD_DIM, STATE))

def reference(tokens, norm_gain, w_z, w_x, w_b, w_c, w_dt, conv_x, conv_b, conv_c, dt_bias, a_log, d_skip, out_gain, w_out, ssm_state, state_x, state_b, state_c):
    residual = tokens
    states, saved_x, saved_b, saved_c = ([], [], [], [])
    for layer_index in range(LAYERS):
        widened = residual.astype(jnp.float32)
        row_scale = lax.rsqrt(lax.optimization_barrier(jnp.mean(widened * widened, axis=1, keepdims=True)) + EPSILON)
        scaled = (widened * norm_gain[layer_index].astype(jnp.float32)).astype(jnp.bfloat16)
        gate_in = (jnp.dot(scaled, w_z[layer_index], preferred_element_type=jnp.float32) * row_scale).astype(jnp.bfloat16)
        x_in = (jnp.dot(scaled, w_x[layer_index], preferred_element_type=jnp.float32) * row_scale).astype(jnp.bfloat16)
        b_in = (jnp.dot(scaled, w_b[layer_index], preferred_element_type=jnp.float32) * row_scale).astype(jnp.bfloat16)
        c_in = (jnp.dot(scaled, w_c[layer_index], preferred_element_type=jnp.float32) * row_scale).astype(jnp.bfloat16)
        step_raw = jnp.dot(scaled, w_dt[layer_index], preferred_element_type=jnp.float32) * row_scale
        conv_xv, kept_x = convolve(state_x[layer_index], x_in, conv_x[layer_index])
        conv_bv, kept_b = convolve(state_b[layer_index], b_in, conv_b[layer_index])
        conv_cv, kept_c = convolve(state_c[layer_index], c_in, conv_c[layer_index])
        mixed_out, state_next = mixer(gate_in, conv_xv, conv_bv, conv_cv, step_raw, dt_bias[layer_index], a_log[layer_index], d_skip[layer_index], out_gain[layer_index], ssm_state[layer_index])
        projected = jnp.dot(mixed_out, w_out[layer_index], preferred_element_type=jnp.float32)
        residual = (widened + projected).astype(jnp.bfloat16)
        states.append(state_next)
        saved_x.append(kept_x)
        saved_b.append(kept_b)
        saved_c.append(kept_c)
    return (residual, jnp.stack(states), jnp.stack(saved_x), jnp.stack(saved_b), jnp.stack(saved_c))
```

```python
import functools

import jax
import jax.numpy as jnp
from jax import lax
from jax.experimental import pallas as pl
from jax.experimental.pallas import tpu as pltpu
from jax.sharding import PartitionSpec as P

EPSILON = 1e-05
F32 = jnp.float32
BF16 = jnp.bfloat16
MESH = pl.DeviceIdType.MESH
NT = (((1,), (1,)), ((), ()))
LANES = 128


def silu(v):
    return v * jax.nn.sigmoid(v)


def kernel(
    tp_n,
    dp_n,
    features,
    tok,
    gain,
    w_z,
    w_x,
    w_bt,
    w_ct,
    w_dtt,
    conv_x,
    conv_b,
    conv_c,
    dt_bias,
    a_log,
    d_skip,
    out_gain,
    w_out_h,
    ssm_h,
    s_x,
    s_b,
    s_c,
    res_o,
    ssm_oh,
    nx_o,
    nb_o,
    nc_o,
    a_buf,
    b_out,
    b_in,
    c_own,
    c_buf,
    d_out,
    d_in,
    r_buf,
    w_bcd,
    conv_bc,
    s_bc,
    st_t,
    w_out,
    ssm,
    ssm_o,
    local_sem,
    out_sem,
    send_sem,
    recv_sem,
):
    layers, heads_here = dt_bias.shape
    rows, width_f = tok.shape
    zw = w_z.shape[2]
    bw = w_bt.shape[1]
    hd = zw // heads_here
    my_tp, my_dp = lax.axis_index("tp"), lax.axis_index("dp")
    my_x, my_core = lax.div(my_dp, 2), lax.rem(my_dp, 2)
    dp_x = dp_n // 2

    def tp_at(k):
        off = jnp.where(lax.rem(k, 2) == 1, lax.div(k + 1, 2), tp_n - lax.div(k, 2))
        return lax.rem(my_tp + off, tp_n)

    def dp_at(k):
        m = lax.div(k, 2)
        off = jnp.where(lax.rem(m, 2) == 1, lax.div(m + 1, 2), dp_x - lax.div(m, 2))
        return lax.rem(my_x + off, dp_x) * 2 + lax.rem(my_core + k, 2)

    def remote(src, dst, layer, phase, s_slot, r_slot, axis, target):
        return pltpu.make_async_remote_copy(
            src_ref=src,
            dst_ref=dst,
            send_sem=send_sem.at[layer, phase, s_slot],
            recv_sem=recv_sem.at[layer, phase, r_slot],
            device_id={axis: target},
            device_id_type=MESH,
        )

    fetch = [
        pltpu.make_async_copy(ssm_h, ssm, local_sem.at[0]),
        pltpu.make_async_copy(w_out_h, w_out, local_sem.at[1]),
    ]
    for f in fetch:
        f.start()
    barrier = pltpu.get_barrier_semaphore()

    def greet_tp(k, carry):
        pl.semaphore_signal(barrier, inc=1, device_id={"tp": tp_at(k)}, device_id_type=MESH)
        return carry

    def greet_dp(k, carry):
        pl.semaphore_signal(barrier, inc=1, device_id={"dp": dp_at(k)}, device_id_type=MESH)
        return carry

    lax.fori_loop(1, tp_n, greet_tp, 0)
    lax.fori_loop(1, dp_n, greet_dp, 0)

    heads_all = w_dtt.shape[1]
    pick = lax.broadcasted_iota(jnp.int32, (16, heads_all), 0)
    col = lax.broadcasted_iota(jnp.int32, (16, heads_all), 1)
    pick = jnp.where((pick < heads_here) & (col == pick + my_tp * heads_here), 1.0, 0.0).astype(BF16)
    for l in range(layers):
        w_bcd[l, 0:bw] = w_bt[l]
        w_bcd[l, bw : 2 * bw] = w_ct[l]
        w_bcd[l, 2 * bw : 2 * bw + 16] = jnp.dot(
            pick, w_dtt[l], preferred_element_type=F32
        ).astype(BF16)
        w_bcd[l, 2 * bw + 16 :] = jnp.zeros((w_bcd.shape[1] - 2 * bw - 16, width_f), BF16)
        conv_bc[l] = jnp.concatenate([conv_b[l].astype(F32), conv_c[l].astype(F32)], axis=1)
        for k in range(s_b.shape[1]):
            s_bc[l, k] = jnp.concatenate([s_b[l, k].astype(F32), s_c[l, k].astype(F32)], axis=1)
    for f in fetch:
        f.wait()

    def turn(i, carry):
        for l in range(layers):
            block = ssm[l, i].reshape(zw, bw)
            st_t[l, i] = block.T.astype(BF16)
        return carry

    lax.fori_loop(0, rows, turn, 0)
    r_buf[0] = tok[...]
    pl.semaphore_wait(barrier, tp_n + dp_n - 2)

    lane = lax.broadcasted_iota(jnp.int32, (rows, LANES), 1)
    head_of = lax.broadcasted_iota(jnp.int32, (rows, zw), 1)
    head_of = lax.div(head_of, hd)

    def per_head(v):
        out = jnp.broadcast_to(v[:, 0:1], (rows, zw))
        for h in range(1, heads_here):
            out = jnp.where(head_of == h, v[:, h : h + 1], out)
        return out

    for l in range(layers):
        own_rows = r_buf.at[l]
        a_buf[l, my_tp] = r_buf[l]

        def send_a(n, carry, l=l, own_rows=own_rows):
            k = tp_n - 1 - n
            remote(own_rows, a_buf.at[l, my_tp], l, 0, k, my_tp, "tp", tp_at(k)).start()
            return carry

        lax.fori_loop(0, tp_n - 1, send_a, 0)

        def step_b(k, carry, l=l):
            i = tp_at(k)

            @pl.when(k > 0)
            def _():
                remote(a_buf.at[l, i], a_buf.at[l, i], l, 0, k, i, "tp", i).wait_recv()

            block = a_buf[l, i].astype(F32)
            scaled = (block * gain[l : l + 1].astype(F32)).astype(BF16)
            b_out[l, i, :, 0:zw] = jnp.dot(scaled, w_z[l], preferred_element_type=F32).astype(BF16)
            b_out[l, i, :, zw : 2 * zw] = jnp.dot(
                scaled, w_x[l], preferred_element_type=F32
            ).astype(BF16)
            rest = lax.dot_general(scaled, w_bcd[l], NT, preferred_element_type=F32)
            b_out[l, i, :, 2 * zw : 2 * zw + LANES] = rest[:, 0:LANES].astype(BF16)
            squares = jnp.sum(block * block, axis=1, keepdims=True)
            small = jnp.where(lane == heads_here, squares, rest[:, LANES:])
            low = small - small.astype(BF16).astype(F32)
            both = jnp.where(lane < LANES // 2, small, pltpu.roll(low, LANES // 2, 1))
            b_out[l, i, :, 2 * zw + LANES :] = both.astype(BF16)

            @pl.when(i != my_dp)
            def _():
                remote(b_out.at[l, i], b_in.at[l, my_dp], l, 1, i, my_dp, "dp", i).start()

            return carry

        lax.fori_loop(0, tp_n, step_b, 0)

        def add_b(k, total, l=l):
            i = dp_at(k)
            remote(b_in.at[l, i], b_in.at[l, i], l, 1, i, i, "dp", i).wait_recv()
            return total + b_in[l, i].astype(F32)

        total = lax.fori_loop(1, dp_n, add_b, b_out[l, my_dp].astype(F32))

        small = total[:, 2 * zw + LANES :]
        small = small + pltpu.roll(small, LANES // 2, 1)
        row_scale = lax.rsqrt(small[:, heads_here : heads_here + 1] / features + EPSILON)
        step_raw = small[:, 0:heads_here] * row_scale
        gate = (total[:, 0:zw] * row_scale).astype(BF16).astype(F32)
        x_new = (total[:, zw : 2 * zw] * row_scale).astype(BF16)
        bc_new = (total[:, 2 * zw : 2 * zw + LANES] * row_scale).astype(BF16)
        taps = conv_x.shape[1]
        conv = x_new.astype(F32) * conv_x[l, taps - 1 : taps].astype(F32)
        conv2 = bc_new.astype(F32) * conv_bc[l, taps - 1 : taps]
        for k in range(taps - 1):
            conv = conv + s_x[l, k].astype(F32) * conv_x[l, k : k + 1].astype(F32)
            conv2 = conv2 + s_bc[l, k] * conv_bc[l, k : k + 1]
        v = silu(conv)
        bc = silu(conv2)
        step = jax.nn.softplus(step_raw + dt_bias[l : l + 1])
        decay = jnp.exp(-step * jnp.exp(a_log[l : l + 1]))
        xs = per_head(step) * v
        turned = pltpu.roll(bc, LANES // 2, 1)
        b_dot_c = 0.5 * jnp.sum(bc * turned, axis=1, keepdims=True)
        cc = jnp.where(lane < LANES // 2, turned, bc)
        row = lax.broadcasted_iota(jnp.int32, (rows, LANES), 0)
        pieces = []
        for s in range(0, rows, 2):
            pieces.append(jnp.where(row == s + lax.div(lane, LANES // 2), cc, 0.0).astype(BF16))
        spread = jnp.concatenate(pieces, axis=1)
        reads = jnp.dot(
            spread, st_t[l].reshape(rows * bw, zw), preferred_element_type=F32
        )
        readout = per_head(decay) * reads + (xs * b_dot_c + per_head(d_skip[l : l + 1]) * v)
        gated = readout * silu(gate)
        scale = lax.rsqrt(jnp.mean(gated * gated, axis=1, keepdims=True) + EPSILON)
        mixed = (gated * scale * out_gain[l : l + 1].astype(F32)).astype(BF16)

        c_own[l] = mixed
        c_buf[l, my_dp] = mixed

        def send_c(n, carry, l=l):
            k = dp_n - 1 - n
            remote(c_own.at[l], c_buf.at[l, my_dp], l, 2, k, my_dp, "dp", dp_at(k)).start()
            return carry

        lax.fori_loop(0, dp_n - 1, send_c, 0)

        xs_t = xs.T
        for s in range(rows):
            for h in range(heads_here):
                b_row = bc[s : s + 1, 0:bw]
                column = xs_t[h * hd : (h + 1) * hd, s : s + 1]
                ssm_o[l, s, h] = ssm[l, s, h] * decay[s : s + 1, h : h + 1] + column * b_row
        pltpu.make_async_copy(ssm_o.at[l], ssm_oh.at[l], out_sem.at[l]).start()
        for k in range(taps - 2):
            nx_o[l, k] = s_x[l, k + 1]
            nb_o[l, k] = s_b[l, k + 1]
            nc_o[l, k] = s_c[l, k + 1]
        nx_o[l, taps - 2] = x_new
        nb_o[l, taps - 2] = bc_new[:, 0:bw]
        nc_o[l, taps - 2] = bc_new[:, bw : 2 * bw]

        def step_d(k, carry, l=l):
            i = dp_at(k)

            @pl.when(k > 0)
            def _():
                remote(c_buf.at[l, i], c_buf.at[l, i], l, 2, k, i, "dp", i).wait_recv()

            part = jnp.dot(c_buf[l, i], w_out[l], preferred_element_type=F32)
            d_out[l, i] = part.astype(BF16)

            @pl.when(i != my_tp)
            def _():
                remote(d_out.at[l, i], d_in.at[l, my_tp], l, 3, i, my_tp, "tp", i).start()

            return carry

        lax.fori_loop(0, dp_n, step_d, 0)

        def add_d(k, total, l=l):
            i = tp_at(k)
            remote(d_in.at[l, i], d_in.at[l, i], l, 3, i, i, "tp", i).wait_recv()
            return total + d_in[l, i].astype(F32)

        projected = lax.fori_loop(1, tp_n, add_d, d_out[l, my_tp].astype(F32))
        new = (r_buf[l].astype(F32) + projected).astype(BF16)
        if l + 1 < layers:
            r_buf[l + 1] = new
        else:
            res_o[...] = new

    for l in range(layers):

        def sent_tp(k, carry, l=l):
            i = tp_at(k)
            remote(r_buf.at[l], a_buf.at[l, my_tp], l, 0, k, my_tp, "tp", i).wait_send()
            remote(d_out.at[l, i], d_in.at[l, my_tp], l, 3, i, my_tp, "tp", i).wait_send()
            return carry

        def sent_dp(k, carry, l=l):
            i = dp_at(k)
            remote(b_out.at[l, i], b_in.at[l, my_dp], l, 1, i, my_dp, "dp", i).wait_send()
            remote(c_own.at[l], c_buf.at[l, my_dp], l, 2, k, my_dp, "dp", i).wait_send()
            return carry

        lax.fori_loop(1, tp_n, sent_tp, 0)
        lax.fori_loop(1, dp_n, sent_dp, 0)
        pltpu.make_async_copy(ssm_o.at[l], ssm_oh.at[l], out_sem.at[l]).wait()


def body(tp_n, dp_n, *args):
    (
        tokens,
        norm_gain,
        w_z,
        w_x,
        w_b,
        w_c,
        w_dt,
        conv_x,
        conv_b,
        conv_c,
        dt_bias,
        a_log,
        d_skip,
        out_gain,
        w_out,
        ssm_state,
        state_x,
        state_b,
        state_c,
    ) = args
    layers, heads_here = dt_bias.shape
    rows, width_f = tokens.shape
    zw, bw = w_z.shape[2], w_b.shape[2]
    assert tp_n == dp_n and 2 * bw == LANES
    wide = 2 * zw + 2 * LANES

    def turn(a):
        return jnp.swapaxes(a, 1, 2)

    operands = (
        tokens,
        norm_gain,
        w_z,
        w_x,
        turn(w_b),
        turn(w_c),
        turn(w_dt),
        conv_x,
        conv_b,
        conv_c,
        dt_bias,
        a_log,
        d_skip,
        out_gain,
        w_out,
        ssm_state,
        turn(state_x),
        turn(state_b),
        turn(state_c),
    )
    vmem = pl.BlockSpec(memory_space=pltpu.VMEM)
    hbm = pl.BlockSpec(memory_space=pl.ANY)
    in_specs = [vmem] * 14 + [hbm, hbm] + [vmem] * 3

    def like(a):
        return jax.ShapeDtypeStruct(a.shape, a.dtype)

    residual, ssm_next, next_x, next_b, next_c = pl.pallas_call(
        functools.partial(kernel, tp_n, dp_n, width_f * dp_n),
        out_shape=(
            like(tokens),
            like(ssm_state),
            like(operands[16]),
            like(operands[17]),
            like(operands[18]),
        ),
        in_specs=in_specs,
        out_specs=(vmem, hbm, vmem, vmem, vmem),
        scratch_shapes=[
            pltpu.VMEM((layers, tp_n, rows, width_f), BF16),
            pltpu.VMEM((layers, dp_n, rows, wide), BF16),
            pltpu.VMEM((layers, dp_n, rows, wide), BF16),
            pltpu.VMEM((layers, rows, zw), BF16),
            pltpu.VMEM((layers, dp_n, rows, zw), BF16),
            pltpu.VMEM((layers, tp_n, rows, width_f), BF16),
            pltpu.VMEM((layers, tp_n, rows, width_f), BF16),
            pltpu.VMEM((layers, rows, width_f), BF16),
            pltpu.VMEM((layers, 2 * LANES, width_f), BF16),
            pltpu.VMEM((layers, conv_x.shape[1], LANES), F32),
            pltpu.VMEM((layers, state_b.shape[2], rows, LANES), F32),
            pltpu.VMEM((layers, rows, bw, zw), BF16),
            pltpu.VMEM(w_out.shape, BF16),
            pltpu.VMEM(ssm_state.shape, F32),
            pltpu.VMEM(ssm_state.shape, F32),
            pltpu.SemaphoreType.DMA((2,)),
            pltpu.SemaphoreType.DMA((layers,)),
            pltpu.SemaphoreType.DMA((layers, 4, max(tp_n, dp_n))),
            pltpu.SemaphoreType.DMA((layers, 4, max(tp_n, dp_n))),
        ],
        compiler_params=pltpu.CompilerParams(collective_id=0, has_side_effects=True),
        name="decode",
    )(*operands)
    return residual, ssm_next, turn(next_x), turn(next_b), turn(next_c)


def solution(mesh):
    placed = (
        P(("grp", "tp"), "dp"),
        P(None, "dp"),
        P(None, "dp", "tp"),
        P(None, "dp", "tp"),
        P(None, "dp", "tp"),
        P(None, "dp", "tp"),
        P(None, "dp", None),
        P(None, None, "tp"),
        P(None, None, "tp"),
        P(None, None, "tp"),
        P(None, "tp"),
        P(None, "tp"),
        P(None, "tp"),
        P(None, "tp"),
        P(None, "tp", "dp"),
        P(None, ("grp", "dp"), "tp", None, None),
        P(None, ("grp", "dp"), None, "tp"),
        P(None, ("grp", "dp"), None, "tp"),
        P(None, ("grp", "dp"), None, "tp"),
    )
    return jax.shard_map(
        functools.partial(body, mesh.shape["tp"], mesh.shape["dp"]),
        mesh=mesh,
        in_specs=placed,
        out_specs=(placed[0], placed[15], placed[16], placed[17], placed[18]),
        check_vma=False,
    )
```

```python
import functools

import jax
import jax.numpy as jnp
from jax import lax
from jax.experimental import pallas as pl
from jax.experimental.pallas import tpu as pltpu
from jax.sharding import PartitionSpec as P

EPSILON = 1e-05
F32 = jnp.float32
BF16 = jnp.bfloat16
MESH = pl.DeviceIdType.MESH
NT = (((1,), (1,)), ((), ()))
LANES = 128
INPUTS = 19
GROUP = 4


def silu(v):
    return v * jax.nn.sigmoid(v)


def kernel(
    tp_n,
    dp_n,
    features,
    *refs,
):
    held, refs = refs[:INPUTS], refs[INPUTS:]
    res_o, ssm_o, nx_o, nb_o, nc_o = refs[:5]
    a_buf, b_out, b_in, c_own, c_buf, d_out, d_in, r_buf = refs[5:13]
    w_bcd, conv_bc, s_bc, st_t = refs[13:17]
    here = refs[17 : 16 + INPUTS]
    local_sem, send_sem, recv_sem = refs[16 + INPUTS :]
    (
        gain,
        w_z,
        w_x,
        w_bt,
        w_ct,
        w_dtt,
        conv_x,
        conv_b,
        conv_c,
        dt_bias,
        a_log,
        d_skip,
        out_gain,
        w_out,
        ssm,
        s_x,
        s_b,
        s_c,
    ) = here
    layers, heads_here = dt_bias.shape
    rows, width_f = res_o.shape
    zw = w_z.shape[2]
    bw = w_bt.shape[1]
    hd = zw // heads_here
    my_tp, my_dp = lax.axis_index("tp"), lax.axis_index("dp")
    my_x, my_core = lax.div(my_dp, 2), lax.rem(my_dp, 2)
    dp_x = dp_n // 2

    def tp_at(k):
        off = jnp.where(lax.rem(k, 2) == 1, lax.div(k + 1, 2), tp_n - lax.div(k, 2))
        return lax.rem(my_tp + off, tp_n)

    def dp_at(k):
        m = lax.div(k, 2)
        off = jnp.where(lax.rem(m, 2) == 1, lax.div(m + 1, 2), dp_x - lax.div(m, 2))
        return lax.rem(my_x + off, dp_x) * 2 + lax.rem(my_core + k, 2)

    def mirror(k, n):
        step = jnp.where(lax.rem(k, 2) == 1, k + 1, k - 1)
        return jnp.where((k == n - 1) & (n % 2 == 0), k, jnp.where(k == 0, 0, step))

    def nth(distance, n):
        return jnp.where(distance <= n // 2, jnp.maximum(2 * distance - 1, 0), 2 * (n - distance))

    def mirror_dp(k):
        return 2 * mirror(lax.div(k, 2), dp_x) + lax.rem(k, 2)

    k_rows = nth(lax.rem(my_dp - my_tp + tp_n, tp_n), tp_n)
    k_sums = 2 * nth(lax.rem(lax.div(my_tp, 2) - my_x + dp_x, dp_x), dp_x) + lax.rem(
        my_tp + my_core, 2
    )

    def remote(src, dst, layer, phase, s_slot, r_slot, axis, target):
        return pltpu.make_async_remote_copy(
            src_ref=src,
            dst_ref=dst,
            send_sem=send_sem.at[layer, phase, s_slot],
            recv_sem=recv_sem.at[layer, phase, r_slot],
            device_id={axis: target},
            device_id_type=MESH,
        )

    fetch = [pltpu.make_async_copy(held[0], r_buf.at[0], local_sem.at[0])]
    for n in range(1, INPUTS):
        fetch.append(pltpu.make_async_copy(held[n], here[n - 1], local_sem.at[n]))
    for f in fetch:
        f.start()
    barrier = pltpu.get_barrier_semaphore()

    def greet_tp(k, carry):
        pl.semaphore_signal(barrier, inc=1, device_id={"tp": tp_at(k)}, device_id_type=MESH)
        return carry

    def greet_dp(k, carry):
        pl.semaphore_signal(barrier, inc=1, device_id={"dp": dp_at(k)}, device_id_type=MESH)
        return carry

    lax.fori_loop(1, tp_n, greet_tp, 0)
    lax.fori_loop(1, dp_n, greet_dp, 0)

    for f in fetch:
        f.wait()
    heads_all = w_dtt.shape[1]
    pick = lax.broadcasted_iota(jnp.int32, (16, heads_all), 0)
    col = lax.broadcasted_iota(jnp.int32, (16, heads_all), 1)
    pick = jnp.where((pick < heads_here) & (col == pick + my_tp * heads_here), 1.0, 0.0).astype(BF16)
    for l in range(layers):
        w_bcd[l, 0:bw] = w_bt[l]
        w_bcd[l, bw : 2 * bw] = w_ct[l]
        w_bcd[l, 2 * bw : 2 * bw + 16] = jnp.dot(
            pick, w_dtt[l], preferred_element_type=F32
        ).astype(BF16)
        w_bcd[l, 2 * bw + 16 :] = jnp.zeros((w_bcd.shape[1] - 2 * bw - 16, width_f), BF16)
        conv_bc[l] = jnp.concatenate([conv_b[l].astype(F32), conv_c[l].astype(F32)], axis=1)
        for k in range(s_b.shape[1]):
            s_bc[l, k] = jnp.concatenate([s_b[l, k].astype(F32), s_c[l, k].astype(F32)], axis=1)

    def turn(i, carry):
        for l in range(layers):
            block = ssm[l, i].reshape(zw, bw)
            st_t[l, i] = block.T.astype(BF16)
        return carry

    lax.fori_loop(0, rows, turn, 0)
    pl.semaphore_wait(barrier, tp_n + dp_n - 2)

    lane_tall = lax.broadcasted_iota(jnp.int32, (GROUP * rows, LANES), 1)
    lane = lax.broadcasted_iota(jnp.int32, (rows, LANES), 1)
    head_of = lax.broadcasted_iota(jnp.int32, (rows, zw), 1)
    head_of = lax.div(head_of, hd)

    def per_head(v):
        out = jnp.broadcast_to(v[:, 0:1], (rows, zw))
        for h in range(1, heads_here):
            out = jnp.where(head_of == h, v[:, h : h + 1], out)
        return out

    for l in range(layers):
        a_buf[l, 0] = r_buf[l]

        def send_a(n, carry, l=l):
            k = tp_n - 1 - n
            slot = mirror(k, tp_n)
            remote(r_buf.at[l], a_buf.at[l, slot], l, 0, k, slot, "tp", tp_at(k)).start()
            return carry

        lax.fori_loop(0, tp_n - 1, send_a, 0)

        for first in range(0, tp_n, GROUP):
            for k in range(max(first, 1), first + GROUP):
                remote(a_buf.at[l, k], a_buf.at[l, k], l, 0, k, k, "tp", tp_at(k)).wait_recv()
            tall = GROUP * rows
            block = a_buf[l, first : first + GROUP].reshape(tall, width_f).astype(F32)
            scaled = (block * gain[l : l + 1].astype(F32)).astype(BF16)
            part_z = jnp.dot(scaled, w_z[l], preferred_element_type=F32).astype(BF16)
            part_x = jnp.dot(scaled, w_x[l], preferred_element_type=F32).astype(BF16)
            rest = lax.dot_general(scaled, w_bcd[l], NT, preferred_element_type=F32)
            squares = jnp.sum(block * block, axis=1, keepdims=True)
            small = jnp.where(lane_tall == heads_here, squares, rest[:, LANES:])
            low = small - small.astype(BF16).astype(F32)
            both = jnp.where(lane_tall < LANES // 2, small, pltpu.roll(low, LANES // 2, 1))
            b_out[l, first : first + GROUP, :, 0:zw] = part_z.reshape(GROUP, rows, zw)
            b_out[l, first : first + GROUP, :, zw : 2 * zw] = part_x.reshape(GROUP, rows, zw)
            b_out[l, first : first + GROUP, :, 2 * zw : 2 * zw + LANES] = (
                rest[:, 0:LANES].astype(BF16).reshape(GROUP, rows, LANES)
            )
            b_out[l, first : first + GROUP, :, 2 * zw + LANES :] = both.astype(BF16).reshape(
                GROUP, rows, LANES
            )
            for k in range(first, first + GROUP):
                i = tp_at(k)

                @pl.when(i != my_dp)
                def _(k=k, i=i):
                    remote(b_out.at[l, k], b_in.at[l, my_dp], l, 1, k, my_dp, "dp", i).start()

        def add_b(k, total, l=l):
            i = dp_at(k)
            remote(b_in.at[l, i], b_in.at[l, i], l, 1, k, i, "dp", i).wait_recv()
            return total + b_in[l, i].astype(F32)

        total = lax.fori_loop(1, dp_n, add_b, b_out[l, k_rows].astype(F32))

        small = total[:, 2 * zw + LANES :]
        small = small + pltpu.roll(small, LANES // 2, 1)
        row_scale = lax.rsqrt(small[:, heads_here : heads_here + 1] / features + EPSILON)
        step_raw = small[:, 0:heads_here] * row_scale
        gate = (total[:, 0:zw] * row_scale).astype(BF16).astype(F32)
        x_new = (total[:, zw : 2 * zw] * row_scale).astype(BF16)
        bc_new = (total[:, 2 * zw : 2 * zw + LANES] * row_scale).astype(BF16)
        taps = conv_x.shape[1]
        conv = x_new.astype(F32) * conv_x[l, taps - 1 : taps].astype(F32)
        conv2 = bc_new.astype(F32) * conv_bc[l, taps - 1 : taps]
        for k in range(taps - 1):
            conv = conv + s_x[l, k].astype(F32) * conv_x[l, k : k + 1].astype(F32)
            conv2 = conv2 + s_bc[l, k] * conv_bc[l, k : k + 1]
        v = silu(conv)
        bc = silu(conv2)
        step = jax.nn.softplus(step_raw + dt_bias[l : l + 1])
        decay = jnp.exp(-step * jnp.exp(a_log[l : l + 1]))
        xs = per_head(step) * v
        turned = pltpu.roll(bc, LANES // 2, 1)
        b_dot_c = 0.5 * jnp.sum(bc * turned, axis=1, keepdims=True)
        cc = jnp.where(lane < LANES // 2, turned, bc)
        row = lax.broadcasted_iota(jnp.int32, (rows, LANES), 0)
        pieces = []
        for s in range(0, rows, 2):
            pieces.append(jnp.where(row == s + lax.div(lane, LANES // 2), cc, 0.0).astype(BF16))
        spread = jnp.concatenate(pieces, axis=1)
        reads = jnp.dot(
            spread, st_t[l].reshape(rows * bw, zw), preferred_element_type=F32
        )
        readout = per_head(decay) * reads + (xs * b_dot_c + per_head(d_skip[l : l + 1]) * v)
        gated = readout * silu(gate)
        scale = lax.rsqrt(jnp.mean(gated * gated, axis=1, keepdims=True) + EPSILON)
        mixed = (gated * scale * out_gain[l : l + 1].astype(F32)).astype(BF16)

        c_own[l] = mixed
        c_buf[l, 0] = mixed

        def send_c(n, carry, l=l):
            k = dp_n - 1 - n
            slot = mirror_dp(k)
            remote(c_own.at[l], c_buf.at[l, slot], l, 2, k, slot, "dp", dp_at(k)).start()
            return carry

        lax.fori_loop(0, dp_n - 1, send_c, 0)

        for first in range(0, dp_n, GROUP):
            for k in range(max(first, 1), first + GROUP):
                remote(c_buf.at[l, k], c_buf.at[l, k], l, 2, k, k, "dp", dp_at(k)).wait_recv()
            block = c_buf[l, first : first + GROUP].reshape(GROUP * rows, zw)
            part = jnp.dot(block, w_out[l], preferred_element_type=F32).astype(BF16)
            d_out[l, first : first + GROUP] = part.reshape(GROUP, rows, width_f)
            for k in range(first, first + GROUP):
                i = dp_at(k)

                @pl.when(i != my_tp)
                def _(k=k, i=i):
                    remote(d_out.at[l, k], d_in.at[l, my_tp], l, 3, k, my_tp, "tp", i).start()

        xs_t = xs.T
        for s in range(rows):
            for h in range(heads_here):
                b_row = bc[s : s + 1, 0:bw]
                column = xs_t[h * hd : (h + 1) * hd, s : s + 1]
                ssm_o[l, s, h] = ssm[l, s, h] * decay[s : s + 1, h : h + 1] + column * b_row
        for k in range(taps - 2):
            nx_o[l, k] = s_x[l, k + 1]
            nb_o[l, k] = s_b[l, k + 1]
            nc_o[l, k] = s_c[l, k + 1]
        nx_o[l, taps - 2] = x_new
        nb_o[l, taps - 2] = bc_new[:, 0:bw]
        nc_o[l, taps - 2] = bc_new[:, bw : 2 * bw]

        def add_d(k, total, l=l):
            i = tp_at(k)
            remote(d_in.at[l, i], d_in.at[l, i], l, 3, k, i, "tp", i).wait_recv()
            return total + d_in[l, i].astype(F32)

        projected = lax.fori_loop(1, tp_n, add_d, d_out[l, k_sums].astype(F32))
        new = (r_buf[l].astype(F32) + projected).astype(BF16)
        if l + 1 < layers:
            r_buf[l + 1] = new
        else:
            res_o[...] = new

    for l in range(layers):

        def sent(k, carry, l=l):
            i, j = tp_at(k), dp_at(k)
            remote(r_buf.at[l], a_buf.at[l, 0], l, 0, k, 0, "tp", i).wait_send()
            remote(c_own.at[l], c_buf.at[l, 0], l, 2, k, 0, "dp", j).wait_send()
            return carry

        def sent_parts(k, carry, l=l):
            i, j = tp_at(k), dp_at(k)

            @pl.when(i != my_dp)
            def _():
                remote(b_out.at[l, k], b_in.at[l, my_dp], l, 1, k, my_dp, "dp", i).wait_send()

            @pl.when(j != my_tp)
            def _():
                remote(d_out.at[l, k], d_in.at[l, my_tp], l, 3, k, my_tp, "tp", j).wait_send()

            return carry

        lax.fori_loop(1, tp_n, sent, 0)
        lax.fori_loop(0, tp_n, sent_parts, 0)


def write_out(*refs):
    sem = refs[-1]
    half = len(refs) // 2
    copies = [
        pltpu.make_async_copy(refs[n], refs[half + n], sem.at[n]) for n in range(half)
    ]
    for c in copies:
        c.start()
    for c in copies:
        c.wait()


def body(tp_n, dp_n, *args):
    (
        tokens,
        norm_gain,
        w_z,
        w_x,
        w_b,
        w_c,
        w_dt,
        conv_x,
        conv_b,
        conv_c,
        dt_bias,
        a_log,
        d_skip,
        out_gain,
        w_out,
        ssm_state,
        state_x,
        state_b,
        state_c,
    ) = args
    layers, heads_here = dt_bias.shape
    rows, width_f = tokens.shape
    zw, bw = w_z.shape[2], w_b.shape[2]
    assert tp_n == dp_n and 2 * bw == LANES
    wide = 2 * zw + 2 * LANES

    def turn(a):
        return jnp.swapaxes(a, 1, 2)

    operands = (
        tokens,
        norm_gain,
        w_z,
        w_x,
        turn(w_b),
        turn(w_c),
        turn(w_dt),
        conv_x,
        conv_b,
        conv_c,
        dt_bias,
        a_log,
        d_skip,
        out_gain,
        w_out,
        ssm_state,
        turn(state_x),
        turn(state_b),
        turn(state_c),
    )
    vmem = pl.BlockSpec(memory_space=pltpu.VMEM)
    hbm = pl.BlockSpec(memory_space=pltpu.HBM)

    def like(a):
        return pltpu.VMEM(a.shape, a.dtype)

    results = pl.pallas_call(
        functools.partial(kernel, tp_n, dp_n, width_f * dp_n),
        out_shape=(
            like(tokens),
            like(ssm_state),
            like(operands[16]),
            like(operands[17]),
            like(operands[18]),
        ),
        in_specs=[hbm] * INPUTS,
        out_specs=(vmem,) * 5,
        scratch_shapes=[
            pltpu.VMEM((layers, tp_n, rows, width_f), BF16),
            pltpu.VMEM((layers, dp_n, rows, wide), BF16),
            pltpu.VMEM((layers, dp_n, rows, wide), BF16),
            pltpu.VMEM((layers, rows, zw), BF16),
            pltpu.VMEM((layers, dp_n, rows, zw), BF16),
            pltpu.VMEM((layers, tp_n, rows, width_f), BF16),
            pltpu.VMEM((layers, tp_n, rows, width_f), BF16),
            pltpu.VMEM((layers, rows, width_f), BF16),
            pltpu.VMEM((layers, 2 * LANES, width_f), BF16),
            pltpu.VMEM((layers, conv_x.shape[1], LANES), F32),
            pltpu.VMEM((layers, state_b.shape[2], rows, LANES), F32),
            pltpu.VMEM((layers, rows, bw, zw), BF16),
            *(pltpu.VMEM(a.shape, a.dtype) for a in operands[1:]),
            pltpu.SemaphoreType.DMA((INPUTS,)),
            pltpu.SemaphoreType.DMA((layers, 4, max(tp_n, dp_n))),
            pltpu.SemaphoreType.DMA((layers, 4, max(tp_n, dp_n))),
        ],
        compiler_params=pltpu.CompilerParams(
            collective_id=0, has_side_effects=True, vmem_limit_bytes=40 * 1024 * 1024
        ),
        name="decode",
    )(*(pltpu.with_memory_space_constraint(a, pltpu.HBM) for a in operands))
    results = [pltpu.with_memory_space_constraint(a, pltpu.VMEM) for a in results]
    residual, ssm_next, next_x, next_b, next_c = pl.pallas_call(
        write_out,
        out_shape=tuple(jax.ShapeDtypeStruct(a.shape, a.dtype) for a in results),
        in_specs=(vmem,) * 5,
        out_specs=(hbm,) * 5,
        scratch_shapes=[pltpu.SemaphoreType.DMA((5,))],
        compiler_params=pltpu.CompilerParams(vmem_limit_bytes=8 * 1024 * 1024),
        name="write_out",
    )(*results)
    return residual, ssm_next, turn(next_x), turn(next_b), turn(next_c)


def solution(mesh):
    placed = (
        P(("grp", "tp"), "dp"),
        P(None, "dp"),
        P(None, "dp", "tp"),
        P(None, "dp", "tp"),
        P(None, "dp", "tp"),
        P(None, "dp", "tp"),
        P(None, "dp", None),
        P(None, None, "tp"),
        P(None, None, "tp"),
        P(None, None, "tp"),
        P(None, "tp"),
        P(None, "tp"),
        P(None, "tp"),
        P(None, "tp"),
        P(None, "tp", "dp"),
        P(None, ("grp", "dp"), "tp", None, None),
        P(None, ("grp", "dp"), None, "tp"),
        P(None, ("grp", "dp"), None, "tp"),
        P(None, ("grp", "dp"), None, "tp"),
    )
    return jax.shard_map(
        functools.partial(body, mesh.shape["tp"], mesh.shape["dp"]),
        mesh=mesh,
        in_specs=placed,
        out_specs=(placed[0], placed[15], placed[16], placed[17], placed[18]),
        check_vma=False,
    )
```

```python
import functools

import jax
import jax.numpy as jnp
from jax import lax
from jax.experimental import pallas as pl
from jax.experimental.pallas import tpu as pltpu
from jax.sharding import PartitionSpec as P

EPSILON = 1e-05
F32 = jnp.float32
BF16 = jnp.bfloat16
MESH = pl.DeviceIdType.MESH
NT = (((1,), (1,)), ((), ()))
LANES = 128
INPUTS = 19
GROUP = 4


def silu(v):
    return v * jax.nn.sigmoid(v)


def kernel(
    tp_n,
    dp_n,
    features,
    *refs,
):
    held, refs = refs[:INPUTS], refs[INPUTS:]
    res_o, ssm_o, nx_o, nb_o, nc_o = refs[:5]
    a_buf, b_out, b_in, c_own, c_buf, d_out, d_in, r_buf = refs[5:13]
    w_z, w_x, w_out, w_bcd, gains, conv_bc, s_bc, st_t = refs[13:21]
    here = refs[21 : 17 + INPUTS]
    local_sem, pair_sem, send_sem, recv_sem = refs[17 + INPUTS :]
    (
        gain,
        w_bt,
        w_ct,
        w_dtt,
        conv_x,
        conv_b,
        conv_c,
        dt_bias,
        a_log,
        d_skip,
        out_gain,
        ssm,
        s_x,
        s_b,
        s_c,
    ) = here
    layers, heads_here = dt_bias.shape
    rows, width_f = res_o.shape
    zw = w_z.shape[3]
    bw = w_bt.shape[1]
    hd = zw // heads_here
    my_tp, my_dp = lax.axis_index("tp"), lax.axis_index("dp")
    my_x, my_core = lax.div(my_dp, 2), lax.rem(my_dp, 2)
    half = tp_n // 2
    uneven = lax.rem(my_tp + my_core, 2) == 1
    row_core = lax.rem(my_tp, 2)

    def nearest(k, n):
        return jnp.where(lax.rem(k, 2) == 1, lax.div(k + 1, 2), lax.rem(n - lax.div(k, 2), n))

    def place(distance, n):
        return jnp.where(distance <= n // 2, jnp.maximum(2 * distance - 1, 0), 2 * (n - distance))

    def tp_at(k):
        return lax.rem(my_tp + nearest(k, tp_n), tp_n)

    def x_at(k):
        return lax.rem(my_x + nearest(k, half), half)

    def rows_at(k):
        odd = jnp.where(lax.rem(k, 2) == 0, k + 1, tp_n - k)
        return lax.rem(my_tp + jnp.where(uneven, odd, 2 * nearest(k, half)), tp_n)

    def rows_place(offset):
        odd = jnp.where(offset < half, offset - 1, tp_n - offset)
        return jnp.where(lax.rem(offset, 2) == 1, odd, place(lax.div(offset, 2), half))

    def x_mirror(k):
        step = jnp.where(lax.rem(k, 2) == 1, k + 1, k - 1)
        return jnp.where((k == half - 1) & (half % 2 == 0), k, jnp.where(k == 0, 0, step))

    k_rows = rows_place(lax.rem(my_dp - my_tp + tp_n, tp_n))

    def remote(src, dst, layer, phase, s_slot, r_slot, target):
        return pltpu.make_async_remote_copy(
            src_ref=src,
            dst_ref=dst,
            send_sem=send_sem.at[layer, phase, s_slot],
            recv_sem=recv_sem.at[layer, phase, r_slot],
            device_id=target,
            device_id_type=MESH,
        )

    def column(z, core):
        return {"tp": z, "dp": 2 * my_x + core}

    def row(x):
        return {"dp": 2 * x + my_core}

    layer_list = range(layers)
    fetch = [pltpu.make_async_copy(held[0], r_buf.at[0], local_sem.at[0])]
    used = 1
    for n in range(3):
        whole = (w_z, w_x, w_out)[n]
        for l in layer_list:
            fetch.append(
                pltpu.make_async_copy(
                    held[1 + n].at[l], whole.at[l, my_core], local_sem.at[used]
                )
            )
            used += 1
    for n in range(4, INPUTS):
        fetch.append(pltpu.make_async_copy(held[n], here[n - 4], local_sem.at[used]))
        used += 1
    for f in fetch:
        f.start()
    barrier = pltpu.get_barrier_semaphore()

    def greet(device):
        pl.semaphore_signal(barrier, inc=1, device_id=device, device_id_type=MESH)

    def greet_tp(k, carry):
        greet(column(tp_at(k), 0))
        greet(column(tp_at(k), 1))
        return carry

    def greet_dp(k, carry):
        greet(row(x_at(k)))
        return carry

    greet(column(my_tp, 1 - my_core))
    lax.fori_loop(1, tp_n, greet_tp, 0)
    lax.fori_loop(1, half, greet_dp, 0)

    for f in fetch:
        f.wait()
    heads_all = w_dtt.shape[1]
    pick = lax.broadcasted_iota(jnp.int32, (16, heads_all), 0)
    col = lax.broadcasted_iota(jnp.int32, (16, heads_all), 1)
    pick = jnp.where((pick < heads_here) & (col == pick + my_tp * heads_here), 1.0, 0.0).astype(BF16)
    for l in range(layers):
        w_bcd[l, my_core, 0:bw] = w_bt[l]
        w_bcd[l, my_core, bw : 2 * bw] = w_ct[l]
        w_bcd[l, my_core, 2 * bw : 2 * bw + 16] = jnp.dot(
            pick, w_dtt[l], preferred_element_type=F32
        ).astype(BF16)
        w_bcd[l, my_core, 2 * bw + 16 :] = jnp.zeros(
            (w_bcd.shape[2] - 2 * bw - 16, width_f), BF16
        )
        conv_bc[l] = jnp.concatenate([conv_b[l].astype(F32), conv_c[l].astype(F32)], axis=1)
        for k in range(s_b.shape[1]):
            s_bc[l, k] = jnp.concatenate([s_b[l, k].astype(F32), s_c[l, k].astype(F32)], axis=1)

    gains[my_core] = jnp.zeros(gains.shape[1:], F32)
    gains[my_core, 0:layers] = gain[...].astype(F32)

    def turn(i, carry):
        for l in range(layers):
            block = ssm[l, i].reshape(zw, bw)
            st_t[l, i] = block.T.astype(BF16)
        return carry

    lax.fori_loop(0, rows, turn, 0)
    pl.semaphore_wait(barrier, 2 * tp_n - 1 + half - 1)

    pair = []
    for whole in [gains.at[my_core]] + [
        w.at[l, my_core] for l in layer_list for w in (w_z, w_x, w_bcd, w_out)
    ]:
        pair.append(
            pltpu.make_async_remote_copy(
                src_ref=whole,
                dst_ref=whole,
                send_sem=pair_sem.at[0, len(pair)],
                recv_sem=pair_sem.at[1, len(pair)],
                device_id=column(my_tp, 1 - my_core),
                device_id_type=MESH,
            )
        )

    lane = lax.broadcasted_iota(jnp.int32, (rows, LANES), 1)
    head_of = lax.broadcasted_iota(jnp.int32, (rows, zw), 1)
    head_of = lax.div(head_of, hd)

    def per_head(v):
        out = jnp.broadcast_to(v[:, 0:1], (rows, zw))
        for h in range(1, heads_here):
            out = jnp.where(head_of == h, v[:, h : h + 1], out)
        return out

    for l in range(layers):
        def send_a(n, carry, l=l):
            k = tp_n - 1 - n
            z = tp_at(k)
            slot = 2 * rows_place(lax.rem(my_tp - z + tp_n, tp_n)) + my_core
            dst = a_buf.at[l, lax.div(slot, 2), my_core]
            remote(r_buf.at[l], dst, l, 0, k, slot, column(z, row_core)).start()
            return carry

        lax.fori_loop(0, tp_n - 1, send_a, 0)

        @pl.when(uneven)
        def _(l=l):
            dst = a_buf.at[l, 0, my_core]
            remote(r_buf.at[l], dst, l, 0, 0, my_core, column(my_tp, row_core)).start()

        @pl.when(jnp.logical_not(uneven))
        def _(l=l):
            a_buf[l, 0, my_core] = r_buf[l]

        if l == 0:
            for p in pair:
                p.start()

        for first in range(0, half, GROUP):
            group = min(GROUP, half)
            for k in range(first, first + group):
                for core in range(2):
                    got = a_buf.at[l, k, core]
                    copy = remote(got, got, l, 0, k, 2 * k + core, column(rows_at(k), core))
                    if k > 0:
                        copy.wait_recv()
                    else:

                        @pl.when(uneven | (my_core != core))
                        def _(copy=copy):
                            copy.wait_recv()

            if l == 0 and first == 0:
                for p in pair:
                    p.wait_recv()
            tall = group * rows
            scaled, squares = [], 0.0
            for core in range(2):
                block = a_buf[l, first : first + group, core].reshape(tall, width_f).astype(F32)
                scaled.append((block * gains[core, l : l + 1]).astype(BF16))
                squares = squares + jnp.sum(block * block, axis=1, keepdims=True)
            both_wide = jnp.concatenate(scaled, axis=1)
            part_z = jnp.dot(
                both_wide, w_z[l].reshape(2 * width_f, zw), preferred_element_type=F32
            ).astype(BF16)
            part_x = jnp.dot(
                both_wide, w_x[l].reshape(2 * width_f, zw), preferred_element_type=F32
            ).astype(BF16)
            rest = lax.dot_general(scaled[0], w_bcd[l, 0], NT, preferred_element_type=F32)
            rest += lax.dot_general(scaled[1], w_bcd[l, 1], NT, preferred_element_type=F32)
            lane_tall = lax.broadcasted_iota(jnp.int32, (tall, LANES), 1)
            small = jnp.where(lane_tall == heads_here, squares, rest[:, LANES:])
            low = small - small.astype(BF16).astype(F32)
            both = jnp.where(lane_tall < LANES // 2, small, pltpu.roll(low, LANES // 2, 1))
            b_out[l, first : first + group, :, 0:zw] = part_z.reshape(group, rows, zw)
            b_out[l, first : first + group, :, zw : 2 * zw] = part_x.reshape(group, rows, zw)
            b_out[l, first : first + group, :, 2 * zw : 2 * zw + LANES] = (
                rest[:, 0:LANES].astype(BF16).reshape(group, rows, LANES)
            )
            b_out[l, first : first + group, :, 2 * zw + LANES :] = both.astype(BF16).reshape(
                group, rows, LANES
            )
            for k in range(first, first + group):
                i = rows_at(k)

                @pl.when(i != my_dp)
                def _(k=k, i=i):
                    dst = b_in.at[l, my_x]
                    remote(b_out.at[l, k], dst, l, 1, k, my_x, row(lax.div(i, 2))).start()

        def add_b(k, total, l=l):
            x = x_at(k)
            remote(b_in.at[l, x], b_in.at[l, x], l, 1, k, x, row(x)).wait_recv()
            return total + b_in[l, x].astype(F32)

        total = lax.fori_loop(1, half, add_b, b_out[l, k_rows].astype(F32))

        small = total[:, 2 * zw + LANES :]
        small = small + pltpu.roll(small, LANES // 2, 1)
        row_scale = lax.rsqrt(small[:, heads_here : heads_here + 1] / features + EPSILON)
        step_raw = small[:, 0:heads_here] * row_scale
        gate = (total[:, 0:zw] * row_scale).astype(BF16).astype(F32)
        x_new = (total[:, zw : 2 * zw] * row_scale).astype(BF16)
        bc_new = (total[:, 2 * zw : 2 * zw + LANES] * row_scale).astype(BF16)
        taps = conv_x.shape[1]
        conv = x_new.astype(F32) * conv_x[l, taps - 1 : taps].astype(F32)
        conv2 = bc_new.astype(F32) * conv_bc[l, taps - 1 : taps]
        for k in range(taps - 1):
            conv = conv + s_x[l, k].astype(F32) * conv_x[l, k : k + 1].astype(F32)
            conv2 = conv2 + s_bc[l, k] * conv_bc[l, k : k + 1]
        v = silu(conv)
        bc = silu(conv2)
        step = jax.nn.softplus(step_raw + dt_bias[l : l + 1])
        decay = jnp.exp(-step * jnp.exp(a_log[l : l + 1]))
        xs = per_head(step) * v
        turned = pltpu.roll(bc, LANES // 2, 1)
        b_dot_c = 0.5 * jnp.sum(bc * turned, axis=1, keepdims=True)
        cc = jnp.where(lane < LANES // 2, turned, bc)
        seq = lax.broadcasted_iota(jnp.int32, (rows, LANES), 0)
        pieces = []
        for s in range(0, rows, 2):
            pieces.append(jnp.where(seq == s + lax.div(lane, LANES // 2), cc, 0.0).astype(BF16))
        spread = jnp.concatenate(pieces, axis=1)
        reads = jnp.dot(
            spread, st_t[l].reshape(rows * bw, zw), preferred_element_type=F32
        )
        readout = per_head(decay) * reads + (xs * b_dot_c + per_head(d_skip[l : l + 1]) * v)
        gated = readout * silu(gate)
        scale = lax.rsqrt(jnp.mean(gated * gated, axis=1, keepdims=True) + EPSILON)
        mixed = (gated * scale * out_gain[l : l + 1].astype(F32)).astype(BF16)

        c_own[l] = mixed
        c_buf[l, 0] = mixed

        def send_c(n, carry, l=l):
            k = half - 1 - n
            slot = x_mirror(k)
            remote(c_own.at[l], c_buf.at[l, slot], l, 2, k, slot, row(x_at(k))).start()
            return carry

        lax.fori_loop(0, half - 1, send_c, 0)

        for first in range(0, half, GROUP):
            group = min(GROUP, half)
            for k in range(max(first, 1), first + group):
                got = c_buf.at[l, k]
                remote(got, got, l, 2, k, k, row(x_at(k))).wait_recv()
            block = c_buf[l, first : first + group].reshape(group * rows, zw)
            for core in range(2):
                part = jnp.dot(block, w_out[l, core], preferred_element_type=F32).astype(BF16)
                d_out[l, first : first + group, core] = part.reshape(group, rows, width_f)
            for k in range(first, first + group):
                z = 2 * x_at(k) + my_core
                for core in range(2):
                    mine = (z == my_tp) & (my_core == core)

                    @pl.when(jnp.logical_not(mine))
                    def _(k=k, z=z, core=core):
                        src, dst = d_out.at[l, k, core], d_in.at[l, my_tp]
                        remote(src, dst, l, 3, 2 * k + core, my_tp, column(z, core)).start()

                    @pl.when(mine)
                    def _(k=k, core=core):
                        d_in[l, my_tp] = d_out[l, k, core]

        xs_t = xs.T
        for s in range(rows):
            for h in range(heads_here):
                b_row = bc[s : s + 1, 0:bw]
                xs_col = xs_t[h * hd : (h + 1) * hd, s : s + 1]
                ssm_o[l, s, h] = ssm[l, s, h] * decay[s : s + 1, h : h + 1] + xs_col * b_row
        for k in range(taps - 2):
            nx_o[l, k] = s_x[l, k + 1]
            nb_o[l, k] = s_b[l, k + 1]
            nc_o[l, k] = s_c[l, k + 1]
        nx_o[l, taps - 2] = x_new
        nb_o[l, taps - 2] = bc_new[:, 0:bw]
        nc_o[l, taps - 2] = bc_new[:, bw : 2 * bw]

        def add_d(k, total, l=l):
            z = tp_at(k)
            got = d_in.at[l, z]
            remote(got, got, l, 3, k, z, column(z, row_core)).wait_recv()
            return total + d_in[l, z].astype(F32)

        @pl.when(uneven)
        def _(l=l):
            got = d_in.at[l, my_tp]
            remote(got, got, l, 3, 0, my_tp, column(my_tp, row_core)).wait_recv()

        projected = lax.fori_loop(1, tp_n, add_d, d_in[l, my_tp].astype(F32))
        new = (r_buf[l].astype(F32) + projected).astype(BF16)
        if l + 1 < layers:
            r_buf[l + 1] = new
        else:
            res_o[...] = new

    for l in range(layers):

        def sent_a(k, carry, l=l):
            dst = a_buf.at[l, 0, my_core]
            remote(r_buf.at[l], dst, l, 0, k, 0, column(tp_at(k), row_core)).wait_send()
            return carry

        def sent_c(k, carry, l=l):
            remote(c_own.at[l], c_buf.at[l, 0], l, 2, k, 0, row(x_at(k))).wait_send()
            return carry

        def sent_parts(k, carry, l=l):
            i = rows_at(k)
            z = 2 * x_at(k) + my_core

            @pl.when(i != my_dp)
            def _():
                dst = b_in.at[l, my_x]
                remote(b_out.at[l, k], dst, l, 1, k, my_x, row(lax.div(i, 2))).wait_send()

            for core in range(2):

                @pl.when(jnp.logical_not((z == my_tp) & (my_core == core)))
                def _(core=core):
                    src, dst = d_out.at[l, k, core], d_in.at[l, my_tp]
                    remote(src, dst, l, 3, 2 * k + core, my_tp, column(z, core)).wait_send()

            return carry

        lax.fori_loop(1, tp_n, sent_a, 0)

        @pl.when(uneven)
        def _(l=l):
            dst = a_buf.at[l, 0, my_core]
            remote(r_buf.at[l], dst, l, 0, 0, my_core, column(my_tp, row_core)).wait_send()

        lax.fori_loop(1, half, sent_c, 0)
        lax.fori_loop(0, half, sent_parts, 0)
    for p in pair:
        p.wait_send()


def write_out(*refs):
    sem = refs[-1]
    half = len(refs) // 2
    copies = [
        pltpu.make_async_copy(refs[n], refs[half + n], sem.at[n]) for n in range(half)
    ]
    for c in copies:
        c.start()
    for c in copies:
        c.wait()


def body(tp_n, dp_n, *args):
    (
        tokens,
        norm_gain,
        w_z,
        w_x,
        w_b,
        w_c,
        w_dt,
        conv_x,
        conv_b,
        conv_c,
        dt_bias,
        a_log,
        d_skip,
        out_gain,
        w_out,
        ssm_state,
        state_x,
        state_b,
        state_c,
    ) = args
    layers, heads_here = dt_bias.shape
    rows, width_f = tokens.shape
    zw, bw = w_z.shape[2], w_b.shape[2]
    assert tp_n == dp_n and 2 * bw == LANES
    wide = 2 * zw + 2 * LANES
    half = tp_n // 2

    def turn(a):
        return jnp.swapaxes(a, 1, 2)

    operands = (
        tokens,
        w_z,
        w_x,
        w_out,
        norm_gain,
        turn(w_b),
        turn(w_c),
        turn(w_dt),
        conv_x,
        conv_b,
        conv_c,
        dt_bias,
        a_log,
        d_skip,
        out_gain,
        ssm_state,
        turn(state_x),
        turn(state_b),
        turn(state_c),
    )
    vmem = pl.BlockSpec(memory_space=pltpu.VMEM)
    hbm = pl.BlockSpec(memory_space=pltpu.HBM)

    def like(a):
        return pltpu.VMEM(a.shape, a.dtype)

    results = pl.pallas_call(
        functools.partial(kernel, tp_n, dp_n, width_f * dp_n),
        out_shape=(
            like(tokens),
            like(ssm_state),
            like(operands[16]),
            like(operands[17]),
            like(operands[18]),
        ),
        in_specs=[hbm] * INPUTS,
        out_specs=(vmem,) * 5,
        scratch_shapes=[
            pltpu.VMEM((layers, half, 2, rows, width_f), BF16),
            pltpu.VMEM((layers, half, rows, wide), BF16),
            pltpu.VMEM((layers, half, rows, wide), BF16),
            pltpu.VMEM((layers, rows, zw), BF16),
            pltpu.VMEM((layers, half, rows, zw), BF16),
            pltpu.VMEM((layers, half, 2, rows, width_f), BF16),
            pltpu.VMEM((layers, tp_n, rows, width_f), BF16),
            pltpu.VMEM((layers, rows, width_f), BF16),
            pltpu.VMEM((layers, 2, width_f, zw), BF16),
            pltpu.VMEM((layers, 2, width_f, zw), BF16),
            pltpu.VMEM((layers, 2, zw, width_f), BF16),
            pltpu.VMEM((layers, 2, 2 * LANES, width_f), BF16),
            pltpu.VMEM((2, 8, width_f), F32),
            pltpu.VMEM((layers, conv_x.shape[1], LANES), F32),
            pltpu.VMEM((layers, state_b.shape[2], rows, LANES), F32),
            pltpu.VMEM((layers, rows, bw, zw), BF16),
            *(pltpu.VMEM(a.shape, a.dtype) for a in operands[4:]),
            pltpu.SemaphoreType.DMA((INPUTS - 3 + 3 * layers,)),
            pltpu.SemaphoreType.DMA((2, 1 + 4 * layers)),
            pltpu.SemaphoreType.DMA((layers, 4, tp_n)),
            pltpu.SemaphoreType.DMA((layers, 4, tp_n)),
        ],
        compiler_params=pltpu.CompilerParams(
            collective_id=0, has_side_effects=True, vmem_limit_bytes=40 * 1024 * 1024
        ),
        name="decode",
    )(*(pltpu.with_memory_space_constraint(a, pltpu.HBM) for a in operands))
    results = [pltpu.with_memory_space_constraint(a, pltpu.VMEM) for a in results]
    residual, ssm_next, next_x, next_b, next_c = pl.pallas_call(
        write_out,
        out_shape=tuple(jax.ShapeDtypeStruct(a.shape, a.dtype) for a in results),
        in_specs=(vmem,) * 5,
        out_specs=(hbm,) * 5,
        scratch_shapes=[pltpu.SemaphoreType.DMA((5,))],
        compiler_params=pltpu.CompilerParams(vmem_limit_bytes=8 * 1024 * 1024),
        name="write_out",
    )(*results)
    return residual, ssm_next, turn(next_x), turn(next_b), turn(next_c)


def solution(mesh):
    placed = (
        P(("grp", "tp"), "dp"),
        P(None, "dp"),
        P(None, "dp", "tp"),
        P(None, "dp", "tp"),
        P(None, "dp", "tp"),
        P(None, "dp", "tp"),
        P(None, "dp", None),
        P(None, None, "tp"),
        P(None, None, "tp"),
        P(None, None, "tp"),
        P(None, "tp"),
        P(None, "tp"),
        P(None, "tp"),
        P(None, "tp"),
        P(None, "tp", "dp"),
        P(None, ("grp", "dp"), "tp", None, None),
        P(None, ("grp", "dp"), None, "tp"),
        P(None, ("grp", "dp"), None, "tp"),
        P(None, ("grp", "dp"), None, "tp"),
    )
    return jax.shard_map(
        functools.partial(body, mesh.shape["tp"], mesh.shape["dp"]),
        mesh=mesh,
        in_specs=placed,
        out_specs=(placed[0], placed[15], placed[16], placed[17], placed[18]),
        check_vma=False,
    )
```

```python
import functools

import jax
import jax.numpy as jnp
from jax import lax
from jax.experimental import pallas as pl
from jax.experimental.pallas import tpu as pltpu
from jax.sharding import PartitionSpec as P

EPSILON = 1e-05
F32 = jnp.float32
BF16 = jnp.bfloat16
MESH = pl.DeviceIdType.MESH
NT = (((1,), (1,)), ((), ()))
LANES = 128
INPUTS = 19
GROUP = 4


def silu(v):
    return v * jax.nn.sigmoid(v)


def kernel(
    tp_n,
    dp_n,
    features,
    *refs,
):
    held, refs = refs[:INPUTS], refs[INPUTS:]
    res_o, ssm_o, nx_o, nb_o, nc_o = refs[:5]
    a_buf, b_out, b_in, c_own, c_buf, d_out, d_in, r_buf = refs[5:13]
    w_z, w_x, w_out, w_bcd, gains, conv_bc, s_bc, st_t = refs[13:21]
    here = refs[21 : 17 + INPUTS]
    local_sem, pair_sem, send_sem, recv_sem = refs[17 + INPUTS :]
    (
        gain,
        w_bt,
        w_ct,
        w_dtt,
        conv_x,
        conv_b,
        conv_c,
        dt_bias,
        a_log,
        d_skip,
        out_gain,
        ssm,
        s_x,
        s_b,
        s_c,
    ) = here
    layers, heads_here = dt_bias.shape
    rows, width_f = res_o.shape
    zw = w_z.shape[3]
    bw = w_bt.shape[1]
    hd = zw // heads_here
    my_tp, my_dp = lax.axis_index("tp"), lax.axis_index("dp")
    my_x, my_core = lax.div(my_dp, 2), lax.rem(my_dp, 2)
    half = tp_n // 2
    uneven = lax.rem(my_tp + my_core, 2) == 1
    row_core = lax.rem(my_tp, 2)

    def nearest(k, n):
        return (k + 1) // 2 if k % 2 else (n - k // 2) % n

    def place(distance, n):
        return jnp.where(distance <= n // 2, jnp.maximum(2 * distance - 1, 0), 2 * (n - distance))

    def tp_at(k):
        return lax.rem(my_tp + nearest(k, tp_n), tp_n)

    def x_at(k):
        return lax.rem(my_x + nearest(k, half), half)

    def rows_at(k):
        odd = tp_n - k if k % 2 else k + 1
        return lax.rem(my_tp + jnp.where(uneven, odd, 2 * nearest(k, half)), tp_n)

    def rows_place(offset):
        odd = jnp.where(offset < half, offset - 1, tp_n - offset)
        return jnp.where(lax.rem(offset, 2) == 1, odd, place(lax.div(offset, 2), half))

    def sent_place(k):
        offset = (tp_n - nearest(k, tp_n)) % tp_n
        if offset % 2:
            return offset - 1 if offset < half else tp_n - offset
        distance = offset // 2
        return max(2 * distance - 1, 0) if 2 * distance <= half else 2 * (half - distance)

    def x_mirror(k):
        if k == 0 or (k == half - 1 and half % 2 == 0):
            return k
        return k + 1 if k % 2 else k - 1

    k_rows = rows_place(lax.rem(my_dp - my_tp + tp_n, tp_n))

    def remote(src, dst, layer, phase, s_slot, r_slot, target):
        return pltpu.make_async_remote_copy(
            src_ref=src,
            dst_ref=dst,
            send_sem=send_sem.at[layer, phase, s_slot],
            recv_sem=recv_sem.at[layer, phase, r_slot],
            device_id=target,
            device_id_type=MESH,
        )

    def column(z, core):
        return {"tp": z, "dp": 2 * my_x + core}

    def row(x):
        return {"dp": 2 * x + my_core}

    layer_list = range(layers)
    fetch = [pltpu.make_async_copy(held[0], r_buf.at[0], local_sem.at[0])]
    used = 1
    for n in range(3):
        whole = (w_z, w_x, w_out)[n]
        for l in layer_list:
            fetch.append(
                pltpu.make_async_copy(
                    held[1 + n].at[l], whole.at[l, my_core], local_sem.at[used]
                )
            )
            used += 1
    for n in range(4, INPUTS):
        fetch.append(pltpu.make_async_copy(held[n], here[n - 4], local_sem.at[used]))
        used += 1
    fetch[0].start()
    barrier = pltpu.get_barrier_semaphore()

    def greet(device):
        pl.semaphore_signal(barrier, inc=1, device_id=device, device_id_type=MESH)

    for k in range(tp_n - 1, 0, -1):
        greet(column(tp_at(k), 0))
        greet(column(tp_at(k), 1))
    for k in range(half - 1, 0, -1):
        greet(row(x_at(k)))
    greet(column(my_tp, 1 - my_core))
    for f in fetch[1:]:
        f.start()

    def copy_a(l, k):
        if k == 0:
            dst = a_buf.at[l, 0, my_core]
            return remote(r_buf.at[l], dst, l, 0, 0, my_core, column(my_tp, row_core))
        slot = sent_place(k)
        dst = a_buf.at[l, slot, my_core]
        return remote(r_buf.at[l], dst, l, 0, k, 2 * slot + my_core, column(tp_at(k), row_core))

    def send_a(l):
        for k in range(tp_n - 1, 0, -1):
            copy_a(l, k).start()

        @pl.when(uneven)
        def _():
            copy_a(l, 0).start()

        @pl.when(jnp.logical_not(uneven))
        def _():
            a_buf[l, 0, my_core] = r_buf[l]

    def copy_b(l, k):
        to = row(lax.div(rows_at(k), 2))
        return remote(b_out.at[l, k], b_in.at[l, my_x], l, 1, k, my_x, to)

    def copy_c(l, k):
        slot = x_mirror(k)
        return remote(c_own.at[l], c_buf.at[l, slot], l, 2, k, slot, row(x_at(k)))

    def copy_d(l, k, core):
        to = column(2 * x_at(k) + my_core, core)
        return remote(d_out.at[l, k, core], d_in.at[l, my_tp], l, 3, 2 * k + core, my_tp, to)

    def sent_abc(l):
        for k in range(1, tp_n):
            copy_a(l, k).wait_send()

        @pl.when(uneven)
        def _():
            copy_a(l, 0).wait_send()

        for k in range(half):

            @pl.when(rows_at(k) != my_dp)
            def _(k=k):
                copy_b(l, k).wait_send()

            if k > 0:
                copy_c(l, k).wait_send()

    def sent_d(l):
        for k in range(half):
            for core in range(2):

                @pl.when(jnp.logical_not((2 * x_at(k) + my_core == my_tp) & (my_core == core)))
                def _(k=k, core=core):
                    copy_d(l, k, core).wait_send()

    pl.semaphore_wait(barrier, 2 * tp_n - 1 + half - 1)
    fetch[0].wait()
    send_a(0)

    for f in fetch[1:]:
        f.wait()
    heads_all = w_dtt.shape[1]
    pick = lax.broadcasted_iota(jnp.int32, (16, heads_all), 0)
    col = lax.broadcasted_iota(jnp.int32, (16, heads_all), 1)
    pick = jnp.where((pick < heads_here) & (col == pick + my_tp * heads_here), 1.0, 0.0).astype(BF16)
    for l in range(layers):
        w_bcd[l, my_core, 0:bw] = w_bt[l]
        w_bcd[l, my_core, bw : 2 * bw] = w_ct[l]
        w_bcd[l, my_core, 2 * bw : 2 * bw + 16] = jnp.dot(
            pick, w_dtt[l], preferred_element_type=F32
        ).astype(BF16)
        w_bcd[l, my_core, 2 * bw + 16 :] = jnp.zeros(
            (w_bcd.shape[2] - 2 * bw - 16, width_f), BF16
        )
        conv_bc[l] = jnp.concatenate([conv_b[l].astype(F32), conv_c[l].astype(F32)], axis=1)
        for k in range(s_b.shape[1]):
            s_bc[l, k] = jnp.concatenate([s_b[l, k].astype(F32), s_c[l, k].astype(F32)], axis=1)

    gains[my_core] = jnp.zeros(gains.shape[1:], F32)
    gains[my_core, 0:layers] = gain[...].astype(F32)

    pair = []
    for whole in [gains.at[my_core]] + [
        w.at[l, my_core] for l in layer_list for w in (w_z, w_x, w_bcd, w_out)
    ]:
        pair.append(
            pltpu.make_async_remote_copy(
                src_ref=whole,
                dst_ref=whole,
                send_sem=pair_sem.at[0, len(pair)],
                recv_sem=pair_sem.at[1, len(pair)],
                device_id=column(my_tp, 1 - my_core),
                device_id_type=MESH,
            )
        )
    for p in pair:
        p.start()

    def turn(i, carry):
        for l in range(layers):
            block = ssm[l, i].reshape(zw, bw)
            st_t[l, i] = block.T.astype(BF16)
        return carry

    lax.fori_loop(0, rows, turn, 0)
    lane = lax.broadcasted_iota(jnp.int32, (rows, LANES), 1)
    head_of = lax.broadcasted_iota(jnp.int32, (rows, zw), 1)
    head_of = lax.div(head_of, hd)

    def per_head(v):
        out = jnp.broadcast_to(v[:, 0:1], (rows, zw))
        for h in range(1, heads_here):
            out = jnp.where(head_of == h, v[:, h : h + 1], out)
        return out

    for l in range(layers):
        if l > 0:
            send_a(l)

        for first in range(0, half, GROUP):
            group = min(GROUP, half)
            for k in range(first, first + group):
                for core in range(2):
                    got = a_buf.at[l, k, core]
                    copy = remote(got, got, l, 0, k, 2 * k + core, column(rows_at(k), core))
                    if k > 0:
                        copy.wait_recv()
                    else:

                        @pl.when(uneven | (my_core != core))
                        def _(copy=copy):
                            copy.wait_recv()

            if l == 0 and first == 0:
                for p in pair:
                    p.wait_recv()
            tall = group * rows
            scaled, squares = [], 0.0
            for core in range(2):
                block = a_buf[l, first : first + group, core].reshape(tall, width_f).astype(F32)
                scaled.append((block * gains[core, l : l + 1]).astype(BF16))
                squares = squares + jnp.sum(block * block, axis=1, keepdims=True)
            both_wide = jnp.concatenate(scaled, axis=1)
            part_z = jnp.dot(
                both_wide, w_z[l].reshape(2 * width_f, zw), preferred_element_type=F32
            ).astype(BF16)
            part_x = jnp.dot(
                both_wide, w_x[l].reshape(2 * width_f, zw), preferred_element_type=F32
            ).astype(BF16)
            rest = lax.dot_general(scaled[0], w_bcd[l, 0], NT, preferred_element_type=F32)
            rest += lax.dot_general(scaled[1], w_bcd[l, 1], NT, preferred_element_type=F32)
            lane_tall = lax.broadcasted_iota(jnp.int32, (tall, LANES), 1)
            small = jnp.where(lane_tall == heads_here, squares, rest[:, LANES:])
            low = small - small.astype(BF16).astype(F32)
            both = jnp.where(lane_tall < LANES // 2, small, pltpu.roll(low, LANES // 2, 1))
            b_out[l, first : first + group, :, 0:zw] = part_z.reshape(group, rows, zw)
            b_out[l, first : first + group, :, zw : 2 * zw] = part_x.reshape(group, rows, zw)
            b_out[l, first : first + group, :, 2 * zw : 2 * zw + LANES] = (
                rest[:, 0:LANES].astype(BF16).reshape(group, rows, LANES)
            )
            b_out[l, first : first + group, :, 2 * zw + LANES :] = both.astype(BF16).reshape(
                group, rows, LANES
            )
            for k in range(first, first + group):

                @pl.when(rows_at(k) != my_dp)
                def _(k=k, l=l):
                    copy_b(l, k).start()

        total = b_out[l, k_rows].astype(F32)
        for k in range(1, half):
            x = x_at(k)
            remote(b_in.at[l, x], b_in.at[l, x], l, 1, k, x, row(x)).wait_recv()
            total = total + b_in[l, x].astype(F32)

        small = total[:, 2 * zw + LANES :]
        small = small + pltpu.roll(small, LANES // 2, 1)
        row_scale = lax.rsqrt(small[:, heads_here : heads_here + 1] / features + EPSILON)
        step_raw = small[:, 0:heads_here] * row_scale
        gate = (total[:, 0:zw] * row_scale).astype(BF16).astype(F32)
        x_new = (total[:, zw : 2 * zw] * row_scale).astype(BF16)
        bc_new = (total[:, 2 * zw : 2 * zw + LANES] * row_scale).astype(BF16)
        taps = conv_x.shape[1]
        conv = x_new.astype(F32) * conv_x[l, taps - 1 : taps].astype(F32)
        conv2 = bc_new.astype(F32) * conv_bc[l, taps - 1 : taps]
        for k in range(taps - 1):
            conv = conv + s_x[l, k].astype(F32) * conv_x[l, k : k + 1].astype(F32)
            conv2 = conv2 + s_bc[l, k] * conv_bc[l, k : k + 1]
        v = silu(conv)
        bc = silu(conv2)
        step = jax.nn.softplus(step_raw + dt_bias[l : l + 1])
        decay = jnp.exp(-step * jnp.exp(a_log[l : l + 1]))
        xs = per_head(step) * v
        turned = pltpu.roll(bc, LANES // 2, 1)
        b_dot_c = 0.5 * jnp.sum(bc * turned, axis=1, keepdims=True)
        cc = jnp.where(lane < LANES // 2, turned, bc)
        seq = lax.broadcasted_iota(jnp.int32, (rows, LANES), 0)
        pieces = []
        for s in range(0, rows, 2):
            pieces.append(jnp.where(seq == s + lax.div(lane, LANES // 2), cc, 0.0).astype(BF16))
        spread = jnp.concatenate(pieces, axis=1)
        reads = jnp.dot(
            spread, st_t[l].reshape(rows * bw, zw), preferred_element_type=F32
        )
        readout = per_head(decay) * reads + (xs * b_dot_c + per_head(d_skip[l : l + 1]) * v)
        gated = readout * silu(gate)
        scale = lax.rsqrt(jnp.mean(gated * gated, axis=1, keepdims=True) + EPSILON)
        mixed = (gated * scale * out_gain[l : l + 1].astype(F32)).astype(BF16)

        c_own[l] = mixed
        c_buf[l, 0] = mixed

        for k in range(half - 1, 0, -1):
            copy_c(l, k).start()

        for first in range(0, half, GROUP):
            group = min(GROUP, half)
            for k in range(max(first, 1), first + group):
                got = c_buf.at[l, k]
                remote(got, got, l, 2, k, k, row(x_at(k))).wait_recv()
            block = c_buf[l, first : first + group].reshape(group * rows, zw)
            for core in range(2):
                part = jnp.dot(block, w_out[l, core], preferred_element_type=F32).astype(BF16)
                d_out[l, first : first + group, core] = part.reshape(group, rows, width_f)
            for k in range(first, first + group):
                z = 2 * x_at(k) + my_core
                for core in range(2):
                    mine = (z == my_tp) & (my_core == core)

                    @pl.when(jnp.logical_not(mine))
                    def _(k=k, core=core, l=l):
                        copy_d(l, k, core).start()

                    @pl.when(mine)
                    def _(k=k, core=core, l=l):
                        d_in[l, my_tp] = d_out[l, k, core]

        xs_t = xs.T
        for s in range(rows):
            for h in range(heads_here):
                b_row = bc[s : s + 1, 0:bw]
                xs_col = xs_t[h * hd : (h + 1) * hd, s : s + 1]
                ssm_o[l, s, h] = ssm[l, s, h] * decay[s : s + 1, h : h + 1] + xs_col * b_row
        for k in range(taps - 2):
            nx_o[l, k] = s_x[l, k + 1]
            nb_o[l, k] = s_b[l, k + 1]
            nc_o[l, k] = s_c[l, k + 1]
        nx_o[l, taps - 2] = x_new
        nb_o[l, taps - 2] = bc_new[:, 0:bw]
        nc_o[l, taps - 2] = bc_new[:, bw : 2 * bw]

        sent_abc(l)
        if l > 0:
            sent_d(l - 1)

        @pl.when(uneven)
        def _(l=l):
            got = d_in.at[l, my_tp]
            remote(got, got, l, 3, 0, my_tp, column(my_tp, row_core)).wait_recv()

        projected = d_in[l, my_tp].astype(F32)
        for k in range(1, tp_n):
            z = tp_at(k)
            got = d_in.at[l, z]
            remote(got, got, l, 3, k, z, column(z, row_core)).wait_recv()
            projected = projected + d_in[l, z].astype(F32)
        new = (r_buf[l].astype(F32) + projected).astype(BF16)
        if l + 1 < layers:
            r_buf[l + 1] = new
        else:
            res_o[...] = new

    sent_d(layers - 1)
    for p in pair:
        p.wait_send()


def write_out(*refs):
    sem = refs[-1]
    half = len(refs) // 2
    copies = [
        pltpu.make_async_copy(refs[n], refs[half + n], sem.at[n]) for n in range(half)
    ]
    for c in copies:
        c.start()
    for c in copies:
        c.wait()


def body(tp_n, dp_n, *args):
    (
        tokens,
        norm_gain,
        w_z,
        w_x,
        w_b,
        w_c,
        w_dt,
        conv_x,
        conv_b,
        conv_c,
        dt_bias,
        a_log,
        d_skip,
        out_gain,
        w_out,
        ssm_state,
        state_x,
        state_b,
        state_c,
    ) = args
    layers, heads_here = dt_bias.shape
    rows, width_f = tokens.shape
    zw, bw = w_z.shape[2], w_b.shape[2]
    assert tp_n == dp_n and 2 * bw == LANES
    wide = 2 * zw + 2 * LANES
    half = tp_n // 2

    def turn(a):
        return jnp.swapaxes(a, 1, 2)

    operands = (
        tokens,
        w_z,
        w_x,
        w_out,
        norm_gain,
        turn(w_b),
        turn(w_c),
        turn(w_dt),
        conv_x,
        conv_b,
        conv_c,
        dt_bias,
        a_log,
        d_skip,
        out_gain,
        ssm_state,
        turn(state_x),
        turn(state_b),
        turn(state_c),
    )
    vmem = pl.BlockSpec(memory_space=pltpu.VMEM)
    hbm = pl.BlockSpec(memory_space=pltpu.HBM)

    def like(a):
        return pltpu.VMEM(a.shape, a.dtype)

    results = pl.pallas_call(
        functools.partial(kernel, tp_n, dp_n, width_f * dp_n),
        out_shape=(
            like(tokens),
            like(ssm_state),
            like(operands[16]),
            like(operands[17]),
            like(operands[18]),
        ),
        in_specs=[hbm] * INPUTS,
        out_specs=(vmem,) * 5,
        scratch_shapes=[
            pltpu.VMEM((layers, half, 2, rows, width_f), BF16),
            pltpu.VMEM((layers, half, rows, wide), BF16),
            pltpu.VMEM((layers, half, rows, wide), BF16),
            pltpu.VMEM((layers, rows, zw), BF16),
            pltpu.VMEM((layers, half, rows, zw), BF16),
            pltpu.VMEM((layers, half, 2, rows, width_f), BF16),
            pltpu.VMEM((layers, tp_n, rows, width_f), BF16),
            pltpu.VMEM((layers, rows, width_f), BF16),
            pltpu.VMEM((layers, 2, width_f, zw), BF16),
            pltpu.VMEM((layers, 2, width_f, zw), BF16),
            pltpu.VMEM((layers, 2, zw, width_f), BF16),
            pltpu.VMEM((layers, 2, 2 * LANES, width_f), BF16),
            pltpu.VMEM((2, 8, width_f), F32),
            pltpu.VMEM((layers, conv_x.shape[1], LANES), F32),
            pltpu.VMEM((layers, state_b.shape[2], rows, LANES), F32),
            pltpu.VMEM((layers, rows, bw, zw), BF16),
            *(pltpu.VMEM(a.shape, a.dtype) for a in operands[4:]),
            pltpu.SemaphoreType.DMA((INPUTS - 3 + 3 * layers,)),
            pltpu.SemaphoreType.DMA((2, 1 + 4 * layers)),
            pltpu.SemaphoreType.DMA((layers, 4, tp_n)),
            pltpu.SemaphoreType.DMA((layers, 4, tp_n)),
        ],
        compiler_params=pltpu.CompilerParams(
            collective_id=0, has_side_effects=True, vmem_limit_bytes=40 * 1024 * 1024
        ),
        name="decode",
    )(*(pltpu.with_memory_space_constraint(a, pltpu.HBM) for a in operands))
    results = [pltpu.with_memory_space_constraint(a, pltpu.VMEM) for a in results]
    residual, ssm_next, next_x, next_b, next_c = pl.pallas_call(
        write_out,
        out_shape=tuple(jax.ShapeDtypeStruct(a.shape, a.dtype) for a in results),
        in_specs=(vmem,) * 5,
        out_specs=(hbm,) * 5,
        scratch_shapes=[pltpu.SemaphoreType.DMA((5,))],
        compiler_params=pltpu.CompilerParams(vmem_limit_bytes=8 * 1024 * 1024),
        name="write_out",
    )(*results)
    return residual, ssm_next, turn(next_x), turn(next_b), turn(next_c)


def solution(mesh):
    placed = (
        P(("grp", "tp"), "dp"),
        P(None, "dp"),
        P(None, "dp", "tp"),
        P(None, "dp", "tp"),
        P(None, "dp", "tp"),
        P(None, "dp", "tp"),
        P(None, "dp", None),
        P(None, None, "tp"),
        P(None, None, "tp"),
        P(None, None, "tp"),
        P(None, "tp"),
        P(None, "tp"),
        P(None, "tp"),
        P(None, "tp"),
        P(None, "tp", "dp"),
        P(None, ("grp", "dp"), "tp", None, None),
        P(None, ("grp", "dp"), None, "tp"),
        P(None, ("grp", "dp"), None, "tp"),
        P(None, ("grp", "dp"), None, "tp"),
    )
    return jax.shard_map(
        functools.partial(body, mesh.shape["tp"], mesh.shape["dp"]),
        mesh=mesh,
        in_specs=placed,
        out_specs=(placed[0], placed[15], placed[16], placed[17], placed[18]),
        check_vma=False,
    )
```

```python
import functools

import jax
import jax.numpy as jnp
from jax import lax
from jax.experimental import pallas as pl
from jax.experimental.pallas import tpu as pltpu
from jax.sharding import PartitionSpec as P

EPSILON = 1e-05
F32 = jnp.float32
BF16 = jnp.bfloat16
MESH = pl.DeviceIdType.MESH
NT = (((1,), (1,)), ((), ()))
LANES = 128
INPUTS = 19
GROUP = 4


def silu(v):
    return v * jax.nn.sigmoid(v)


def kernel(
    tp_n,
    dp_n,
    features,
    *refs,
):
    held, refs = refs[:INPUTS], refs[INPUTS:]
    res_o, ssm_o, nx_o, nb_o, nc_o = refs[:5]
    a_buf, b_out, b_in, c_own, c_buf, d_out, d_in, r_buf = refs[5:13]
    w_z, w_x, w_out, w_bcd, gains, conv_bc, s_bc, st_t = refs[13:21]
    here = refs[21 : 17 + INPUTS]
    local_sem, pair_sem, send_sem, recv_sem = refs[17 + INPUTS :]
    (
        gain,
        w_bt,
        w_ct,
        w_dtt,
        conv_x,
        conv_b,
        conv_c,
        dt_bias,
        a_log,
        d_skip,
        out_gain,
        ssm,
        s_x,
        s_b,
        s_c,
    ) = here
    layers, heads_here = dt_bias.shape
    rows, width_f = res_o.shape
    zw = w_z.shape[3]
    bw = w_bt.shape[1]
    hd = zw // heads_here
    my_tp, my_dp = lax.axis_index("tp"), lax.axis_index("dp")
    my_x, my_core = lax.div(my_dp, 2), lax.rem(my_dp, 2)
    half, near = tp_n // 2, tp_n // 4
    uneven = lax.rem(my_tp + my_core, 2) == 1
    row_core = lax.rem(my_tp, 2)

    def nearest(k, n):
        return (k + 1) // 2 if k % 2 else (n - k // 2) % n

    def place(distance, n):
        return jnp.where(distance <= n // 2, jnp.maximum(2 * distance - 1, 0), 2 * (n - distance))

    def tp_at(k):
        return lax.rem(my_tp + nearest(k, tp_n), tp_n)

    def x_at(k):
        return lax.rem(my_x + nearest(k, half), half)

    def rows_at(k):
        odd = tp_n - k if k % 2 else k + 1
        return lax.rem(my_tp + jnp.where(uneven, odd, 2 * nearest(k, half)), tp_n)

    def rows_place(offset):
        odd = jnp.where(offset < half, offset - 1, tp_n - offset)
        return jnp.where(lax.rem(offset, 2) == 1, odd, place(lax.div(offset, 2), half))

    def sent_place(k):
        offset = (tp_n - nearest(k, tp_n)) % tp_n
        if offset % 2:
            return offset - 1 if offset < half else tp_n - offset
        distance = offset // 2
        return max(2 * distance - 1, 0) if 2 * distance <= half else 2 * (half - distance)

    def x_mirror(k):
        if k == 0 or (k == half - 1 and half % 2 == 0):
            return k
        return k + 1 if k % 2 else k - 1

    k_rows = rows_place(lax.rem(my_dp - my_tp + tp_n, tp_n))

    def remote(src, dst, layer, phase, s_slot, r_slot, target):
        return pltpu.make_async_remote_copy(
            src_ref=src,
            dst_ref=dst,
            send_sem=send_sem.at[layer, phase, s_slot],
            recv_sem=recv_sem.at[layer, phase, r_slot],
            device_id=target,
            device_id_type=MESH,
        )

    def column(z, core):
        return {"tp": z, "dp": 2 * my_x + core}

    def row(x):
        return {"dp": 2 * x + my_core}

    layer_list = range(layers)
    fetch = [pltpu.make_async_copy(held[0], r_buf.at[0], local_sem.at[0])]
    used = 1
    for n in range(3):
        whole = (w_z, w_x, w_out)[n]
        for l in layer_list:
            fetch.append(
                pltpu.make_async_copy(
                    held[1 + n].at[l], whole.at[l, my_core], local_sem.at[used]
                )
            )
            used += 1
    for n in range(4, INPUTS):
        fetch.append(pltpu.make_async_copy(held[n], here[n - 4], local_sem.at[used]))
        used += 1
    fetch[0].start()
    barrier = pltpu.get_barrier_semaphore()

    def greet(device):
        pl.semaphore_signal(barrier, inc=1, device_id=device, device_id_type=MESH)

    for k in range(2 * near, 0, -1):
        greet(column(tp_at(k), 0))
        greet(column(tp_at(k), 1))
    for k in range(half - 1, 0, -1):
        greet(row(x_at(k)))
    greet(column(my_tp, 1 - my_core))
    for f in fetch[1:]:
        f.start()

    def copy_a(l, k):
        if k == 0:
            dst = a_buf.at[l, 0, my_core]
            return remote(r_buf.at[l], dst, l, 0, 0, my_core, column(my_tp, row_core))
        slot = sent_place(k)
        dst = a_buf.at[l, slot, my_core]
        return remote(r_buf.at[l], dst, l, 0, k, 2 * slot + my_core, column(tp_at(k), row_core))

    def reach(l):
        return 2 * near if l == 0 else tp_n - 1

    def send_a(l):
        for k in range(reach(l), 0, -1):
            copy_a(l, k).start()

        @pl.when(uneven)
        def _():
            copy_a(l, 0).start()

        @pl.when(jnp.logical_not(uneven))
        def _():
            a_buf[l, 0, my_core] = r_buf[l]

    def offset_of(odd, k):
        if odd:
            return -k if k % 2 else k + 1
        return -k if k % 2 == 0 else k + 1

    def relayed(odd, down):
        offsets = [offset_of(odd, k) for k in range(half)]
        step = near if down else -near
        return [
            (offsets.index(o - step), k)
            for k, o in enumerate(offsets)
            if (o > near if down else o < -near)
        ]

    def copy_relay(source, target, down):
        z = lax.rem(my_tp + (tp_n - near if down else near), tp_n)
        src, dst = a_buf.at[0, source], a_buf.at[0, target]
        return remote(src, dst, 0, 4, target, target, column(z, my_core))

    def relay(odd, down):
        for source, target in relayed(odd, down):
            for core in range(2):
                got = a_buf.at[0, source, core]
                remote(
                    got, got, 0, 0, 0, 2 * source + core, column(rows_at(source), core)
                ).wait_recv()
            copy_relay(source, target, down).start()

    def wait_first_a(odd, k):
        if abs(offset_of(odd, k)) > near:
            copy_relay(k, k, 0).wait_recv()
        elif k not in [source for down in range(2) for source, _ in relayed(odd, down)]:
            for core in range(2):
                got = a_buf.at[0, k, core]
                copy = remote(got, got, 0, 0, k, 2 * k + core, column(rows_at(k), core))
                if offset_of(odd, k) != 0:
                    copy.wait_recv()
                else:

                    @pl.when(my_core != core)
                    def _(copy=copy):
                        copy.wait_recv()

    def copy_b(l, k):
        to = row(lax.div(rows_at(k), 2))
        return remote(b_out.at[l, k], b_in.at[l, my_x], l, 1, k, my_x, to)

    def copy_c(l, k):
        slot = x_mirror(k)
        return remote(c_own.at[l], c_buf.at[l, slot], l, 2, k, slot, row(x_at(k)))

    def copy_d(l, k, core):
        to = column(2 * x_at(k) + my_core, core)
        return remote(d_out.at[l, k, core], d_in.at[l, my_tp], l, 3, 2 * k + core, my_tp, to)

    def sent_abc(l):
        for k in range(1, reach(l) + 1):
            copy_a(l, k).wait_send()

        @pl.when(uneven)
        def _():
            copy_a(l, 0).wait_send()

        if l == 0:
            for odd in range(2):

                @pl.when(uneven == (odd == 1))
                def _(odd=odd):
                    for down in range(2):
                        for source, target in relayed(odd, down):
                            copy_relay(source, target, down).wait_send()

        for k in range(half):

            @pl.when(rows_at(k) != my_dp)
            def _(k=k):
                copy_b(l, k).wait_send()

            if k > 0:
                copy_c(l, k).wait_send()

    def sent_d(l):
        for k in range(half):
            for core in range(2):

                @pl.when(jnp.logical_not((2 * x_at(k) + my_core == my_tp) & (my_core == core)))
                def _(k=k, core=core):
                    copy_d(l, k, core).wait_send()

    pl.semaphore_wait(barrier, 4 * near + 1 + half - 1)
    fetch[0].wait()
    send_a(0)

    for f in fetch[1:]:
        f.wait()
    heads_all = w_dtt.shape[1]
    pick = lax.broadcasted_iota(jnp.int32, (16, heads_all), 0)
    col = lax.broadcasted_iota(jnp.int32, (16, heads_all), 1)
    pick = jnp.where((pick < heads_here) & (col == pick + my_tp * heads_here), 1.0, 0.0).astype(BF16)
    for l in range(layers):
        w_bcd[l, my_core, 0:bw] = w_bt[l]
        w_bcd[l, my_core, bw : 2 * bw] = w_ct[l]
        w_bcd[l, my_core, 2 * bw : 2 * bw + 16] = jnp.dot(
            pick, w_dtt[l], preferred_element_type=F32
        ).astype(BF16)
        w_bcd[l, my_core, 2 * bw + 16 :] = jnp.zeros(
            (w_bcd.shape[2] - 2 * bw - 16, width_f), BF16
        )
        conv_bc[l] = jnp.concatenate([conv_b[l].astype(F32), conv_c[l].astype(F32)], axis=1)
        for k in range(s_b.shape[1]):
            s_bc[l, k] = jnp.concatenate([s_b[l, k].astype(F32), s_c[l, k].astype(F32)], axis=1)

    gains[my_core] = jnp.zeros(gains.shape[1:], F32)
    gains[my_core, 0:layers] = gain[...].astype(F32)

    pair = []
    for whole in [gains.at[my_core]] + [
        w.at[l, my_core] for l in layer_list for w in (w_z, w_x, w_bcd, w_out)
    ]:
        pair.append(
            pltpu.make_async_remote_copy(
                src_ref=whole,
                dst_ref=whole,
                send_sem=pair_sem.at[0, len(pair)],
                recv_sem=pair_sem.at[1, len(pair)],
                device_id=column(my_tp, 1 - my_core),
                device_id_type=MESH,
            )
        )
    for p in pair:
        p.start()

    down_first = my_tp < half
    for odd in range(2):
        for order in ((0, 1), (1, 0)):

            @pl.when((uneven == (odd == 1)) & (down_first == (order[0] == 1)))
            def _(odd=odd, order=order):
                for down in order:
                    relay(odd, down)

    def turn(i, carry):
        for l in range(layers):
            block = ssm[l, i].reshape(zw, bw)
            st_t[l, i] = block.T.astype(BF16)
        return carry

    lane = lax.broadcasted_iota(jnp.int32, (rows, LANES), 1)
    head_of = lax.broadcasted_iota(jnp.int32, (rows, zw), 1)
    head_of = lax.div(head_of, hd)

    def per_head(v):
        out = jnp.broadcast_to(v[:, 0:1], (rows, zw))
        for h in range(1, heads_here):
            out = jnp.where(head_of == h, v[:, h : h + 1], out)
        return out

    for l in range(layers):
        if l > 0:
            send_a(l)

        for first in range(0, half, GROUP):
            group = min(GROUP, half)
            if l == 0:
                for odd in range(2):

                    @pl.when(uneven == (odd == 1))
                    def _(odd=odd, first=first, group=group):
                        for k in range(first, first + group):
                            wait_first_a(odd, k)

            else:
                for k in range(first, first + group):
                    for core in range(2):
                        got = a_buf.at[l, k, core]
                        copy = remote(got, got, l, 0, k, 2 * k + core, column(rows_at(k), core))
                        if k > 0:
                            copy.wait_recv()
                        else:

                            @pl.when(uneven | (my_core != core))
                            def _(copy=copy):
                                copy.wait_recv()

            if l == 0 and first == 0:
                for p in pair:
                    p.wait_recv()
            tall = group * rows
            scaled, squares = [], 0.0
            for core in range(2):
                block = a_buf[l, first : first + group, core].reshape(tall, width_f).astype(F32)
                scaled.append((block * gains[core, l : l + 1]).astype(BF16))
                squares = squares + jnp.sum(block * block, axis=1, keepdims=True)
            both_wide = jnp.concatenate(scaled, axis=1)
            part_z = jnp.dot(
                both_wide, w_z[l].reshape(2 * width_f, zw), preferred_element_type=F32
            ).astype(BF16)
            part_x = jnp.dot(
                both_wide, w_x[l].reshape(2 * width_f, zw), preferred_element_type=F32
            ).astype(BF16)
            rest = lax.dot_general(scaled[0], w_bcd[l, 0], NT, preferred_element_type=F32)
            rest += lax.dot_general(scaled[1], w_bcd[l, 1], NT, preferred_element_type=F32)
            lane_tall = lax.broadcasted_iota(jnp.int32, (tall, LANES), 1)
            small = jnp.where(lane_tall == heads_here, squares, rest[:, LANES:])
            low = small - small.astype(BF16).astype(F32)
            both = jnp.where(lane_tall < LANES // 2, small, pltpu.roll(low, LANES // 2, 1))
            b_out[l, first : first + group, :, 0:zw] = part_z.reshape(group, rows, zw)
            b_out[l, first : first + group, :, zw : 2 * zw] = part_x.reshape(group, rows, zw)
            b_out[l, first : first + group, :, 2 * zw : 2 * zw + LANES] = (
                rest[:, 0:LANES].astype(BF16).reshape(group, rows, LANES)
            )
            b_out[l, first : first + group, :, 2 * zw + LANES :] = both.astype(BF16).reshape(
                group, rows, LANES
            )
            for k in range(first, first + group):

                @pl.when(rows_at(k) != my_dp)
                def _(k=k, l=l):
                    copy_b(l, k).start()

        if l == 0:
            lax.fori_loop(0, rows, turn, 0)
        total = b_out[l, k_rows].astype(F32)
        for k in range(1, half):
            x = x_at(k)
            remote(b_in.at[l, x], b_in.at[l, x], l, 1, k, x, row(x)).wait_recv()
            total = total + b_in[l, x].astype(F32)

        small = total[:, 2 * zw + LANES :]
        small = small + pltpu.roll(small, LANES // 2, 1)
        row_scale = lax.rsqrt(small[:, heads_here : heads_here + 1] / features + EPSILON)
        step_raw = small[:, 0:heads_here] * row_scale
        gate = (total[:, 0:zw] * row_scale).astype(BF16).astype(F32)
        x_new = (total[:, zw : 2 * zw] * row_scale).astype(BF16)
        bc_new = (total[:, 2 * zw : 2 * zw + LANES] * row_scale).astype(BF16)
        taps = conv_x.shape[1]
        conv = x_new.astype(F32) * conv_x[l, taps - 1 : taps].astype(F32)
        conv2 = bc_new.astype(F32) * conv_bc[l, taps - 1 : taps]
        for k in range(taps - 1):
            conv = conv + s_x[l, k].astype(F32) * conv_x[l, k : k + 1].astype(F32)
            conv2 = conv2 + s_bc[l, k] * conv_bc[l, k : k + 1]
        v = silu(conv)
        bc = silu(conv2)
        step = jax.nn.softplus(step_raw + dt_bias[l : l + 1])
        decay = jnp.exp(-step * jnp.exp(a_log[l : l + 1]))
        xs = per_head(step) * v
        turned = pltpu.roll(bc, LANES // 2, 1)
        b_dot_c = 0.5 * jnp.sum(bc * turned, axis=1, keepdims=True)
        cc = jnp.where(lane < LANES // 2, turned, bc)
        seq = lax.broadcasted_iota(jnp.int32, (rows, LANES), 0)
        pieces = []
        for s in range(0, rows, 2):
            pieces.append(jnp.where(seq == s + lax.div(lane, LANES // 2), cc, 0.0).astype(BF16))
        spread = jnp.concatenate(pieces, axis=1)
        reads = jnp.dot(
            spread, st_t[l].reshape(rows * bw, zw), preferred_element_type=F32
        )
        readout = per_head(decay) * reads + (xs * b_dot_c + per_head(d_skip[l : l + 1]) * v)
        gated = readout * silu(gate)
        scale = lax.rsqrt(jnp.mean(gated * gated, axis=1, keepdims=True) + EPSILON)
        mixed = (gated * scale * out_gain[l : l + 1].astype(F32)).astype(BF16)

        c_own[l] = mixed
        c_buf[l, 0] = mixed

        for k in range(half - 1, 0, -1):
            copy_c(l, k).start()

        for first in range(0, half, GROUP):
            group = min(GROUP, half)
            for k in range(max(first, 1), first + group):
                got = c_buf.at[l, k]
                remote(got, got, l, 2, k, k, row(x_at(k))).wait_recv()
            block = c_buf[l, first : first + group].reshape(group * rows, zw)
            for core in range(2):
                part = jnp.dot(block, w_out[l, core], preferred_element_type=F32).astype(BF16)
                d_out[l, first : first + group, core] = part.reshape(group, rows, width_f)
            for k in range(first, first + group):
                z = 2 * x_at(k) + my_core
                for core in range(2):
                    mine = (z == my_tp) & (my_core == core)

                    @pl.when(jnp.logical_not(mine))
                    def _(k=k, core=core, l=l):
                        copy_d(l, k, core).start()

                    @pl.when(mine)
                    def _(k=k, core=core, l=l):
                        d_in[l, my_tp] = d_out[l, k, core]

        xs_t = xs.T
        for s in range(rows):
            for h in range(heads_here):
                b_row = bc[s : s + 1, 0:bw]
                xs_col = xs_t[h * hd : (h + 1) * hd, s : s + 1]
                ssm_o[l, s, h] = ssm[l, s, h] * decay[s : s + 1, h : h + 1] + xs_col * b_row
        for k in range(taps - 2):
            nx_o[l, k] = s_x[l, k + 1]
            nb_o[l, k] = s_b[l, k + 1]
            nc_o[l, k] = s_c[l, k + 1]
        nx_o[l, taps - 2] = x_new
        nb_o[l, taps - 2] = bc_new[:, 0:bw]
        nc_o[l, taps - 2] = bc_new[:, bw : 2 * bw]

        sent_abc(l)
        if l > 0:
            sent_d(l - 1)

        @pl.when(uneven)
        def _(l=l):
            got = d_in.at[l, my_tp]
            remote(got, got, l, 3, 0, my_tp, column(my_tp, row_core)).wait_recv()

        projected = d_in[l, my_tp].astype(F32)
        for k in range(1, tp_n):
            z = tp_at(k)
            got = d_in.at[l, z]
            remote(got, got, l, 3, k, z, column(z, row_core)).wait_recv()
            projected = projected + d_in[l, z].astype(F32)
        new = (r_buf[l].astype(F32) + projected).astype(BF16)
        if l + 1 < layers:
            r_buf[l + 1] = new
        else:
            res_o[...] = new

    sent_d(layers - 1)
    for p in pair:
        p.wait_send()


def write_out(*refs):
    sem = refs[-1]
    half = len(refs) // 2
    copies = []
    for n in range(half):
        cuts = refs[n].shape[1] // 4 if len(refs[n].shape) == 5 else 0
        for at in range(4 * refs[n].shape[0]) if cuts else (None,):
            src, dst = refs[n], refs[half + n]
            if cuts:
                part = pl.ds(at % 4 * cuts, cuts)
                src, dst = src.at[at // 4, part], dst.at[at // 4, part]
            copies.append(pltpu.make_async_copy(src, dst, sem.at[len(copies)]))
    for c in copies:
        c.start()
    for c in copies:
        c.wait()


def body(tp_n, dp_n, *args):
    (
        tokens,
        norm_gain,
        w_z,
        w_x,
        w_b,
        w_c,
        w_dt,
        conv_x,
        conv_b,
        conv_c,
        dt_bias,
        a_log,
        d_skip,
        out_gain,
        w_out,
        ssm_state,
        state_x,
        state_b,
        state_c,
    ) = args
    layers, heads_here = dt_bias.shape
    rows, width_f = tokens.shape
    zw, bw = w_z.shape[2], w_b.shape[2]
    assert tp_n == dp_n and 2 * bw == LANES
    wide = 2 * zw + 2 * LANES
    half = tp_n // 2

    def turn(a):
        return jnp.swapaxes(a, 1, 2)

    operands = (
        tokens,
        w_z,
        w_x,
        w_out,
        norm_gain,
        turn(w_b),
        turn(w_c),
        turn(w_dt),
        conv_x,
        conv_b,
        conv_c,
        dt_bias,
        a_log,
        d_skip,
        out_gain,
        ssm_state,
        turn(state_x),
        turn(state_b),
        turn(state_c),
    )
    vmem = pl.BlockSpec(memory_space=pltpu.VMEM)
    hbm = pl.BlockSpec(memory_space=pltpu.HBM)

    def like(a):
        return pltpu.VMEM(a.shape, a.dtype)

    results = pl.pallas_call(
        functools.partial(kernel, tp_n, dp_n, width_f * dp_n),
        out_shape=(
            like(tokens),
            like(ssm_state),
            like(operands[16]),
            like(operands[17]),
            like(operands[18]),
        ),
        in_specs=[hbm] * INPUTS,
        out_specs=(vmem,) * 5,
        scratch_shapes=[
            pltpu.VMEM((layers, half, 2, rows, width_f), BF16),
            pltpu.VMEM((layers, half, rows, wide), BF16),
            pltpu.VMEM((layers, half, rows, wide), BF16),
            pltpu.VMEM((layers, rows, zw), BF16),
            pltpu.VMEM((layers, half, rows, zw), BF16),
            pltpu.VMEM((layers, half, 2, rows, width_f), BF16),
            pltpu.VMEM((layers, tp_n, rows, width_f), BF16),
            pltpu.VMEM((layers, rows, width_f), BF16),
            pltpu.VMEM((layers, 2, width_f, zw), BF16),
            pltpu.VMEM((layers, 2, width_f, zw), BF16),
            pltpu.VMEM((layers, 2, zw, width_f), BF16),
            pltpu.VMEM((layers, 2, 2 * LANES, width_f), BF16),
            pltpu.VMEM((2, 8, width_f), F32),
            pltpu.VMEM((layers, conv_x.shape[1], LANES), F32),
            pltpu.VMEM((layers, state_b.shape[2], rows, LANES), F32),
            pltpu.VMEM((layers, rows, bw, zw), BF16),
            *(pltpu.VMEM(a.shape, a.dtype) for a in operands[4:]),
            pltpu.SemaphoreType.DMA((INPUTS - 3 + 3 * layers,)),
            pltpu.SemaphoreType.DMA((2, 1 + 4 * layers)),
            pltpu.SemaphoreType.DMA((layers, 5, tp_n)),
            pltpu.SemaphoreType.DMA((layers, 5, tp_n)),
        ],
        compiler_params=pltpu.CompilerParams(
            collective_id=0, has_side_effects=True, vmem_limit_bytes=40 * 1024 * 1024
        ),
        name="decode",
    )(*(pltpu.with_memory_space_constraint(a, pltpu.HBM) for a in operands))
    results = [pltpu.with_memory_space_constraint(a, pltpu.VMEM) for a in results]
    residual, ssm_next, next_x, next_b, next_c = pl.pallas_call(
        write_out,
        out_shape=tuple(jax.ShapeDtypeStruct(a.shape, a.dtype) for a in results),
        in_specs=(vmem,) * 5,
        out_specs=(hbm,) * 5,
        scratch_shapes=[pltpu.SemaphoreType.DMA((4 + 4 * layers,))],
        compiler_params=pltpu.CompilerParams(vmem_limit_bytes=8 * 1024 * 1024),
        name="write_out",
    )(*results)
    return residual, ssm_next, turn(next_x), turn(next_b), turn(next_c)


def solution(mesh):
    placed = (
        P(("grp", "tp"), "dp"),
        P(None, "dp"),
        P(None, "dp", "tp"),
        P(None, "dp", "tp"),
        P(None, "dp", "tp"),
        P(None, "dp", "tp"),
        P(None, "dp", None),
        P(None, None, "tp"),
        P(None, None, "tp"),
        P(None, None, "tp"),
        P(None, "tp"),
        P(None, "tp"),
        P(None, "tp"),
        P(None, "tp"),
        P(None, "tp", "dp"),
        P(None, ("grp", "dp"), "tp", None, None),
        P(None, ("grp", "dp"), None, "tp"),
        P(None, ("grp", "dp"), None, "tp"),
        P(None, ("grp", "dp"), None, "tp"),
    )
    return jax.shard_map(
        functools.partial(body, mesh.shape["tp"], mesh.shape["dp"]),
        mesh=mesh,
        in_specs=placed,
        out_specs=(placed[0], placed[15], placed[16], placed[17], placed[18]),
        check_vma=False,
    )
```

```python
import functools

import jax
import jax.numpy as jnp
from jax import lax
from jax.experimental import pallas as pl
from jax.experimental.pallas import tpu as pltpu
from jax.sharding import PartitionSpec as P

EPSILON = 1e-05
F32 = jnp.float32
BF16 = jnp.bfloat16
MESH = pl.DeviceIdType.MESH
NT = (((1,), (1,)), ((), ()))
LANES = 128
INPUTS = 19
GROUP = 4


def silu(v):
    return v * jax.nn.sigmoid(v)


def kernel(
    tp_n,
    dp_n,
    features,
    *refs,
):
    held, refs = refs[:INPUTS], refs[INPUTS:]
    res_o, ssm_o, nx_o, nb_o, nc_o = refs[:5]
    a_buf, b_out, b_in, c_own, c_buf, d_out, d_in, r_buf = refs[5:13]
    w_z, w_x, w_out, w_bcd, gains, conv_bc, s_bc, st_t = refs[13:21]
    here = refs[21 : 17 + INPUTS]
    d_far, r_far, local_sem, pair_sem, send_sem, recv_sem = refs[17 + INPUTS :]
    (
        gain,
        w_bt,
        w_ct,
        w_dtt,
        conv_x,
        conv_b,
        conv_c,
        dt_bias,
        a_log,
        d_skip,
        out_gain,
        ssm,
        s_x,
        s_b,
        s_c,
    ) = here
    layers, heads_here = dt_bias.shape
    rows, width_f = res_o.shape
    zw = w_z.shape[3]
    bw = w_bt.shape[1]
    hd = zw // heads_here
    my_tp, my_dp = lax.axis_index("tp"), lax.axis_index("dp")
    my_x, my_core = lax.div(my_dp, 2), lax.rem(my_dp, 2)
    half, near = tp_n // 2, tp_n // 4
    uneven = lax.rem(my_tp + my_core, 2) == 1
    row_core = lax.rem(my_tp, 2)

    def nearest(k, n):
        return (k + 1) // 2 if k % 2 else (n - k // 2) % n

    def place(distance, n):
        return jnp.where(distance <= n // 2, jnp.maximum(2 * distance - 1, 0), 2 * (n - distance))

    def tp_at(k):
        return lax.rem(my_tp + nearest(k, tp_n), tp_n)

    def x_at(k):
        return lax.rem(my_x + nearest(k, half), half)

    def rows_at(k):
        odd = tp_n - k if k % 2 else k + 1
        return lax.rem(my_tp + jnp.where(uneven, odd, 2 * nearest(k, half)), tp_n)

    def rows_place(offset):
        odd = jnp.where(offset < half, offset - 1, tp_n - offset)
        return jnp.where(lax.rem(offset, 2) == 1, odd, place(lax.div(offset, 2), half))

    def sent_place(k):
        offset = (tp_n - nearest(k, tp_n)) % tp_n
        if offset % 2:
            return offset - 1 if offset < half else tp_n - offset
        distance = offset // 2
        return max(2 * distance - 1, 0) if 2 * distance <= half else 2 * (half - distance)

    def x_mirror(k):
        if k == 0 or (k == half - 1 and half % 2 == 0):
            return k
        return k + 1 if k % 2 else k - 1

    k_rows = rows_place(lax.rem(my_dp - my_tp + tp_n, tp_n))

    def remote(src, dst, layer, phase, s_slot, r_slot, target):
        return pltpu.make_async_remote_copy(
            src_ref=src,
            dst_ref=dst,
            send_sem=send_sem.at[layer, phase, s_slot],
            recv_sem=recv_sem.at[layer, phase, r_slot],
            device_id=target,
            device_id_type=MESH,
        )

    def column(z, core):
        return {"tp": z, "dp": 2 * my_x + core}

    def row(x):
        return {"dp": 2 * x + my_core}

    layer_list = range(layers)
    fetch = [pltpu.make_async_copy(held[0], r_buf.at[0], local_sem.at[0])]
    used = 1
    for n in range(3):
        whole = (w_z, w_x, w_out)[n]
        for l in layer_list:
            fetch.append(
                pltpu.make_async_copy(
                    held[1 + n].at[l], whole.at[l, my_core], local_sem.at[used]
                )
            )
            used += 1
    for n in range(4, INPUTS):
        fetch.append(pltpu.make_async_copy(held[n], here[n - 4], local_sem.at[used]))
        used += 1
    fetch[0].start()
    barrier = pltpu.get_barrier_semaphore()

    def greet(device):
        pl.semaphore_signal(barrier, inc=1, device_id=device, device_id_type=MESH)

    for k in range(2 * near, 0, -1):
        greet(column(tp_at(k), 0))
        greet(column(tp_at(k), 1))
    for k in range(half - 1, 0, -1):
        greet(row(x_at(k)))
    greet(column(my_tp, 1 - my_core))
    for f in fetch[1:]:
        f.start()

    def copy_a(l, k):
        if k == 0:
            dst = a_buf.at[l, 0, my_core]
            return remote(r_buf.at[l], dst, l, 0, 0, my_core, column(my_tp, row_core))
        slot = sent_place(k)
        dst = a_buf.at[l, slot, my_core]
        return remote(r_buf.at[l], dst, l, 0, k, 2 * slot + my_core, column(tp_at(k), row_core))

    def copy_a2(l, n):
        steps = [(s, False) for s in range(-near, near + 1)]
        steps += [(s, True) for s in range(1 - near, near)]
        s, far = steps[n]
        offset = -s if not far else (half - s if s >= 0 else -half - s)
        slot = offset - 1 if offset > 0 else -offset
        src = r_far.at[1] if far else r_buf.at[l]
        dst = a_buf.at[l, slot, my_core]
        to = column(lax.rem(my_tp + s + tp_n, tp_n), row_core)
        return s, remote(src, dst, l, 0, n, 2 * slot + my_core, to)

    def each_a(l, act):
        if l == 0:
            copies = [(k, copy_a(l, k)) for k in range(2 * near, -1, -1)]
        else:
            copies = [copy_a2(l, n) for n in range(tp_n)]
        for s, copy in copies:
            if s != 0:
                act(copy)

        @pl.when(uneven)
        def _():
            for s, copy in copies:
                if s == 0:
                    act(copy)

    def send_a(l):
        each_a(l, lambda copy: copy.start())

        @pl.when(jnp.logical_not(uneven))
        def _():
            a_buf[l, 0, my_core] = r_buf[l]
            if l > 0:
                a_buf[l, half - 1, my_core] = r_far[1]

    def offset_of(odd, k):
        if odd:
            return -k if k % 2 else k + 1
        return -k if k % 2 == 0 else k + 1

    def relayed(odd, down):
        offsets = [offset_of(odd, k) for k in range(half)]
        step = near if down else -near
        return [
            (offsets.index(o - step), k)
            for k, o in enumerate(offsets)
            if (o > near if down else o < -near)
        ]

    def copy_relay(source, target, down):
        z = lax.rem(my_tp + (tp_n - near if down else near), tp_n)
        src, dst = a_buf.at[0, source], a_buf.at[0, target]
        return remote(src, dst, 0, 4, target, target, column(z, my_core))

    def relay(odd, down):
        for source, target in relayed(odd, down):
            for core in range(2):
                got = a_buf.at[0, source, core]
                remote(
                    got, got, 0, 0, 0, 2 * source + core, column(rows_at(source), core)
                ).wait_recv()
            copy_relay(source, target, down).start()

    def wait_first_a(odd, k):
        if abs(offset_of(odd, k)) > near:
            copy_relay(k, k, 0).wait_recv()
        elif k not in [source for down in range(2) for source, _ in relayed(odd, down)]:
            for core in range(2):
                got = a_buf.at[0, k, core]
                copy = remote(got, got, 0, 0, k, 2 * k + core, column(rows_at(k), core))
                if offset_of(odd, k) != 0:
                    copy.wait_recv()
                else:

                    @pl.when(my_core != core)
                    def _(copy=copy):
                        copy.wait_recv()

    def copy_b(l, k):
        to = row(lax.div(rows_at(k), 2))
        return remote(b_out.at[l, k], b_in.at[l, my_x], l, 1, k, my_x, to)

    def copy_c(l, k):
        slot = x_mirror(k)
        return remote(c_own.at[l], c_buf.at[l, slot], l, 2, k, slot, row(x_at(k)))

    def copy_d(l, k, core):
        to = column(2 * x_at(k) + my_core, core)
        return remote(d_out.at[l, k, core], d_in.at[l, my_tp], l, 3, 2 * k + core, my_tp, to)

    def copy_d2(l, k, core):
        z = lax.rem(2 * x_at(k) + my_core + half, tp_n)
        src, dst = d_out.at[l, k, core], d_far.at[my_tp]
        return z, remote(src, dst, l, 5, 2 * k + core, my_tp, column(z, core))

    def copy_far():
        src = a_buf.at[0, half - 1, 1 - my_core]
        return remote(src, r_far.at[0], 0, 6, 0, 0, column(my_tp, 1 - my_core))

    def sent_abc(l):
        each_a(l, lambda copy: copy.wait_send())

        if l == 0:
            for odd in range(2):

                @pl.when(uneven == (odd == 1))
                def _(odd=odd):
                    for down in range(2):
                        for source, target in relayed(odd, down):
                            copy_relay(source, target, down).wait_send()

        for k in range(half):

            @pl.when(rows_at(k) != my_dp)
            def _(k=k):
                copy_b(l, k).wait_send()

            if k > 0:
                copy_c(l, k).wait_send()

    def sent_d(l):
        for k in range(half):
            for core in range(2):

                @pl.when(jnp.logical_not((2 * x_at(k) + my_core == my_tp) & (my_core == core)))
                def _(k=k, core=core):
                    copy_d(l, k, core).wait_send()

                if l + 1 < layers:
                    z, copy = copy_d2(l, k, core)

                    @pl.when(jnp.logical_not((z == my_tp) & (my_core == core)))
                    def _(copy=copy):
                        copy.wait_send()

    pl.semaphore_wait(barrier, 4 * near + 1 + half - 1)
    fetch[0].wait()
    send_a(0)

    for f in fetch[1:]:
        f.wait()
    heads_all = w_dtt.shape[1]
    pick = lax.broadcasted_iota(jnp.int32, (16, heads_all), 0)
    col = lax.broadcasted_iota(jnp.int32, (16, heads_all), 1)
    pick = jnp.where((pick < heads_here) & (col == pick + my_tp * heads_here), 1.0, 0.0).astype(BF16)
    for l in range(layers):
        w_bcd[l, my_core, 0:bw] = w_bt[l]
        w_bcd[l, my_core, bw : 2 * bw] = w_ct[l]
        w_bcd[l, my_core, 2 * bw : 2 * bw + 16] = jnp.dot(
            pick, w_dtt[l], preferred_element_type=F32
        ).astype(BF16)
        w_bcd[l, my_core, 2 * bw + 16 :] = jnp.zeros(
            (w_bcd.shape[2] - 2 * bw - 16, width_f), BF16
        )
        conv_bc[l] = jnp.concatenate([conv_b[l].astype(F32), conv_c[l].astype(F32)], axis=1)
        for k in range(s_b.shape[1]):
            s_bc[l, k] = jnp.concatenate([s_b[l, k].astype(F32), s_c[l, k].astype(F32)], axis=1)

    gains[my_core] = jnp.zeros(gains.shape[1:], F32)
    gains[my_core, 0:layers] = gain[...].astype(F32)

    pair = []
    for whole in [gains.at[my_core]] + [
        w.at[l, my_core] for l in layer_list for w in (w_z, w_x, w_bcd, w_out)
    ]:
        pair.append(
            pltpu.make_async_remote_copy(
                src_ref=whole,
                dst_ref=whole,
                send_sem=pair_sem.at[0, len(pair)],
                recv_sem=pair_sem.at[1, len(pair)],
                device_id=column(my_tp, 1 - my_core),
                device_id_type=MESH,
            )
        )
    for p in pair:
        p.start()

    down_first = my_tp < half
    for odd in range(2):
        for order in ((0, 1), (1, 0)):

            @pl.when((uneven == (odd == 1)) & (down_first == (order[0] == 1)))
            def _(odd=odd, order=order):
                for down in order:
                    relay(odd, down)

    def turn(i, carry):
        for l in range(layers):
            block = ssm[l, i].reshape(zw, bw)
            st_t[l, i] = block.T.astype(BF16)
        return carry

    lane = lax.broadcasted_iota(jnp.int32, (rows, LANES), 1)
    head_of = lax.broadcasted_iota(jnp.int32, (rows, zw), 1)
    head_of = lax.div(head_of, hd)

    def per_head(v):
        out = jnp.broadcast_to(v[:, 0:1], (rows, zw))
        for h in range(1, heads_here):
            out = jnp.where(head_of == h, v[:, h : h + 1], out)
        return out

    for l in range(layers):
        if l > 0:
            send_a(l)

        for first in range(0, half, GROUP):
            group = min(GROUP, half)
            if l == 0:
                for odd in range(2):

                    @pl.when(uneven == (odd == 1))
                    def _(odd=odd, first=first, group=group):
                        for k in range(first, first + group):
                            wait_first_a(odd, k)

            else:
                for k in range(first, first + group):
                    for core in range(2):
                        got = a_buf.at[l, k, core]
                        copy = remote(got, got, l, 0, k, 2 * k + core, column(rows_at(k), core))
                        if k not in (0, half - 1):
                            copy.wait_recv()
                        else:

                            @pl.when(uneven | (my_core != core))
                            def _(copy=copy):
                                copy.wait_recv()

            if l == 0 and first == 0:
                for p in pair:
                    p.wait_recv()
            tall = group * rows
            scaled, squares = [], 0.0
            for core in range(2):
                block = a_buf[l, first : first + group, core].reshape(tall, width_f).astype(F32)
                scaled.append((block * gains[core, l : l + 1]).astype(BF16))
                squares = squares + jnp.sum(block * block, axis=1, keepdims=True)
            both_wide = jnp.concatenate(scaled, axis=1)
            part_z = jnp.dot(
                both_wide, w_z[l].reshape(2 * width_f, zw), preferred_element_type=F32
            ).astype(BF16)
            part_x = jnp.dot(
                both_wide, w_x[l].reshape(2 * width_f, zw), preferred_element_type=F32
            ).astype(BF16)
            rest = lax.dot_general(scaled[0], w_bcd[l, 0], NT, preferred_element_type=F32)
            rest += lax.dot_general(scaled[1], w_bcd[l, 1], NT, preferred_element_type=F32)
            lane_tall = lax.broadcasted_iota(jnp.int32, (tall, LANES), 1)
            small = jnp.where(lane_tall == heads_here, squares, rest[:, LANES:])
            low = small - small.astype(BF16).astype(F32)
            both = jnp.where(lane_tall < LANES // 2, small, pltpu.roll(low, LANES // 2, 1))
            b_out[l, first : first + group, :, 0:zw] = part_z.reshape(group, rows, zw)
            b_out[l, first : first + group, :, zw : 2 * zw] = part_x.reshape(group, rows, zw)
            b_out[l, first : first + group, :, 2 * zw : 2 * zw + LANES] = (
                rest[:, 0:LANES].astype(BF16).reshape(group, rows, LANES)
            )
            b_out[l, first : first + group, :, 2 * zw + LANES :] = both.astype(BF16).reshape(
                group, rows, LANES
            )
            for k in range(first, first + group):

                @pl.when(rows_at(k) != my_dp)
                def _(k=k, l=l):
                    copy_b(l, k).start()

        if l == 0:

            @pl.when(jnp.logical_not(uneven))
            def _():
                copy_far().start()
                r_far[0] = a_buf[0, half - 1, my_core]

            lax.fori_loop(0, rows, turn, 0)
        total = b_out[l, k_rows].astype(F32)
        for k in range(1, half):
            x = x_at(k)
            remote(b_in.at[l, x], b_in.at[l, x], l, 1, k, x, row(x)).wait_recv()
            total = total + b_in[l, x].astype(F32)

        small = total[:, 2 * zw + LANES :]
        small = small + pltpu.roll(small, LANES // 2, 1)
        row_scale = lax.rsqrt(small[:, heads_here : heads_here + 1] / features + EPSILON)
        step_raw = small[:, 0:heads_here] * row_scale
        gate = (total[:, 0:zw] * row_scale).astype(BF16).astype(F32)
        x_new = (total[:, zw : 2 * zw] * row_scale).astype(BF16)
        bc_new = (total[:, 2 * zw : 2 * zw + LANES] * row_scale).astype(BF16)
        taps = conv_x.shape[1]
        conv = x_new.astype(F32) * conv_x[l, taps - 1 : taps].astype(F32)
        conv2 = bc_new.astype(F32) * conv_bc[l, taps - 1 : taps]
        for k in range(taps - 1):
            conv = conv + s_x[l, k].astype(F32) * conv_x[l, k : k + 1].astype(F32)
            conv2 = conv2 + s_bc[l, k] * conv_bc[l, k : k + 1]
        v = silu(conv)
        bc = silu(conv2)
        step = jax.nn.softplus(step_raw + dt_bias[l : l + 1])
        decay = jnp.exp(-step * jnp.exp(a_log[l : l + 1]))
        xs = per_head(step) * v
        turned = pltpu.roll(bc, LANES // 2, 1)
        b_dot_c = 0.5 * jnp.sum(bc * turned, axis=1, keepdims=True)
        cc = jnp.where(lane < LANES // 2, turned, bc)
        seq = lax.broadcasted_iota(jnp.int32, (rows, LANES), 0)
        pieces = []
        for s in range(0, rows, 2):
            pieces.append(jnp.where(seq == s + lax.div(lane, LANES // 2), cc, 0.0).astype(BF16))
        spread = jnp.concatenate(pieces, axis=1)
        reads = jnp.dot(
            spread, st_t[l].reshape(rows * bw, zw), preferred_element_type=F32
        )
        readout = per_head(decay) * reads + (xs * b_dot_c + per_head(d_skip[l : l + 1]) * v)
        gated = readout * silu(gate)
        scale = lax.rsqrt(jnp.mean(gated * gated, axis=1, keepdims=True) + EPSILON)
        mixed = (gated * scale * out_gain[l : l + 1].astype(F32)).astype(BF16)

        c_own[l] = mixed
        c_buf[l, 0] = mixed

        for k in range(half - 1, 0, -1):
            copy_c(l, k).start()

        for first in range(0, half, GROUP):
            group = min(GROUP, half)
            for k in range(max(first, 1), first + group):
                got = c_buf.at[l, k]
                remote(got, got, l, 2, k, k, row(x_at(k))).wait_recv()
            block = c_buf[l, first : first + group].reshape(group * rows, zw)
            for core in range(2):
                part = jnp.dot(block, w_out[l, core], preferred_element_type=F32).astype(BF16)
                d_out[l, first : first + group, core] = part.reshape(group, rows, width_f)
            for k in range(first, first + group):
                z = 2 * x_at(k) + my_core
                for core in range(2):
                    mine = (z == my_tp) & (my_core == core)

                    @pl.when(jnp.logical_not(mine))
                    def _(k=k, core=core, l=l):
                        copy_d(l, k, core).start()

                    @pl.when(mine)
                    def _(k=k, core=core, l=l):
                        d_in[l, my_tp] = d_out[l, k, core]

                    if l + 1 < layers:
                        z2, copy = copy_d2(l, k, core)
                        mine2 = (z2 == my_tp) & (my_core == core)

                        @pl.when(jnp.logical_not(mine2))
                        def _(copy=copy):
                            copy.start()

                        @pl.when(mine2)
                        def _(k=k, core=core, l=l):
                            d_far[my_tp] = d_out[l, k, core]

        xs_t = xs.T
        for s in range(rows):
            for h in range(heads_here):
                b_row = bc[s : s + 1, 0:bw]
                xs_col = xs_t[h * hd : (h + 1) * hd, s : s + 1]
                ssm_o[l, s, h] = ssm[l, s, h] * decay[s : s + 1, h : h + 1] + xs_col * b_row
        for k in range(taps - 2):
            nx_o[l, k] = s_x[l, k + 1]
            nb_o[l, k] = s_b[l, k + 1]
            nc_o[l, k] = s_c[l, k + 1]
        nx_o[l, taps - 2] = x_new
        nb_o[l, taps - 2] = bc_new[:, 0:bw]
        nc_o[l, taps - 2] = bc_new[:, bw : 2 * bw]

        sent_abc(l)
        if l > 0:
            sent_d(l - 1)

        @pl.when(uneven)
        def _(l=l):
            got = d_in.at[l, my_tp]
            remote(got, got, l, 3, 0, my_tp, column(my_tp, row_core)).wait_recv()

        projected = d_in[l, my_tp].astype(F32)
        for k in range(1, tp_n):
            z = tp_at(k)
            got = d_in.at[l, z]
            remote(got, got, l, 3, k, z, column(z, row_core)).wait_recv()
            projected = projected + d_in[l, z].astype(F32)
        new = (r_buf[l].astype(F32) + projected).astype(BF16)
        if l + 1 < layers:
            r_buf[l + 1] = new

            @pl.when(uneven)
            def _(l=l):
                copy_far().wait_recv()
                got = d_far.at[my_tp]
                remote(got, got, l, 5, 0, my_tp, column(my_tp, row_core)).wait_recv()

            @pl.when(jnp.logical_not(uneven))
            def _():
                copy_far().wait_send()

            projected = d_far[my_tp].astype(F32)
            for k in range(1, tp_n):
                z = tp_at(k)
                got = d_far.at[z]
                remote(got, got, l, 5, k, z, column(z, row_core)).wait_recv()
                projected = projected + d_far[z].astype(F32)
            r_far[1] = (r_far[0].astype(F32) + projected).astype(BF16)
        else:
            res_o[...] = new

    sent_d(layers - 1)
    for p in pair:
        p.wait_send()


def write_out(*refs):
    sem = refs[-1]
    half = len(refs) // 2
    copies = []
    for n in range(half):
        cuts = refs[n].shape[1] // 4 if len(refs[n].shape) == 5 else 0
        for at in range(4 * refs[n].shape[0]) if cuts else (None,):
            src, dst = refs[n], refs[half + n]
            if cuts:
                part = pl.ds(at % 4 * cuts, cuts)
                src, dst = src.at[at // 4, part], dst.at[at // 4, part]
            copies.append(pltpu.make_async_copy(src, dst, sem.at[len(copies)]))
    for c in copies:
        c.start()
    for c in copies:
        c.wait()


def body(tp_n, dp_n, *args):
    (
        tokens,
        norm_gain,
        w_z,
        w_x,
        w_b,
        w_c,
        w_dt,
        conv_x,
        conv_b,
        conv_c,
        dt_bias,
        a_log,
        d_skip,
        out_gain,
        w_out,
        ssm_state,
        state_x,
        state_b,
        state_c,
    ) = args
    layers, heads_here = dt_bias.shape
    rows, width_f = tokens.shape
    zw, bw = w_z.shape[2], w_b.shape[2]
    assert tp_n == dp_n and layers == 2 and tp_n % 8 == 0 and 2 * bw == LANES
    wide = 2 * zw + 2 * LANES
    half = tp_n // 2

    def turn(a):
        return jnp.swapaxes(a, 1, 2)

    operands = (
        tokens,
        w_z,
        w_x,
        w_out,
        norm_gain,
        turn(w_b),
        turn(w_c),
        turn(w_dt),
        conv_x,
        conv_b,
        conv_c,
        dt_bias,
        a_log,
        d_skip,
        out_gain,
        ssm_state,
        turn(state_x),
        turn(state_b),
        turn(state_c),
    )
    vmem = pl.BlockSpec(memory_space=pltpu.VMEM)
    hbm = pl.BlockSpec(memory_space=pltpu.HBM)

    def like(a):
        return pltpu.VMEM(a.shape, a.dtype)

    results = pl.pallas_call(
        functools.partial(kernel, tp_n, dp_n, width_f * dp_n),
        out_shape=(
            like(tokens),
            like(ssm_state),
            like(operands[16]),
            like(operands[17]),
            like(operands[18]),
        ),
        in_specs=[hbm] * INPUTS,
        out_specs=(vmem,) * 5,
        scratch_shapes=[
            pltpu.VMEM((layers, half, 2, rows, width_f), BF16),
            pltpu.VMEM((layers, half, rows, wide), BF16),
            pltpu.VMEM((layers, half, rows, wide), BF16),
            pltpu.VMEM((layers, rows, zw), BF16),
            pltpu.VMEM((layers, half, rows, zw), BF16),
            pltpu.VMEM((layers, half, 2, rows, width_f), BF16),
            pltpu.VMEM((layers, tp_n, rows, width_f), BF16),
            pltpu.VMEM((layers, rows, width_f), BF16),
            pltpu.VMEM((layers, 2, width_f, zw), BF16),
            pltpu.VMEM((layers, 2, width_f, zw), BF16),
            pltpu.VMEM((layers, 2, zw, width_f), BF16),
            pltpu.VMEM((layers, 2, 2 * LANES, width_f), BF16),
            pltpu.VMEM((2, 8, width_f), F32),
            pltpu.VMEM((layers, conv_x.shape[1], LANES), F32),
            pltpu.VMEM((layers, state_b.shape[2], rows, LANES), F32),
            pltpu.VMEM((layers, rows, bw, zw), BF16),
            *(pltpu.VMEM(a.shape, a.dtype) for a in operands[4:]),
            pltpu.VMEM((tp_n, rows, width_f), BF16),
            pltpu.VMEM((2, rows, width_f), BF16),
            pltpu.SemaphoreType.DMA((INPUTS - 3 + 3 * layers,)),
            pltpu.SemaphoreType.DMA((2, 1 + 4 * layers)),
            pltpu.SemaphoreType.DMA((layers, 7, tp_n)),
            pltpu.SemaphoreType.DMA((layers, 7, tp_n)),
        ],
        compiler_params=pltpu.CompilerParams(
            collective_id=0, has_side_effects=True, vmem_limit_bytes=40 * 1024 * 1024
        ),
        name="decode",
    )(*(pltpu.with_memory_space_constraint(a, pltpu.HBM) for a in operands))
    results = [pltpu.with_memory_space_constraint(a, pltpu.VMEM) for a in results]
    residual, ssm_next, next_x, next_b, next_c = pl.pallas_call(
        write_out,
        out_shape=tuple(jax.ShapeDtypeStruct(a.shape, a.dtype) for a in results),
        in_specs=(vmem,) * 5,
        out_specs=(hbm,) * 5,
        scratch_shapes=[pltpu.SemaphoreType.DMA((4 + 4 * layers,))],
        compiler_params=pltpu.CompilerParams(vmem_limit_bytes=8 * 1024 * 1024),
        name="write_out",
    )(*results)
    return residual, ssm_next, turn(next_x), turn(next_b), turn(next_c)


def solution(mesh):
    placed = (
        P(("grp", "tp"), "dp"),
        P(None, "dp"),
        P(None, "dp", "tp"),
        P(None, "dp", "tp"),
        P(None, "dp", "tp"),
        P(None, "dp", "tp"),
        P(None, "dp", None),
        P(None, None, "tp"),
        P(None, None, "tp"),
        P(None, None, "tp"),
        P(None, "tp"),
        P(None, "tp"),
        P(None, "tp"),
        P(None, "tp"),
        P(None, "tp", "dp"),
        P(None, ("grp", "dp"), "tp", None, None),
        P(None, ("grp", "dp"), None, "tp"),
        P(None, ("grp", "dp"), None, "tp"),
        P(None, ("grp", "dp"), None, "tp"),
    )
    return jax.shard_map(
        functools.partial(body, mesh.shape["tp"], mesh.shape["dp"]),
        mesh=mesh,
        in_specs=placed,
        out_specs=(placed[0], placed[15], placed[16], placed[17], placed[18]),
        check_vma=False,
    )
```

```python
import functools

import jax
import jax.numpy as jnp
from jax import lax
from jax.experimental import pallas as pl
from jax.experimental.pallas import tpu as pltpu
from jax.sharding import PartitionSpec as P

EPSILON = 1e-05
F32 = jnp.float32
BF16 = jnp.bfloat16
MESH = pl.DeviceIdType.MESH
NT = (((1,), (1,)), ((), ()))
LANES = 128
INPUTS = 19
GROUP = 2


def silu(v):
    return v * jax.nn.sigmoid(v)


def kernel(
    tp_n,
    dp_n,
    features,
    *refs,
):
    held, refs = refs[:INPUTS], refs[INPUTS:]
    res_o, ssm_o, nx_o, nb_o, nc_o = refs[:5]
    a_buf, b_out, b_in, c_own, c_buf, d_out, d_in, r_buf = refs[5:13]
    w_z, w_x, w_out, w_bcd, gains, conv_bc, s_bc, st_t = refs[13:21]
    here = refs[21 : 17 + INPUTS]
    local_sem, pair_sem, send_sem, recv_sem = refs[17 + INPUTS :]
    (
        gain,
        w_bt,
        w_ct,
        w_dtt,
        conv_x,
        conv_b,
        conv_c,
        dt_bias,
        a_log,
        d_skip,
        out_gain,
        ssm,
        s_x,
        s_b,
        s_c,
    ) = here
    layers, heads_here = dt_bias.shape
    rows, width_f = res_o.shape
    zw = w_z.shape[3]
    bw = w_bt.shape[1]
    hd = zw // heads_here
    my_tp, my_dp = lax.axis_index("tp"), lax.axis_index("dp")
    my_x, my_core = lax.div(my_dp, 2), lax.rem(my_dp, 2)
    half, near = tp_n // 2, tp_n // 4
    uneven = lax.rem(my_tp + my_core, 2) == 1
    row_core = lax.rem(my_tp, 2)

    def nearest(k, n):
        return (k + 1) // 2 if k % 2 else (n - k // 2) % n

    def place(distance, n):
        return jnp.where(distance <= n // 2, jnp.maximum(2 * distance - 1, 0), 2 * (n - distance))

    def tp_at(k):
        return lax.rem(my_tp + nearest(k, tp_n), tp_n)

    def x_at(k):
        return lax.rem(my_x + nearest(k, half), half)

    def rows_at(k):
        odd = tp_n - k if k % 2 else k + 1
        return lax.rem(my_tp + jnp.where(uneven, odd, 2 * nearest(k, half)), tp_n)

    def rows_place(offset):
        odd = jnp.where(offset < half, offset - 1, tp_n - offset)
        return jnp.where(lax.rem(offset, 2) == 1, odd, place(lax.div(offset, 2), half))

    def sent_place(k):
        offset = (tp_n - nearest(k, tp_n)) % tp_n
        if offset % 2:
            return offset - 1 if offset < half else tp_n - offset
        distance = offset // 2
        return max(2 * distance - 1, 0) if 2 * distance <= half else 2 * (half - distance)

    def x_mirror(k):
        if k == 0 or (k == half - 1 and half % 2 == 0):
            return k
        return k + 1 if k % 2 else k - 1

    k_rows = rows_place(lax.rem(my_dp - my_tp + tp_n, tp_n))

    def remote(src, dst, layer, phase, s_slot, r_slot, target):
        return pltpu.make_async_remote_copy(
            src_ref=src,
            dst_ref=dst,
            send_sem=send_sem.at[layer, phase, s_slot],
            recv_sem=recv_sem.at[layer, phase, r_slot],
            device_id=target,
            device_id_type=MESH,
        )

    def column(z, core):
        return {"tp": z, "dp": 2 * my_x + core}

    def row(x):
        return {"dp": 2 * x + my_core}

    layer_list = range(layers)
    fetch = [pltpu.make_async_copy(held[0], r_buf.at[0], local_sem.at[0])]
    used = 1
    for n in range(3):
        whole = (w_z, w_x, w_out)[n]
        for l in layer_list:
            fetch.append(
                pltpu.make_async_copy(
                    held[1 + n].at[l], whole.at[l, my_core], local_sem.at[used]
                )
            )
            used += 1
    for n in range(4, INPUTS):
        fetch.append(pltpu.make_async_copy(held[n], here[n - 4], local_sem.at[used]))
        used += 1
    fetch[0].start()
    barrier = pltpu.get_barrier_semaphore()

    def greet(device):
        pl.semaphore_signal(barrier, inc=1, device_id=device, device_id_type=MESH)

    for k in range(2 * near, 0, -1):
        greet(column(tp_at(k), 0))
        greet(column(tp_at(k), 1))
    for k in range(half - 1, 0, -1):
        greet(row(x_at(k)))
    greet(column(my_tp, 1 - my_core))
    for f in fetch[1:]:
        f.start()

    def copy_a(l, k):
        if k == 0:
            dst = a_buf.at[l, 0, my_core]
            return remote(r_buf.at[l], dst, l, 0, 0, my_core, column(my_tp, row_core))
        slot = sent_place(k)
        dst = a_buf.at[l, slot, my_core]
        return remote(r_buf.at[l], dst, l, 0, k, 2 * slot + my_core, column(tp_at(k), row_core))

    def reach(l):
        return 2 * near if l == 0 else tp_n - 1

    def send_a(l):
        for k in range(reach(l), 0, -1):
            copy_a(l, k).start()

        @pl.when(uneven)
        def _():
            copy_a(l, 0).start()

        @pl.when(jnp.logical_not(uneven))
        def _():
            a_buf[l, 0, my_core] = r_buf[l]

    def offset_of(odd, k):
        if odd:
            return -k if k % 2 else k + 1
        return -k if k % 2 == 0 else k + 1

    def relayed(odd, down):
        offsets = [offset_of(odd, k) for k in range(half)]
        step = near if down else -near
        return [
            (offsets.index(o - step), k)
            for k, o in enumerate(offsets)
            if (o > near if down else o < -near)
        ]

    def copy_relay(source, target, down):
        z = lax.rem(my_tp + (tp_n - near if down else near), tp_n)
        src, dst = a_buf.at[0, source], a_buf.at[0, target]
        return remote(src, dst, 0, 4, target, target, column(z, my_core))

    def relay(odd, down):
        for source, target in relayed(odd, down):
            for core in range(2):
                got = a_buf.at[0, source, core]
                remote(
                    got, got, 0, 0, 0, 2 * source + core, column(rows_at(source), core)
                ).wait_recv()
            copy_relay(source, target, down).start()

    def wait_first_a(odd, k):
        if abs(offset_of(odd, k)) > near:
            copy_relay(k, k, 0).wait_recv()
        elif k not in [source for down in range(2) for source, _ in relayed(odd, down)]:
            for core in range(2):
                got = a_buf.at[0, k, core]
                copy = remote(got, got, 0, 0, k, 2 * k + core, column(rows_at(k), core))
                if offset_of(odd, k) != 0:
                    copy.wait_recv()
                else:

                    @pl.when(my_core != core)
                    def _(copy=copy):
                        copy.wait_recv()

    def copy_b(l, k):
        to = row(lax.div(rows_at(k), 2))
        return remote(b_out.at[l, k], b_in.at[l, my_x], l, 1, k, my_x, to)

    def copy_c(l, k):
        slot = x_mirror(k)
        return remote(c_own.at[l], c_buf.at[l, slot], l, 2, k, slot, row(x_at(k)))

    def copy_d(l, k, core):
        to = column(2 * x_at(k) + my_core, core)
        return remote(d_out.at[l, k, core], d_in.at[l, my_tp], l, 3, 2 * k + core, my_tp, to)

    def sent_abc(l):
        for k in range(1, reach(l) + 1):
            copy_a(l, k).wait_send()

        @pl.when(uneven)
        def _():
            copy_a(l, 0).wait_send()

        if l == 0:
            for odd in range(2):

                @pl.when(uneven == (odd == 1))
                def _(odd=odd):
                    for down in range(2):
                        for source, target in relayed(odd, down):
                            copy_relay(source, target, down).wait_send()

        for k in range(half):

            @pl.when(rows_at(k) != my_dp)
            def _(k=k):
                copy_b(l, k).wait_send()

            if k > 0:
                copy_c(l, k).wait_send()

    def sent_d(l):
        for k in range(half):
            for core in range(2):

                @pl.when(jnp.logical_not((2 * x_at(k) + my_core == my_tp) & (my_core == core)))
                def _(k=k, core=core):
                    copy_d(l, k, core).wait_send()

    pl.semaphore_wait(barrier, 4 * near + 1 + half - 1)
    fetch[0].wait()
    send_a(0)

    for f in fetch[1:]:
        f.wait()
    heads_all = w_dtt.shape[1]
    pick = lax.broadcasted_iota(jnp.int32, (16, heads_all), 0)
    col = lax.broadcasted_iota(jnp.int32, (16, heads_all), 1)
    pick = jnp.where((pick < heads_here) & (col == pick + my_tp * heads_here), 1.0, 0.0).astype(BF16)
    for l in range(layers):
        w_bcd[l, my_core, 0:bw] = w_bt[l]
        w_bcd[l, my_core, bw : 2 * bw] = w_ct[l]
        w_bcd[l, my_core, 2 * bw : 2 * bw + 16] = jnp.dot(
            pick, w_dtt[l], preferred_element_type=F32
        ).astype(BF16)
        w_bcd[l, my_core, 2 * bw + 16 :] = jnp.zeros(
            (w_bcd.shape[2] - 2 * bw - 16, width_f), BF16
        )
        conv_bc[l] = jnp.concatenate([conv_b[l].astype(F32), conv_c[l].astype(F32)], axis=1)
        for k in range(s_b.shape[1]):
            s_bc[l, k] = jnp.concatenate([s_b[l, k].astype(F32), s_c[l, k].astype(F32)], axis=1)

    gains[my_core] = jnp.zeros(gains.shape[1:], F32)
    gains[my_core, 0:layers] = gain[...].astype(F32)

    pair = []
    for whole in [gains.at[my_core]] + [
        w.at[l, my_core] for l in layer_list for w in (w_z, w_x, w_bcd, w_out)
    ]:
        pair.append(
            pltpu.make_async_remote_copy(
                src_ref=whole,
                dst_ref=whole,
                send_sem=pair_sem.at[0, len(pair)],
                recv_sem=pair_sem.at[1, len(pair)],
                device_id=column(my_tp, 1 - my_core),
                device_id_type=MESH,
            )
        )
    for p in pair:
        p.start()

    down_first = my_tp < half
    for odd in range(2):
        for order in ((0, 1), (1, 0)):

            @pl.when((uneven == (odd == 1)) & (down_first == (order[0] == 1)))
            def _(odd=odd, order=order):
                for down in order:
                    relay(odd, down)

    def turn(i, carry):
        for l in range(layers):
            block = ssm[l, i].reshape(zw, bw)
            st_t[l, i] = block.T.astype(BF16)
        return carry

    lane = lax.broadcasted_iota(jnp.int32, (rows, LANES), 1)
    head_of = lax.broadcasted_iota(jnp.int32, (rows, zw), 1)
    head_of = lax.div(head_of, hd)

    def per_head(v):
        out = jnp.broadcast_to(v[:, 0:1], (rows, zw))
        for h in range(1, heads_here):
            out = jnp.where(head_of == h, v[:, h : h + 1], out)
        return out

    for l in range(layers):
        if l > 0:
            send_a(l)

        for first in range(0, half, GROUP):
            group = min(GROUP, half)
            if l == 0:
                for odd in range(2):

                    @pl.when(uneven == (odd == 1))
                    def _(odd=odd, first=first, group=group):
                        for k in range(first, first + group):
                            wait_first_a(odd, k)

            else:
                for k in range(first, first + group):
                    for core in range(2):
                        got = a_buf.at[l, k, core]
                        copy = remote(got, got, l, 0, k, 2 * k + core, column(rows_at(k), core))
                        if k > 0:
                            copy.wait_recv()
                        else:

                            @pl.when(uneven | (my_core != core))
                            def _(copy=copy):
                                copy.wait_recv()

            if l == 0 and first == 0:
                for p in pair:
                    p.wait_recv()
            tall = group * rows
            scaled, squares = [], 0.0
            for core in range(2):
                block = a_buf[l, first : first + group, core].reshape(tall, width_f).astype(F32)
                scaled.append((block * gains[core, l : l + 1]).astype(BF16))
                squares = squares + jnp.sum(block * block, axis=1, keepdims=True)
            both_wide = jnp.concatenate(scaled, axis=1)
            part_z = jnp.dot(
                both_wide, w_z[l].reshape(2 * width_f, zw), preferred_element_type=F32
            ).astype(BF16)
            part_x = jnp.dot(
                both_wide, w_x[l].reshape(2 * width_f, zw), preferred_element_type=F32
            ).astype(BF16)
            rest = lax.dot_general(scaled[0], w_bcd[l, 0], NT, preferred_element_type=F32)
            rest += lax.dot_general(scaled[1], w_bcd[l, 1], NT, preferred_element_type=F32)
            lane_tall = lax.broadcasted_iota(jnp.int32, (tall, LANES), 1)
            small = jnp.where(lane_tall == heads_here, squares, rest[:, LANES:])
            low = small - small.astype(BF16).astype(F32)
            both = jnp.where(lane_tall < LANES // 2, small, pltpu.roll(low, LANES // 2, 1))
            b_out[l, first : first + group, :, 0:zw] = part_z.reshape(group, rows, zw)
            b_out[l, first : first + group, :, zw : 2 * zw] = part_x.reshape(group, rows, zw)
            b_out[l, first : first + group, :, 2 * zw : 2 * zw + LANES] = (
                rest[:, 0:LANES].astype(BF16).reshape(group, rows, LANES)
            )
            b_out[l, first : first + group, :, 2 * zw + LANES :] = both.astype(BF16).reshape(
                group, rows, LANES
            )
            for k in range(first, first + group):

                @pl.when(rows_at(k) != my_dp)
                def _(k=k, l=l):
                    copy_b(l, k).start()

        if l == 0:
            lax.fori_loop(0, rows, turn, 0)
        total = b_out[l, k_rows].astype(F32)
        for k in range(1, half):
            x = x_at(k)
            remote(b_in.at[l, x], b_in.at[l, x], l, 1, k, x, row(x)).wait_recv()
            total = total + b_in[l, x].astype(F32)

        small = total[:, 2 * zw + LANES :]
        small = small + pltpu.roll(small, LANES // 2, 1)
        row_scale = lax.rsqrt(small[:, heads_here : heads_here + 1] / features + EPSILON)
        step_raw = small[:, 0:heads_here] * row_scale
        gate = (total[:, 0:zw] * row_scale).astype(BF16).astype(F32)
        x_new = (total[:, zw : 2 * zw] * row_scale).astype(BF16)
        bc_new = (total[:, 2 * zw : 2 * zw + LANES] * row_scale).astype(BF16)
        taps = conv_x.shape[1]
        conv = x_new.astype(F32) * conv_x[l, taps - 1 : taps].astype(F32)
        conv2 = bc_new.astype(F32) * conv_bc[l, taps - 1 : taps]
        for k in range(taps - 1):
            conv = conv + s_x[l, k].astype(F32) * conv_x[l, k : k + 1].astype(F32)
            conv2 = conv2 + s_bc[l, k] * conv_bc[l, k : k + 1]
        v = silu(conv)
        bc = silu(conv2)
        step = jax.nn.softplus(step_raw + dt_bias[l : l + 1])
        decay = jnp.exp(-step * jnp.exp(a_log[l : l + 1]))
        xs = per_head(step) * v
        turned = pltpu.roll(bc, LANES // 2, 1)
        b_dot_c = 0.5 * jnp.sum(bc * turned, axis=1, keepdims=True)
        cc = jnp.where(lane < LANES // 2, turned, bc)
        seq = lax.broadcasted_iota(jnp.int32, (rows, LANES), 0)
        pieces = []
        for s in range(0, rows, 2):
            pieces.append(jnp.where(seq == s + lax.div(lane, LANES // 2), cc, 0.0).astype(BF16))
        spread = jnp.concatenate(pieces, axis=1)
        reads = jnp.dot(
            spread, st_t[l].reshape(rows * bw, zw), preferred_element_type=F32
        )
        readout = per_head(decay) * reads + (xs * b_dot_c + per_head(d_skip[l : l + 1]) * v)
        gated = readout * silu(gate)
        scale = lax.rsqrt(jnp.mean(gated * gated, axis=1, keepdims=True) + EPSILON)
        mixed = (gated * scale * out_gain[l : l + 1].astype(F32)).astype(BF16)

        c_own[l] = mixed
        c_buf[l, 0] = mixed

        for k in range(half - 1, 0, -1):
            copy_c(l, k).start()

        for first in range(0, half, GROUP):
            group = min(GROUP, half)
            for k in range(max(first, 1), first + group):
                got = c_buf.at[l, k]
                remote(got, got, l, 2, k, k, row(x_at(k))).wait_recv()
            block = c_buf[l, first : first + group].reshape(group * rows, zw)
            for core in range(2):
                part = jnp.dot(block, w_out[l, core], preferred_element_type=F32).astype(BF16)
                d_out[l, first : first + group, core] = part.reshape(group, rows, width_f)
            for k in range(first, first + group):
                z = 2 * x_at(k) + my_core
                for core in range(2):
                    mine = (z == my_tp) & (my_core == core)

                    @pl.when(jnp.logical_not(mine))
                    def _(k=k, core=core, l=l):
                        copy_d(l, k, core).start()

                    @pl.when(mine)
                    def _(k=k, core=core, l=l):
                        d_in[l, my_tp] = d_out[l, k, core]

        xs_t = xs.T
        for s in range(rows):
            for h in range(heads_here):
                b_row = bc[s : s + 1, 0:bw]
                xs_col = xs_t[h * hd : (h + 1) * hd, s : s + 1]
                ssm_o[l, s, h] = ssm[l, s, h] * decay[s : s + 1, h : h + 1] + xs_col * b_row
        for k in range(taps - 2):
            nx_o[l, k] = s_x[l, k + 1]
            nb_o[l, k] = s_b[l, k + 1]
            nc_o[l, k] = s_c[l, k + 1]
        nx_o[l, taps - 2] = x_new
        nb_o[l, taps - 2] = bc_new[:, 0:bw]
        nc_o[l, taps - 2] = bc_new[:, bw : 2 * bw]

        sent_abc(l)
        if l > 0:
            sent_d(l - 1)

        @pl.when(uneven)
        def _(l=l):
            got = d_in.at[l, my_tp]
            remote(got, got, l, 3, 0, my_tp, column(my_tp, row_core)).wait_recv()

        projected = d_in[l, my_tp].astype(F32)
        for k in range(1, tp_n):
            z = tp_at(k)
            got = d_in.at[l, z]
            remote(got, got, l, 3, k, z, column(z, row_core)).wait_recv()
            projected = projected + d_in[l, z].astype(F32)
        new = (r_buf[l].astype(F32) + projected).astype(BF16)
        if l + 1 < layers:
            r_buf[l + 1] = new
        else:
            res_o[...] = new

    sent_d(layers - 1)
    for p in pair:
        p.wait_send()


def write_out(*refs):
    sem = refs[-1]
    half = len(refs) // 2
    copies = []
    for n in range(half):
        cuts = refs[n].shape[1] // 4 if len(refs[n].shape) == 5 else 0
        for at in range(4 * refs[n].shape[0]) if cuts else (None,):
            src, dst = refs[n], refs[half + n]
            if cuts:
                part = pl.ds(at % 4 * cuts, cuts)
                src, dst = src.at[at // 4, part], dst.at[at // 4, part]
            copies.append(pltpu.make_async_copy(src, dst, sem.at[len(copies)]))
    for c in copies:
        c.start()
    for c in copies:
        c.wait()


def body(tp_n, dp_n, *args):
    (
        tokens,
        norm_gain,
        w_z,
        w_x,
        w_b,
        w_c,
        w_dt,
        conv_x,
        conv_b,
        conv_c,
        dt_bias,
        a_log,
        d_skip,
        out_gain,
        w_out,
        ssm_state,
        state_x,
        state_b,
        state_c,
    ) = args
    layers, heads_here = dt_bias.shape
    rows, width_f = tokens.shape
    zw, bw = w_z.shape[2], w_b.shape[2]
    assert tp_n == dp_n and 2 * bw == LANES
    wide = 2 * zw + 2 * LANES
    half = tp_n // 2

    def turn(a):
        return jnp.swapaxes(a, 1, 2)

    operands = (
        tokens,
        w_z,
        w_x,
        w_out,
        norm_gain,
        turn(w_b),
        turn(w_c),
        turn(w_dt),
        conv_x,
        conv_b,
        conv_c,
        dt_bias,
        a_log,
        d_skip,
        out_gain,
        ssm_state,
        turn(state_x),
        turn(state_b),
        turn(state_c),
    )
    vmem = pl.BlockSpec(memory_space=pltpu.VMEM)
    hbm = pl.BlockSpec(memory_space=pltpu.HBM)

    def like(a):
        return pltpu.VMEM(a.shape, a.dtype)

    results = pl.pallas_call(
        functools.partial(kernel, tp_n, dp_n, width_f * dp_n),
        out_shape=(
            like(tokens),
            like(ssm_state),
            like(operands[16]),
            like(operands[17]),
            like(operands[18]),
        ),
        in_specs=[hbm] * INPUTS,
        out_specs=(vmem,) * 5,
        scratch_shapes=[
            pltpu.VMEM((layers, half, 2, rows, width_f), BF16),
            pltpu.VMEM((layers, half, rows, wide), BF16),
            pltpu.VMEM((layers, half, rows, wide), BF16),
            pltpu.VMEM((layers, rows, zw), BF16),
            pltpu.VMEM((layers, half, rows, zw), BF16),
            pltpu.VMEM((layers, half, 2, rows, width_f), BF16),
            pltpu.VMEM((layers, tp_n, rows, width_f), BF16),
            pltpu.VMEM((layers, rows, width_f), BF16),
            pltpu.VMEM((layers, 2, width_f, zw), BF16),
            pltpu.VMEM((layers, 2, width_f, zw), BF16),
            pltpu.VMEM((layers, 2, zw, width_f), BF16),
            pltpu.VMEM((layers, 2, 2 * LANES, width_f), BF16),
            pltpu.VMEM((2, 8, width_f), F32),
            pltpu.VMEM((layers, conv_x.shape[1], LANES), F32),
            pltpu.VMEM((layers, state_b.shape[2], rows, LANES), F32),
            pltpu.VMEM((layers, rows, bw, zw), BF16),
            *(pltpu.VMEM(a.shape, a.dtype) for a in operands[4:]),
            pltpu.SemaphoreType.DMA((INPUTS - 3 + 3 * layers,)),
            pltpu.SemaphoreType.DMA((2, 1 + 4 * layers)),
            pltpu.SemaphoreType.DMA((layers, 5, tp_n)),
            pltpu.SemaphoreType.DMA((layers, 5, tp_n)),
        ],
        compiler_params=pltpu.CompilerParams(
            collective_id=0, has_side_effects=True, vmem_limit_bytes=40 * 1024 * 1024
        ),
        name="decode",
    )(*(pltpu.with_memory_space_constraint(a, pltpu.HBM) for a in operands))
    results = [pltpu.with_memory_space_constraint(a, pltpu.VMEM) for a in results]
    residual, ssm_next, next_x, next_b, next_c = pl.pallas_call(
        write_out,
        out_shape=tuple(jax.ShapeDtypeStruct(a.shape, a.dtype) for a in results),
        in_specs=(vmem,) * 5,
        out_specs=(hbm,) * 5,
        scratch_shapes=[pltpu.SemaphoreType.DMA((4 + 4 * layers,))],
        compiler_params=pltpu.CompilerParams(vmem_limit_bytes=8 * 1024 * 1024),
        name="write_out",
    )(*results)
    return residual, ssm_next, turn(next_x), turn(next_b), turn(next_c)


def solution(mesh):
    placed = (
        P(("grp", "tp"), "dp"),
        P(None, "dp"),
        P(None, "dp", "tp"),
        P(None, "dp", "tp"),
        P(None, "dp", "tp"),
        P(None, "dp", "tp"),
        P(None, "dp", None),
        P(None, None, "tp"),
        P(None, None, "tp"),
        P(None, None, "tp"),
        P(None, "tp"),
        P(None, "tp"),
        P(None, "tp"),
        P(None, "tp"),
        P(None, "tp", "dp"),
        P(None, ("grp", "dp"), "tp", None, None),
        P(None, ("grp", "dp"), None, "tp"),
        P(None, ("grp", "dp"), None, "tp"),
        P(None, ("grp", "dp"), None, "tp"),
    )
    return jax.shard_map(
        functools.partial(body, mesh.shape["tp"], mesh.shape["dp"]),
        mesh=mesh,
        in_specs=placed,
        out_specs=(placed[0], placed[15], placed[16], placed[17], placed[18]),
        check_vma=False,
    )
```

```python
import functools

import jax
import jax.numpy as jnp
from jax import lax
from jax.experimental import pallas as pl
from jax.experimental.pallas import tpu as pltpu
from jax.sharding import PartitionSpec as P

EPSILON = 1e-05
F32 = jnp.float32
BF16 = jnp.bfloat16
MESH = pl.DeviceIdType.MESH
NT = (((1,), (1,)), ((), ()))
LANES = 128
INPUTS = 19
GROUP = 1


def silu(v):
    return v * jax.nn.sigmoid(v)


def kernel(
    tp_n,
    dp_n,
    features,
    *refs,
):
    held, refs = refs[:INPUTS], refs[INPUTS:]
    res_o, ssm_o, nx_o, nb_o, nc_o = refs[:5]
    a_buf, b_out, b_in, c_own, c_buf, d_out, d_in, r_buf = refs[5:13]
    w_z, w_x, w_out, w_bcd, gains, conv_bc, s_bc, st_t = refs[13:21]
    here = refs[21 : 17 + INPUTS]
    local_sem, pair_sem, send_sem, recv_sem = refs[17 + INPUTS :]
    (
        gain,
        w_bt,
        w_ct,
        w_dtt,
        conv_x,
        conv_b,
        conv_c,
        dt_bias,
        a_log,
        d_skip,
        out_gain,
        ssm,
        s_x,
        s_b,
        s_c,
    ) = here
    layers, heads_here = dt_bias.shape
    rows, width_f = res_o.shape
    zw = w_z.shape[3]
    bw = w_bt.shape[1]
    hd = zw // heads_here
    my_tp, my_dp = lax.axis_index("tp"), lax.axis_index("dp")
    my_x, my_core = lax.div(my_dp, 2), lax.rem(my_dp, 2)
    half, near = tp_n // 2, tp_n // 4
    uneven = lax.rem(my_tp + my_core, 2) == 1
    row_core = lax.rem(my_tp, 2)

    def nearest(k, n):
        return (k + 1) // 2 if k % 2 else (n - k // 2) % n

    def place(distance, n):
        return jnp.where(distance <= n // 2, jnp.maximum(2 * distance - 1, 0), 2 * (n - distance))

    def tp_at(k):
        return lax.rem(my_tp + nearest(k, tp_n), tp_n)

    def x_at(k):
        return lax.rem(my_x + nearest(k, half), half)

    def rows_at(k):
        odd = tp_n - k if k % 2 else k + 1
        return lax.rem(my_tp + jnp.where(uneven, odd, 2 * nearest(k, half)), tp_n)

    def rows_place(offset):
        odd = jnp.where(offset < half, offset - 1, tp_n - offset)
        return jnp.where(lax.rem(offset, 2) == 1, odd, place(lax.div(offset, 2), half))

    def sent_place(k):
        offset = (tp_n - nearest(k, tp_n)) % tp_n
        if offset % 2:
            return offset - 1 if offset < half else tp_n - offset
        distance = offset // 2
        return max(2 * distance - 1, 0) if 2 * distance <= half else 2 * (half - distance)

    def x_mirror(k):
        if k == 0 or (k == half - 1 and half % 2 == 0):
            return k
        return k + 1 if k % 2 else k - 1

    k_rows = rows_place(lax.rem(my_dp - my_tp + tp_n, tp_n))

    def remote(src, dst, layer, phase, s_slot, r_slot, target):
        return pltpu.make_async_remote_copy(
            src_ref=src,
            dst_ref=dst,
            send_sem=send_sem.at[layer, phase, s_slot],
            recv_sem=recv_sem.at[layer, phase, r_slot],
            device_id=target,
            device_id_type=MESH,
        )

    def column(z, core):
        return {"tp": z, "dp": 2 * my_x + core}

    def row(x):
        return {"dp": 2 * x + my_core}

    layer_list = range(layers)
    fetch = [pltpu.make_async_copy(held[0], r_buf.at[0], local_sem.at[0])]
    used = 1
    for n in range(3):
        whole = (w_z, w_x, w_out)[n]
        for l in layer_list:
            fetch.append(
                pltpu.make_async_copy(
                    held[1 + n].at[l], whole.at[l, my_core], local_sem.at[used]
                )
            )
            used += 1
    for n in range(4, INPUTS):
        fetch.append(pltpu.make_async_copy(held[n], here[n - 4], local_sem.at[used]))
        used += 1
    fetch[0].start()
    barrier = pltpu.get_barrier_semaphore()

    def greet(device):
        pl.semaphore_signal(barrier, inc=1, device_id=device, device_id_type=MESH)

    for k in range(2 * near, 0, -1):
        greet(column(tp_at(k), 0))
        greet(column(tp_at(k), 1))
    for k in range(half - 1, 0, -1):
        greet(row(x_at(k)))
    greet(column(my_tp, 1 - my_core))
    for f in fetch[1:]:
        f.start()

    def copy_a(l, k):
        if k == 0:
            dst = a_buf.at[l, 0, my_core]
            return remote(r_buf.at[l], dst, l, 0, 0, my_core, column(my_tp, row_core))
        slot = sent_place(k)
        dst = a_buf.at[l, slot, my_core]
        return remote(r_buf.at[l], dst, l, 0, k, 2 * slot + my_core, column(tp_at(k), row_core))

    def reach(l):
        return 2 * near if l == 0 else tp_n - 1

    def send_a(l):
        for k in range(reach(l), 0, -1):
            copy_a(l, k).start()

        @pl.when(uneven)
        def _():
            copy_a(l, 0).start()

        @pl.when(jnp.logical_not(uneven))
        def _():
            a_buf[l, 0, my_core] = r_buf[l]

    def offset_of(odd, k):
        if odd:
            return -k if k % 2 else k + 1
        return -k if k % 2 == 0 else k + 1

    def relayed(odd, down):
        offsets = [offset_of(odd, k) for k in range(half)]
        step = near if down else -near
        return [
            (offsets.index(o - step), k)
            for k, o in enumerate(offsets)
            if (o > near if down else o < -near)
        ]

    def copy_relay(source, target, down):
        z = lax.rem(my_tp + (tp_n - near if down else near), tp_n)
        src, dst = a_buf.at[0, source], a_buf.at[0, target]
        return remote(src, dst, 0, 4, target, target, column(z, my_core))

    def relay(odd, down):
        for source, target in relayed(odd, down):
            for core in range(2):
                got = a_buf.at[0, source, core]
                remote(
                    got, got, 0, 0, 0, 2 * source + core, column(rows_at(source), core)
                ).wait_recv()
            copy_relay(source, target, down).start()

    def wait_first_a(odd, k):
        if abs(offset_of(odd, k)) > near:
            copy_relay(k, k, 0).wait_recv()
        elif k not in [source for down in range(2) for source, _ in relayed(odd, down)]:
            for core in range(2):
                got = a_buf.at[0, k, core]
                copy = remote(got, got, 0, 0, k, 2 * k + core, column(rows_at(k), core))
                if offset_of(odd, k) != 0:
                    copy.wait_recv()
                else:

                    @pl.when(my_core != core)
                    def _(copy=copy):
                        copy.wait_recv()

    def copy_b(l, k):
        to = row(lax.div(rows_at(k), 2))
        return remote(b_out.at[l, k], b_in.at[l, my_x], l, 1, k, my_x, to)

    def copy_c(l, k):
        slot = x_mirror(k)
        return remote(c_own.at[l], c_buf.at[l, slot], l, 2, k, slot, row(x_at(k)))

    def copy_d(l, k, core):
        to = column(2 * x_at(k) + my_core, core)
        return remote(d_out.at[l, k, core], d_in.at[l, my_tp], l, 3, 2 * k + core, my_tp, to)

    def sent_abc(l):
        for k in range(1, reach(l) + 1):
            copy_a(l, k).wait_send()

        @pl.when(uneven)
        def _():
            copy_a(l, 0).wait_send()

        if l == 0:
            for odd in range(2):

                @pl.when(uneven == (odd == 1))
                def _(odd=odd):
                    for down in range(2):
                        for source, target in relayed(odd, down):
                            copy_relay(source, target, down).wait_send()

        for k in range(half):

            @pl.when(rows_at(k) != my_dp)
            def _(k=k):
                copy_b(l, k).wait_send()

            if k > 0:
                copy_c(l, k).wait_send()

    def sent_d(l):
        for k in range(half):
            for core in range(2):

                @pl.when(jnp.logical_not((2 * x_at(k) + my_core == my_tp) & (my_core == core)))
                def _(k=k, core=core):
                    copy_d(l, k, core).wait_send()

    pl.semaphore_wait(barrier, 4 * near + 1 + half - 1)
    fetch[0].wait()
    send_a(0)

    for f in fetch[1:]:
        f.wait()
    heads_all = w_dtt.shape[1]
    pick = lax.broadcasted_iota(jnp.int32, (16, heads_all), 0)
    col = lax.broadcasted_iota(jnp.int32, (16, heads_all), 1)
    pick = jnp.where((pick < heads_here) & (col == pick + my_tp * heads_here), 1.0, 0.0).astype(BF16)
    for l in range(layers):
        w_bcd[l, my_core, 0:bw] = w_bt[l]
        w_bcd[l, my_core, bw : 2 * bw] = w_ct[l]
        w_bcd[l, my_core, 2 * bw : 2 * bw + 16] = jnp.dot(
            pick, w_dtt[l], preferred_element_type=F32
        ).astype(BF16)
        w_bcd[l, my_core, 2 * bw + 16 :] = jnp.zeros(
            (w_bcd.shape[2] - 2 * bw - 16, width_f), BF16
        )
        conv_bc[l] = jnp.concatenate([conv_b[l].astype(F32), conv_c[l].astype(F32)], axis=1)
        for k in range(s_b.shape[1]):
            s_bc[l, k] = jnp.concatenate([s_b[l, k].astype(F32), s_c[l, k].astype(F32)], axis=1)

    gains[my_core] = jnp.zeros(gains.shape[1:], F32)
    gains[my_core, 0:layers] = gain[...].astype(F32)

    pair = []
    for whole in [gains.at[my_core]] + [
        w.at[l, my_core] for l in layer_list for w in (w_z, w_x, w_bcd, w_out)
    ]:
        pair.append(
            pltpu.make_async_remote_copy(
                src_ref=whole,
                dst_ref=whole,
                send_sem=pair_sem.at[0, len(pair)],
                recv_sem=pair_sem.at[1, len(pair)],
                device_id=column(my_tp, 1 - my_core),
                device_id_type=MESH,
            )
        )
    for p in pair:
        p.start()

    down_first = my_tp < half
    for odd in range(2):
        for order in ((0, 1), (1, 0)):

            @pl.when((uneven == (odd == 1)) & (down_first == (order[0] == 1)))
            def _(odd=odd, order=order):
                for down in order:
                    relay(odd, down)

    def turn(i, carry):
        for l in range(layers):
            block = ssm[l, i].reshape(zw, bw)
            st_t[l, i] = block.T.astype(BF16)
        return carry

    lane = lax.broadcasted_iota(jnp.int32, (rows, LANES), 1)
    head_of = lax.broadcasted_iota(jnp.int32, (rows, zw), 1)
    head_of = lax.div(head_of, hd)

    def per_head(v):
        out = jnp.broadcast_to(v[:, 0:1], (rows, zw))
        for h in range(1, heads_here):
            out = jnp.where(head_of == h, v[:, h : h + 1], out)
        return out

    for l in range(layers):
        if l > 0:
            send_a(l)

        for first in range(0, half, GROUP):
            group = min(GROUP, half)
            if l == 0:
                for odd in range(2):

                    @pl.when(uneven == (odd == 1))
                    def _(odd=odd, first=first, group=group):
                        for k in range(first, first + group):
                            wait_first_a(odd, k)

            else:
                for k in range(first, first + group):
                    for core in range(2):
                        got = a_buf.at[l, k, core]
                        copy = remote(got, got, l, 0, k, 2 * k + core, column(rows_at(k), core))
                        if k > 0:
                            copy.wait_recv()
                        else:

                            @pl.when(uneven | (my_core != core))
                            def _(copy=copy):
                                copy.wait_recv()

            if l == 0 and first == 0:
                for p in pair:
                    p.wait_recv()
            tall = group * rows
            scaled, squares = [], 0.0
            for core in range(2):
                block = a_buf[l, first : first + group, core].reshape(tall, width_f).astype(F32)
                scaled.append((block * gains[core, l : l + 1]).astype(BF16))
                squares = squares + jnp.sum(block * block, axis=1, keepdims=True)
            both_wide = jnp.concatenate(scaled, axis=1)
            part_z = jnp.dot(
                both_wide, w_z[l].reshape(2 * width_f, zw), preferred_element_type=F32
            ).astype(BF16)
            part_x = jnp.dot(
                both_wide, w_x[l].reshape(2 * width_f, zw), preferred_element_type=F32
            ).astype(BF16)
            rest = lax.dot_general(scaled[0], w_bcd[l, 0], NT, preferred_element_type=F32)
            rest += lax.dot_general(scaled[1], w_bcd[l, 1], NT, preferred_element_type=F32)
            lane_tall = lax.broadcasted_iota(jnp.int32, (tall, LANES), 1)
            small = jnp.where(lane_tall == heads_here, squares, rest[:, LANES:])
            low = small - small.astype(BF16).astype(F32)
            both = jnp.where(lane_tall < LANES // 2, small, pltpu.roll(low, LANES // 2, 1))
            b_out[l, first : first + group, :, 0:zw] = part_z.reshape(group, rows, zw)
            b_out[l, first : first + group, :, zw : 2 * zw] = part_x.reshape(group, rows, zw)
            b_out[l, first : first + group, :, 2 * zw : 2 * zw + LANES] = (
                rest[:, 0:LANES].astype(BF16).reshape(group, rows, LANES)
            )
            b_out[l, first : first + group, :, 2 * zw + LANES :] = both.astype(BF16).reshape(
                group, rows, LANES
            )
            for k in range(first, first + group):

                @pl.when(rows_at(k) != my_dp)
                def _(k=k, l=l):
                    copy_b(l, k).start()

        if l == 0:
            lax.fori_loop(0, rows, turn, 0)
        total = b_out[l, k_rows].astype(F32)
        for k in range(1, half):
            x = x_at(k)
            remote(b_in.at[l, x], b_in.at[l, x], l, 1, k, x, row(x)).wait_recv()
            total = total + b_in[l, x].astype(F32)

        small = total[:, 2 * zw + LANES :]
        small = small + pltpu.roll(small, LANES // 2, 1)
        row_scale = lax.rsqrt(small[:, heads_here : heads_here + 1] / features + EPSILON)
        step_raw = small[:, 0:heads_here] * row_scale
        gate = (total[:, 0:zw] * row_scale).astype(BF16).astype(F32)
        x_new = (total[:, zw : 2 * zw] * row_scale).astype(BF16)
        bc_new = (total[:, 2 * zw : 2 * zw + LANES] * row_scale).astype(BF16)
        taps = conv_x.shape[1]
        conv = x_new.astype(F32) * conv_x[l, taps - 1 : taps].astype(F32)
        conv2 = bc_new.astype(F32) * conv_bc[l, taps - 1 : taps]
        for k in range(taps - 1):
            conv = conv + s_x[l, k].astype(F32) * conv_x[l, k : k + 1].astype(F32)
            conv2 = conv2 + s_bc[l, k] * conv_bc[l, k : k + 1]
        v = silu(conv)
        bc = silu(conv2)
        step = jax.nn.softplus(step_raw + dt_bias[l : l + 1])
        decay = jnp.exp(-step * jnp.exp(a_log[l : l + 1]))
        xs = per_head(step) * v
        turned = pltpu.roll(bc, LANES // 2, 1)
        b_dot_c = 0.5 * jnp.sum(bc * turned, axis=1, keepdims=True)
        cc = jnp.where(lane < LANES // 2, turned, bc)
        seq = lax.broadcasted_iota(jnp.int32, (rows, LANES), 0)
        pieces = []
        for s in range(0, rows, 2):
            pieces.append(jnp.where(seq == s + lax.div(lane, LANES // 2), cc, 0.0).astype(BF16))
        spread = jnp.concatenate(pieces, axis=1)
        reads = jnp.dot(
            spread, st_t[l].reshape(rows * bw, zw), preferred_element_type=F32
        )
        readout = per_head(decay) * reads + (xs * b_dot_c + per_head(d_skip[l : l + 1]) * v)
        gated = readout * silu(gate)
        scale = lax.rsqrt(jnp.mean(gated * gated, axis=1, keepdims=True) + EPSILON)
        mixed = (gated * scale * out_gain[l : l + 1].astype(F32)).astype(BF16)

        c_own[l] = mixed
        c_buf[l, 0] = mixed

        for k in range(half - 1, 0, -1):
            copy_c(l, k).start()

        for first in range(0, half, GROUP):
            group = min(GROUP, half)
            for k in range(max(first, 1), first + group):
                got = c_buf.at[l, k]
                remote(got, got, l, 2, k, k, row(x_at(k))).wait_recv()
            block = c_buf[l, first : first + group].reshape(group * rows, zw)
            for core in range(2):
                part = jnp.dot(block, w_out[l, core], preferred_element_type=F32).astype(BF16)
                d_out[l, first : first + group, core] = part.reshape(group, rows, width_f)
            for k in range(first, first + group):
                z = 2 * x_at(k) + my_core
                for core in range(2):
                    mine = (z == my_tp) & (my_core == core)

                    @pl.when(jnp.logical_not(mine))
                    def _(k=k, core=core, l=l):
                        copy_d(l, k, core).start()

                    @pl.when(mine)
                    def _(k=k, core=core, l=l):
                        d_in[l, my_tp] = d_out[l, k, core]

        xs_t = xs.T
        for s in range(rows):
            for h in range(heads_here):
                b_row = bc[s : s + 1, 0:bw]
                xs_col = xs_t[h * hd : (h + 1) * hd, s : s + 1]
                ssm_o[l, s, h] = ssm[l, s, h] * decay[s : s + 1, h : h + 1] + xs_col * b_row
        for k in range(taps - 2):
            nx_o[l, k] = s_x[l, k + 1]
            nb_o[l, k] = s_b[l, k + 1]
            nc_o[l, k] = s_c[l, k + 1]
        nx_o[l, taps - 2] = x_new
        nb_o[l, taps - 2] = bc_new[:, 0:bw]
        nc_o[l, taps - 2] = bc_new[:, bw : 2 * bw]

        sent_abc(l)
        if l > 0:
            sent_d(l - 1)

        @pl.when(uneven)
        def _(l=l):
            got = d_in.at[l, my_tp]
            remote(got, got, l, 3, 0, my_tp, column(my_tp, row_core)).wait_recv()

        projected = d_in[l, my_tp].astype(F32)
        for k in range(1, tp_n):
            z = tp_at(k)
            got = d_in.at[l, z]
            remote(got, got, l, 3, k, z, column(z, row_core)).wait_recv()
            projected = projected + d_in[l, z].astype(F32)
        new = (r_buf[l].astype(F32) + projected).astype(BF16)
        if l + 1 < layers:
            r_buf[l + 1] = new
        else:
            res_o[...] = new

    sent_d(layers - 1)
    for p in pair:
        p.wait_send()


def write_out(*refs):
    sem = refs[-1]
    half = len(refs) // 2
    copies = []
    for n in range(half):
        cuts = refs[n].shape[1] // 4 if len(refs[n].shape) == 5 else 0
        for at in range(4 * refs[n].shape[0]) if cuts else (None,):
            src, dst = refs[n], refs[half + n]
            if cuts:
                part = pl.ds(at % 4 * cuts, cuts)
                src, dst = src.at[at // 4, part], dst.at[at // 4, part]
            copies.append(pltpu.make_async_copy(src, dst, sem.at[len(copies)]))
    for c in copies:
        c.start()
    for c in copies:
        c.wait()


def body(tp_n, dp_n, *args):
    (
        tokens,
        norm_gain,
        w_z,
        w_x,
        w_b,
        w_c,
        w_dt,
        conv_x,
        conv_b,
        conv_c,
        dt_bias,
        a_log,
        d_skip,
        out_gain,
        w_out,
        ssm_state,
        state_x,
        state_b,
        state_c,
    ) = args
    layers, heads_here = dt_bias.shape
    rows, width_f = tokens.shape
    zw, bw = w_z.shape[2], w_b.shape[2]
    assert tp_n == dp_n and 2 * bw == LANES
    wide = 2 * zw + 2 * LANES
    half = tp_n // 2

    def turn(a):
        return jnp.swapaxes(a, 1, 2)

    operands = (
        tokens,
        w_z,
        w_x,
        w_out,
        norm_gain,
        turn(w_b),
        turn(w_c),
        turn(w_dt),
        conv_x,
        conv_b,
        conv_c,
        dt_bias,
        a_log,
        d_skip,
        out_gain,
        ssm_state,
        turn(state_x),
        turn(state_b),
        turn(state_c),
    )
    vmem = pl.BlockSpec(memory_space=pltpu.VMEM)
    hbm = pl.BlockSpec(memory_space=pltpu.HBM)

    def like(a):
        return pltpu.VMEM(a.shape, a.dtype)

    results = pl.pallas_call(
        functools.partial(kernel, tp_n, dp_n, width_f * dp_n),
        out_shape=(
            like(tokens),
            like(ssm_state),
            like(operands[16]),
            like(operands[17]),
            like(operands[18]),
        ),
        in_specs=[hbm] * INPUTS,
        out_specs=(vmem,) * 5,
        scratch_shapes=[
            pltpu.VMEM((layers, half, 2, rows, width_f), BF16),
            pltpu.VMEM((layers, half, rows, wide), BF16),
            pltpu.VMEM((layers, half, rows, wide), BF16),
            pltpu.VMEM((layers, rows, zw), BF16),
            pltpu.VMEM((layers, half, rows, zw), BF16),
            pltpu.VMEM((layers, half, 2, rows, width_f), BF16),
            pltpu.VMEM((layers, tp_n, rows, width_f), BF16),
            pltpu.VMEM((layers, rows, width_f), BF16),
            pltpu.VMEM((layers, 2, width_f, zw), BF16),
            pltpu.VMEM((layers, 2, width_f, zw), BF16),
            pltpu.VMEM((layers, 2, zw, width_f), BF16),
            pltpu.VMEM((layers, 2, 2 * LANES, width_f), BF16),
            pltpu.VMEM((2, 8, width_f), F32),
            pltpu.VMEM((layers, conv_x.shape[1], LANES), F32),
            pltpu.VMEM((layers, state_b.shape[2], rows, LANES), F32),
            pltpu.VMEM((layers, rows, bw, zw), BF16),
            *(pltpu.VMEM(a.shape, a.dtype) for a in operands[4:]),
            pltpu.SemaphoreType.DMA((INPUTS - 3 + 3 * layers,)),
            pltpu.SemaphoreType.DMA((2, 1 + 4 * layers)),
            pltpu.SemaphoreType.DMA((layers, 5, tp_n)),
            pltpu.SemaphoreType.DMA((layers, 5, tp_n)),
        ],
        compiler_params=pltpu.CompilerParams(
            collective_id=0, has_side_effects=True, vmem_limit_bytes=40 * 1024 * 1024
        ),
        name="decode",
    )(*(pltpu.with_memory_space_constraint(a, pltpu.HBM) for a in operands))
    results = [pltpu.with_memory_space_constraint(a, pltpu.VMEM) for a in results]
    residual, ssm_next, next_x, next_b, next_c = pl.pallas_call(
        write_out,
        out_shape=tuple(jax.ShapeDtypeStruct(a.shape, a.dtype) for a in results),
        in_specs=(vmem,) * 5,
        out_specs=(hbm,) * 5,
        scratch_shapes=[pltpu.SemaphoreType.DMA((4 + 4 * layers,))],
        compiler_params=pltpu.CompilerParams(vmem_limit_bytes=8 * 1024 * 1024),
        name="write_out",
    )(*results)
    return residual, ssm_next, turn(next_x), turn(next_b), turn(next_c)


def solution(mesh):
    placed = (
        P(("grp", "tp"), "dp"),
        P(None, "dp"),
        P(None, "dp", "tp"),
        P(None, "dp", "tp"),
        P(None, "dp", "tp"),
        P(None, "dp", "tp"),
        P(None, "dp", None),
        P(None, None, "tp"),
        P(None, None, "tp"),
        P(None, None, "tp"),
        P(None, "tp"),
        P(None, "tp"),
        P(None, "tp"),
        P(None, "tp"),
        P(None, "tp", "dp"),
        P(None, ("grp", "dp"), "tp", None, None),
        P(None, ("grp", "dp"), None, "tp"),
        P(None, ("grp", "dp"), None, "tp"),
        P(None, ("grp", "dp"), None, "tp"),
    )
    return jax.shard_map(
        functools.partial(body, mesh.shape["tp"], mesh.shape["dp"]),
        mesh=mesh,
        in_specs=placed,
        out_specs=(placed[0], placed[15], placed[16], placed[17], placed[18]),
        check_vma=False,
    )
```

```python
import functools

import jax
import jax.numpy as jnp
from jax import lax
from jax.experimental import pallas as pl
from jax.experimental.pallas import tpu as pltpu
from jax.sharding import PartitionSpec as P

EPSILON = 1e-05
F32 = jnp.float32
BF16 = jnp.bfloat16
MESH = pl.DeviceIdType.MESH
NT = (((1,), (1,)), ((), ()))
LANES = 128
INPUTS = 19
GROUP = 1


def silu(v):
    return v * jax.nn.sigmoid(v)


def kernel(
    tp_n,
    dp_n,
    features,
    *refs,
):
    held, refs = refs[:INPUTS], refs[INPUTS:]
    res_o, ssm_o, nx_o, nb_o, nc_o = refs[:5]
    a_buf, b_out, b_in, c_own, c_buf, d_out, d_in, r_buf = refs[5:13]
    w_z, w_x, w_out, w_bcd, gains, conv_bc, s_bc, st_t = refs[13:21]
    here = refs[21 : 17 + INPUTS]
    d_far, r_far, local_sem, pair_sem, send_sem, recv_sem = refs[17 + INPUTS :]
    (
        gain,
        w_bt,
        w_ct,
        w_dtt,
        conv_x,
        conv_b,
        conv_c,
        dt_bias,
        a_log,
        d_skip,
        out_gain,
        ssm,
        s_x,
        s_b,
        s_c,
    ) = here
    layers, heads_here = dt_bias.shape
    rows, width_f = res_o.shape
    zw = w_z.shape[3]
    bw = w_bt.shape[1]
    hd = zw // heads_here
    my_tp, my_dp = lax.axis_index("tp"), lax.axis_index("dp")
    my_x, my_core = lax.div(my_dp, 2), lax.rem(my_dp, 2)
    half, near = tp_n // 2, tp_n // 4
    uneven = lax.rem(my_tp + my_core, 2) == 1
    row_core = lax.rem(my_tp, 2)

    def nearest(k, n):
        return (k + 1) // 2 if k % 2 else (n - k // 2) % n

    def place(distance, n):
        return jnp.where(distance <= n // 2, jnp.maximum(2 * distance - 1, 0), 2 * (n - distance))

    def tp_at(k):
        return lax.rem(my_tp + nearest(k, tp_n), tp_n)

    def x_at(k):
        return lax.rem(my_x + nearest(k, half), half)

    def rows_at(k):
        odd = tp_n - k if k % 2 else k + 1
        return lax.rem(my_tp + jnp.where(uneven, odd, 2 * nearest(k, half)), tp_n)

    def rows_place(offset):
        odd = jnp.where(offset < half, offset - 1, tp_n - offset)
        return jnp.where(lax.rem(offset, 2) == 1, odd, place(lax.div(offset, 2), half))

    def sent_place(k):
        offset = (tp_n - nearest(k, tp_n)) % tp_n
        if offset % 2:
            return offset - 1 if offset < half else tp_n - offset
        distance = offset // 2
        return max(2 * distance - 1, 0) if 2 * distance <= half else 2 * (half - distance)

    def x_mirror(k):
        if k == 0 or (k == half - 1 and half % 2 == 0):
            return k
        return k + 1 if k % 2 else k - 1

    k_rows = rows_place(lax.rem(my_dp - my_tp + tp_n, tp_n))

    def remote(src, dst, layer, phase, s_slot, r_slot, target):
        return pltpu.make_async_remote_copy(
            src_ref=src,
            dst_ref=dst,
            send_sem=send_sem.at[layer, phase, s_slot],
            recv_sem=recv_sem.at[layer, phase, r_slot],
            device_id=target,
            device_id_type=MESH,
        )

    def column(z, core):
        return {"tp": z, "dp": 2 * my_x + core}

    def row(x):
        return {"dp": 2 * x + my_core}

    layer_list = range(layers)
    fetch = [pltpu.make_async_copy(held[0], r_buf.at[0], local_sem.at[0])]
    used = 1
    for n in range(3):
        whole = (w_z, w_x, w_out)[n]
        for l in layer_list:
            fetch.append(
                pltpu.make_async_copy(
                    held[1 + n].at[l], whole.at[l, my_core], local_sem.at[used]
                )
            )
            used += 1
    for n in range(4, INPUTS):
        fetch.append(pltpu.make_async_copy(held[n], here[n - 4], local_sem.at[used]))
        used += 1
    fetch[0].start()
    barrier = pltpu.get_barrier_semaphore()

    def greet(device):
        pl.semaphore_signal(barrier, inc=1, device_id=device, device_id_type=MESH)

    for k in range(2 * near, 0, -1):
        greet(column(tp_at(k), 0))
        greet(column(tp_at(k), 1))
    for k in range(half - 1, 0, -1):
        greet(row(x_at(k)))
    greet(column(my_tp, 1 - my_core))
    for f in fetch[1:]:
        f.start()

    def copy_a(l, k):
        if k == 0:
            dst = a_buf.at[l, 0, my_core]
            return remote(r_buf.at[l], dst, l, 0, 0, my_core, column(my_tp, row_core))
        slot = sent_place(k)
        dst = a_buf.at[l, slot, my_core]
        return remote(r_buf.at[l], dst, l, 0, k, 2 * slot + my_core, column(tp_at(k), row_core))

    def copy_a2(l, n):
        steps = [(s, False) for s in range(-near, near + 1)]
        steps += [(s, True) for s in range(1 - near, near)]
        s, far = steps[n]
        offset = -s if not far else (half - s if s >= 0 else -half - s)
        slot = offset - 1 if offset > 0 else -offset
        src = r_far.at[1] if far else r_buf.at[l]
        dst = a_buf.at[l, slot, my_core]
        to = column(lax.rem(my_tp + s + tp_n, tp_n), row_core)
        return s, remote(src, dst, l, 0, n, 2 * slot + my_core, to)

    def each_a(l, act):
        if l == 0:
            copies = [(k, copy_a(l, k)) for k in range(2 * near, -1, -1)]
        else:
            copies = [copy_a2(l, n) for n in range(tp_n)]
        for s, copy in copies:
            if s != 0:
                act(copy)

        @pl.when(uneven)
        def _():
            for s, copy in copies:
                if s == 0:
                    act(copy)

    def send_a(l):
        each_a(l, lambda copy: copy.start())

        @pl.when(jnp.logical_not(uneven))
        def _():
            a_buf[l, 0, my_core] = r_buf[l]
            if l > 0:
                a_buf[l, half - 1, my_core] = r_far[1]

    def offset_of(odd, k):
        if odd:
            return -k if k % 2 else k + 1
        return -k if k % 2 == 0 else k + 1

    def relayed(odd, down):
        offsets = [offset_of(odd, k) for k in range(half)]
        step = near if down else -near
        return [
            (offsets.index(o - step), k)
            for k, o in enumerate(offsets)
            if (o > near if down else o < -near)
        ]

    def copy_relay(source, target, down):
        z = lax.rem(my_tp + (tp_n - near if down else near), tp_n)
        src, dst = a_buf.at[0, source], a_buf.at[0, target]
        return remote(src, dst, 0, 4, target, target, column(z, my_core))

    def relay(odd, down):
        for source, target in relayed(odd, down):
            for core in range(2):
                got = a_buf.at[0, source, core]
                remote(
                    got, got, 0, 0, 0, 2 * source + core, column(rows_at(source), core)
                ).wait_recv()
            copy_relay(source, target, down).start()

    def wait_first_a(odd, k):
        if abs(offset_of(odd, k)) > near:
            copy_relay(k, k, 0).wait_recv()
        elif k not in [source for down in range(2) for source, _ in relayed(odd, down)]:
            for core in range(2):
                got = a_buf.at[0, k, core]
                copy = remote(got, got, 0, 0, k, 2 * k + core, column(rows_at(k), core))
                if offset_of(odd, k) != 0:
                    copy.wait_recv()
                else:

                    @pl.when(my_core != core)
                    def _(copy=copy):
                        copy.wait_recv()

    def copy_b(l, k):
        to = row(lax.div(rows_at(k), 2))
        return remote(b_out.at[l, k], b_in.at[l, my_x], l, 1, k, my_x, to)

    def copy_c(l, k):
        slot = x_mirror(k)
        return remote(c_own.at[l], c_buf.at[l, slot], l, 2, k, slot, row(x_at(k)))

    def copy_d(l, k, core):
        to = column(2 * x_at(k) + my_core, core)
        return remote(d_out.at[l, k, core], d_in.at[l, my_tp], l, 3, 2 * k + core, my_tp, to)

    def copy_d2(l, k, core):
        z = lax.rem(2 * x_at(k) + my_core + half, tp_n)
        src, dst = d_out.at[l, k, core], d_far.at[my_tp]
        return z, remote(src, dst, l, 5, 2 * k + core, my_tp, column(z, core))

    def copy_far():
        src = a_buf.at[0, half - 1, 1 - my_core]
        return remote(src, r_far.at[0], 0, 6, 0, 0, column(my_tp, 1 - my_core))

    def sent_abc(l):
        each_a(l, lambda copy: copy.wait_send())

        if l == 0:
            for odd in range(2):

                @pl.when(uneven == (odd == 1))
                def _(odd=odd):
                    for down in range(2):
                        for source, target in relayed(odd, down):
                            copy_relay(source, target, down).wait_send()

        for k in range(half):

            @pl.when(rows_at(k) != my_dp)
            def _(k=k):
                copy_b(l, k).wait_send()

            if k > 0:
                copy_c(l, k).wait_send()

    def sent_d(l):
        for k in range(half):
            for core in range(2):

                @pl.when(jnp.logical_not((2 * x_at(k) + my_core == my_tp) & (my_core == core)))
                def _(k=k, core=core):
                    copy_d(l, k, core).wait_send()

                if l + 1 < layers:
                    z, copy = copy_d2(l, k, core)

                    @pl.when(jnp.logical_not((z == my_tp) & (my_core == core)))
                    def _(copy=copy):
                        copy.wait_send()

    pl.semaphore_wait(barrier, 4 * near + 1 + half - 1)
    fetch[0].wait()
    send_a(0)

    for f in fetch[1:]:
        f.wait()
    heads_all = w_dtt.shape[1]
    pick = lax.broadcasted_iota(jnp.int32, (16, heads_all), 0)
    col = lax.broadcasted_iota(jnp.int32, (16, heads_all), 1)
    pick = jnp.where((pick < heads_here) & (col == pick + my_tp * heads_here), 1.0, 0.0).astype(BF16)
    for l in range(layers):
        w_bcd[l, my_core, 0:bw] = w_bt[l]
        w_bcd[l, my_core, bw : 2 * bw] = w_ct[l]
        w_bcd[l, my_core, 2 * bw : 2 * bw + 16] = jnp.dot(
            pick, w_dtt[l], preferred_element_type=F32
        ).astype(BF16)
        w_bcd[l, my_core, 2 * bw + 16 :] = jnp.zeros(
            (w_bcd.shape[2] - 2 * bw - 16, width_f), BF16
        )
        conv_bc[l] = jnp.concatenate([conv_b[l].astype(F32), conv_c[l].astype(F32)], axis=1)
        for k in range(s_b.shape[1]):
            s_bc[l, k] = jnp.concatenate([s_b[l, k].astype(F32), s_c[l, k].astype(F32)], axis=1)

    gains[my_core] = jnp.zeros(gains.shape[1:], F32)
    gains[my_core, 0:layers] = gain[...].astype(F32)

    pair = []
    for whole in [gains.at[my_core]] + [
        w.at[l, my_core] for l in layer_list for w in (w_z, w_x, w_bcd, w_out)
    ]:
        pair.append(
            pltpu.make_async_remote_copy(
                src_ref=whole,
                dst_ref=whole,
                send_sem=pair_sem.at[0, len(pair)],
                recv_sem=pair_sem.at[1, len(pair)],
                device_id=column(my_tp, 1 - my_core),
                device_id_type=MESH,
            )
        )
    for p in pair:
        p.start()

    down_first = my_tp < half
    for odd in range(2):
        for order in ((0, 1), (1, 0)):

            @pl.when((uneven == (odd == 1)) & (down_first == (order[0] == 1)))
            def _(odd=odd, order=order):
                for down in order:
                    relay(odd, down)

    def turn(i, carry):
        for l in range(layers):
            block = ssm[l, i].reshape(zw, bw)
            st_t[l, i] = block.T.astype(BF16)
        return carry

    lane = lax.broadcasted_iota(jnp.int32, (rows, LANES), 1)
    head_of = lax.broadcasted_iota(jnp.int32, (rows, zw), 1)
    head_of = lax.div(head_of, hd)

    def per_head(v):
        out = jnp.broadcast_to(v[:, 0:1], (rows, zw))
        for h in range(1, heads_here):
            out = jnp.where(head_of == h, v[:, h : h + 1], out)
        return out

    for l in range(layers):
        if l > 0:
            send_a(l)

        for first in range(0, half, GROUP):
            group = min(GROUP, half)
            if l == 0:
                for odd in range(2):

                    @pl.when(uneven == (odd == 1))
                    def _(odd=odd, first=first, group=group):
                        for k in range(first, first + group):
                            wait_first_a(odd, k)

            else:
                for k in range(first, first + group):
                    for core in range(2):
                        got = a_buf.at[l, k, core]
                        copy = remote(got, got, l, 0, k, 2 * k + core, column(rows_at(k), core))
                        if k not in (0, half - 1):
                            copy.wait_recv()
                        else:

                            @pl.when(uneven | (my_core != core))
                            def _(copy=copy):
                                copy.wait_recv()

            if l == 0 and first == 0:
                for p in pair:
                    p.wait_recv()
            tall = group * rows
            scaled, squares = [], 0.0
            for core in range(2):
                block = a_buf[l, first : first + group, core].reshape(tall, width_f).astype(F32)
                scaled.append((block * gains[core, l : l + 1]).astype(BF16))
                squares = squares + jnp.sum(block * block, axis=1, keepdims=True)
            both_wide = jnp.concatenate(scaled, axis=1)
            part_z = jnp.dot(
                both_wide, w_z[l].reshape(2 * width_f, zw), preferred_element_type=F32
            ).astype(BF16)
            part_x = jnp.dot(
                both_wide, w_x[l].reshape(2 * width_f, zw), preferred_element_type=F32
            ).astype(BF16)
            rest = lax.dot_general(scaled[0], w_bcd[l, 0], NT, preferred_element_type=F32)
            rest += lax.dot_general(scaled[1], w_bcd[l, 1], NT, preferred_element_type=F32)
            lane_tall = lax.broadcasted_iota(jnp.int32, (tall, LANES), 1)
            small = jnp.where(lane_tall == heads_here, squares, rest[:, LANES:])
            low = small - small.astype(BF16).astype(F32)
            both = jnp.where(lane_tall < LANES // 2, small, pltpu.roll(low, LANES // 2, 1))
            b_out[l, first : first + group, :, 0:zw] = part_z.reshape(group, rows, zw)
            b_out[l, first : first + group, :, zw : 2 * zw] = part_x.reshape(group, rows, zw)
            b_out[l, first : first + group, :, 2 * zw : 2 * zw + LANES] = (
                rest[:, 0:LANES].astype(BF16).reshape(group, rows, LANES)
            )
            b_out[l, first : first + group, :, 2 * zw + LANES :] = both.astype(BF16).reshape(
                group, rows, LANES
            )
            for k in range(first, first + group):

                @pl.when(rows_at(k) != my_dp)
                def _(k=k, l=l):
                    copy_b(l, k).start()

        if l == 0:

            @pl.when(jnp.logical_not(uneven))
            def _():
                copy_far().start()
                r_far[0] = a_buf[0, half - 1, my_core]

            lax.fori_loop(0, rows, turn, 0)
        total = b_out[l, k_rows].astype(F32)
        for k in range(1, half):
            x = x_at(k)
            remote(b_in.at[l, x], b_in.at[l, x], l, 1, k, x, row(x)).wait_recv()
            total = total + b_in[l, x].astype(F32)

        small = total[:, 2 * zw + LANES :]
        small = small + pltpu.roll(small, LANES // 2, 1)
        row_scale = lax.rsqrt(small[:, heads_here : heads_here + 1] / features + EPSILON)
        step_raw = small[:, 0:heads_here] * row_scale
        gate = (total[:, 0:zw] * row_scale).astype(BF16).astype(F32)
        x_new = (total[:, zw : 2 * zw] * row_scale).astype(BF16)
        bc_new = (total[:, 2 * zw : 2 * zw + LANES] * row_scale).astype(BF16)
        taps = conv_x.shape[1]
        conv = x_new.astype(F32) * conv_x[l, taps - 1 : taps].astype(F32)
        conv2 = bc_new.astype(F32) * conv_bc[l, taps - 1 : taps]
        for k in range(taps - 1):
            conv = conv + s_x[l, k].astype(F32) * conv_x[l, k : k + 1].astype(F32)
            conv2 = conv2 + s_bc[l, k] * conv_bc[l, k : k + 1]
        v = silu(conv)
        bc = silu(conv2)
        step = jax.nn.softplus(step_raw + dt_bias[l : l + 1])
        decay = jnp.exp(-step * jnp.exp(a_log[l : l + 1]))
        xs = per_head(step) * v
        turned = pltpu.roll(bc, LANES // 2, 1)
        b_dot_c = 0.5 * jnp.sum(bc * turned, axis=1, keepdims=True)
        cc = jnp.where(lane < LANES // 2, turned, bc)
        seq = lax.broadcasted_iota(jnp.int32, (rows, LANES), 0)
        pieces = []
        for s in range(0, rows, 2):
            pieces.append(jnp.where(seq == s + lax.div(lane, LANES // 2), cc, 0.0).astype(BF16))
        spread = jnp.concatenate(pieces, axis=1)
        reads = jnp.dot(
            spread, st_t[l].reshape(rows * bw, zw), preferred_element_type=F32
        )
        readout = per_head(decay) * reads + (xs * b_dot_c + per_head(d_skip[l : l + 1]) * v)
        gated = readout * silu(gate)
        scale = lax.rsqrt(jnp.mean(gated * gated, axis=1, keepdims=True) + EPSILON)
        mixed = (gated * scale * out_gain[l : l + 1].astype(F32)).astype(BF16)

        c_own[l] = mixed
        c_buf[l, 0] = mixed

        for k in range(half - 1, 0, -1):
            copy_c(l, k).start()

        for first in range(0, half, GROUP):
            group = min(GROUP, half)
            for k in range(max(first, 1), first + group):
                got = c_buf.at[l, k]
                remote(got, got, l, 2, k, k, row(x_at(k))).wait_recv()
            block = c_buf[l, first : first + group].reshape(group * rows, zw)
            for core in range(2):
                part = jnp.dot(block, w_out[l, core], preferred_element_type=F32).astype(BF16)
                d_out[l, first : first + group, core] = part.reshape(group, rows, width_f)
            for k in range(first, first + group):
                z = 2 * x_at(k) + my_core
                for core in range(2):
                    mine = (z == my_tp) & (my_core == core)

                    @pl.when(jnp.logical_not(mine))
                    def _(k=k, core=core, l=l):
                        copy_d(l, k, core).start()

                    @pl.when(mine)
                    def _(k=k, core=core, l=l):
                        d_in[l, my_tp] = d_out[l, k, core]

                    if l + 1 < layers:
                        z2, copy = copy_d2(l, k, core)
                        mine2 = (z2 == my_tp) & (my_core == core)

                        @pl.when(jnp.logical_not(mine2))
                        def _(copy=copy):
                            copy.start()

                        @pl.when(mine2)
                        def _(k=k, core=core, l=l):
                            d_far[my_tp] = d_out[l, k, core]

        xs_t = xs.T
        for s in range(rows):
            for h in range(heads_here):
                b_row = bc[s : s + 1, 0:bw]
                xs_col = xs_t[h * hd : (h + 1) * hd, s : s + 1]
                ssm_o[l, s, h] = ssm[l, s, h] * decay[s : s + 1, h : h + 1] + xs_col * b_row
        for k in range(taps - 2):
            nx_o[l, k] = s_x[l, k + 1]
            nb_o[l, k] = s_b[l, k + 1]
            nc_o[l, k] = s_c[l, k + 1]
        nx_o[l, taps - 2] = x_new
        nb_o[l, taps - 2] = bc_new[:, 0:bw]
        nc_o[l, taps - 2] = bc_new[:, bw : 2 * bw]

        sent_abc(l)
        if l > 0:
            sent_d(l - 1)

        @pl.when(uneven)
        def _(l=l):
            got = d_in.at[l, my_tp]
            remote(got, got, l, 3, 0, my_tp, column(my_tp, row_core)).wait_recv()

        projected = d_in[l, my_tp].astype(F32)
        for k in range(1, tp_n):
            z = tp_at(k)
            got = d_in.at[l, z]
            remote(got, got, l, 3, k, z, column(z, row_core)).wait_recv()
            projected = projected + d_in[l, z].astype(F32)
        new = (r_buf[l].astype(F32) + projected).astype(BF16)
        if l + 1 < layers:
            r_buf[l + 1] = new

            @pl.when(uneven)
            def _(l=l):
                copy_far().wait_recv()
                got = d_far.at[my_tp]
                remote(got, got, l, 5, 0, my_tp, column(my_tp, row_core)).wait_recv()

            @pl.when(jnp.logical_not(uneven))
            def _():
                copy_far().wait_send()

            projected = d_far[my_tp].astype(F32)
            for k in range(1, tp_n):
                z = tp_at(k)
                got = d_far.at[z]
                remote(got, got, l, 5, k, z, column(z, row_core)).wait_recv()
                projected = projected + d_far[z].astype(F32)
            r_far[1] = (r_far[0].astype(F32) + projected).astype(BF16)
        else:
            res_o[...] = new

    sent_d(layers - 1)
    for p in pair:
        p.wait_send()


def write_out(*refs):
    sem = refs[-1]
    half = len(refs) // 2
    copies = []
    for n in range(half):
        cuts = refs[n].shape[1] // 4 if len(refs[n].shape) == 5 else 0
        for at in range(4 * refs[n].shape[0]) if cuts else (None,):
            src, dst = refs[n], refs[half + n]
            if cuts:
                part = pl.ds(at % 4 * cuts, cuts)
                src, dst = src.at[at // 4, part], dst.at[at // 4, part]
            copies.append(pltpu.make_async_copy(src, dst, sem.at[len(copies)]))
    for c in copies:
        c.start()
    for c in copies:
        c.wait()


def body(tp_n, dp_n, *args):
    (
        tokens,
        norm_gain,
        w_z,
        w_x,
        w_b,
        w_c,
        w_dt,
        conv_x,
        conv_b,
        conv_c,
        dt_bias,
        a_log,
        d_skip,
        out_gain,
        w_out,
        ssm_state,
        state_x,
        state_b,
        state_c,
    ) = args
    layers, heads_here = dt_bias.shape
    rows, width_f = tokens.shape
    zw, bw = w_z.shape[2], w_b.shape[2]
    assert tp_n == dp_n and layers == 2 and tp_n % 8 == 0 and 2 * bw == LANES
    wide = 2 * zw + 2 * LANES
    half = tp_n // 2

    def turn(a):
        return jnp.swapaxes(a, 1, 2)

    operands = (
        tokens,
        w_z,
        w_x,
        w_out,
        norm_gain,
        turn(w_b),
        turn(w_c),
        turn(w_dt),
        conv_x,
        conv_b,
        conv_c,
        dt_bias,
        a_log,
        d_skip,
        out_gain,
        ssm_state,
        turn(state_x),
        turn(state_b),
        turn(state_c),
    )
    vmem = pl.BlockSpec(memory_space=pltpu.VMEM)
    hbm = pl.BlockSpec(memory_space=pltpu.HBM)

    def like(a):
        return pltpu.VMEM(a.shape, a.dtype)

    results = pl.pallas_call(
        functools.partial(kernel, tp_n, dp_n, width_f * dp_n),
        out_shape=(
            like(tokens),
            like(ssm_state),
            like(operands[16]),
            like(operands[17]),
            like(operands[18]),
        ),
        in_specs=[hbm] * INPUTS,
        out_specs=(vmem,) * 5,
        scratch_shapes=[
            pltpu.VMEM((layers, half, 2, rows, width_f), BF16),
            pltpu.VMEM((layers, half, rows, wide), BF16),
            pltpu.VMEM((layers, half, rows, wide), BF16),
            pltpu.VMEM((layers, rows, zw), BF16),
            pltpu.VMEM((layers, half, rows, zw), BF16),
            pltpu.VMEM((layers, half, 2, rows, width_f), BF16),
            pltpu.VMEM((layers, tp_n, rows, width_f), BF16),
            pltpu.VMEM((layers, rows, width_f), BF16),
            pltpu.VMEM((layers, 2, width_f, zw), BF16),
            pltpu.VMEM((layers, 2, width_f, zw), BF16),
            pltpu.VMEM((layers, 2, zw, width_f), BF16),
            pltpu.VMEM((layers, 2, 2 * LANES, width_f), BF16),
            pltpu.VMEM((2, 8, width_f), F32),
            pltpu.VMEM((layers, conv_x.shape[1], LANES), F32),
            pltpu.VMEM((layers, state_b.shape[2], rows, LANES), F32),
            pltpu.VMEM((layers, rows, bw, zw), BF16),
            *(pltpu.VMEM(a.shape, a.dtype) for a in operands[4:]),
            pltpu.VMEM((tp_n, rows, width_f), BF16),
            pltpu.VMEM((2, rows, width_f), BF16),
            pltpu.SemaphoreType.DMA((INPUTS - 3 + 3 * layers,)),
            pltpu.SemaphoreType.DMA((2, 1 + 4 * layers)),
            pltpu.SemaphoreType.DMA((layers, 7, tp_n)),
            pltpu.SemaphoreType.DMA((layers, 7, tp_n)),
        ],
        compiler_params=pltpu.CompilerParams(
            collective_id=0, has_side_effects=True, vmem_limit_bytes=40 * 1024 * 1024
        ),
        name="decode",
    )(*(pltpu.with_memory_space_constraint(a, pltpu.HBM) for a in operands))
    results = [pltpu.with_memory_space_constraint(a, pltpu.VMEM) for a in results]
    residual, ssm_next, next_x, next_b, next_c = pl.pallas_call(
        write_out,
        out_shape=tuple(jax.ShapeDtypeStruct(a.shape, a.dtype) for a in results),
        in_specs=(vmem,) * 5,
        out_specs=(hbm,) * 5,
        scratch_shapes=[pltpu.SemaphoreType.DMA((4 + 4 * layers,))],
        compiler_params=pltpu.CompilerParams(vmem_limit_bytes=8 * 1024 * 1024),
        name="write_out",
    )(*results)
    return residual, ssm_next, turn(next_x), turn(next_b), turn(next_c)


def solution(mesh):
    placed = (
        P(("grp", "tp"), "dp"),
        P(None, "dp"),
        P(None, "dp", "tp"),
        P(None, "dp", "tp"),
        P(None, "dp", "tp"),
        P(None, "dp", "tp"),
        P(None, "dp", None),
        P(None, None, "tp"),
        P(None, None, "tp"),
        P(None, None, "tp"),
        P(None, "tp"),
        P(None, "tp"),
        P(None, "tp"),
        P(None, "tp"),
        P(None, "tp", "dp"),
        P(None, ("grp", "dp"), "tp", None, None),
        P(None, ("grp", "dp"), None, "tp"),
        P(None, ("grp", "dp"), None, "tp"),
        P(None, ("grp", "dp"), None, "tp"),
    )
    return jax.shard_map(
        functools.partial(body, mesh.shape["tp"], mesh.shape["dp"]),
        mesh=mesh,
        in_specs=placed,
        out_specs=(placed[0], placed[15], placed[16], placed[17], placed[18]),
        check_vma=False,
    )
```
